32 devices in a mesh: ep: 8 (over z, core), tp: 4 (over y, x).
Axes of the slice: x: 2, y: 2, z: 4, core: 2. Of those that a mesh axis runs over, the one named last changes fastest.
Arguments:
- receptance: bfloat16 [2048, 2048], P('ep', 'tp'), may hold values from -6 to 6
- key_in: bfloat16 [2048, 2048], P('ep', 'tp'), may hold values from -6 to 6
- value_in: bfloat16 [2048, 2048], P('ep', 'tp'), may hold values from -6 to 6
- decay_in: bfloat16 [2048, 2048], P('ep', 'tp'), may hold values from -16 to 2
- rate_in: bfloat16 [2048, 2048], P('ep', 'tp'), may hold values from -12 to 4
- norm_gain: float32 [2048], P('tp'), may hold values from 0.1 to 1.9
- out_weight: bfloat16 [2048, 4096], P('tp'), may hold values from -0.125 to 0.125
- moe_in: bfloat16 [1024, 4096], P('ep'), may hold values from -6 to 6
- ffn_gain: float32 [4096], replicated, may hold values from 0.1 to 1.9
- routes: int32 [1024, 4], P('ep'), may hold values from 0 to 7, all different within a row; in each aligned block of 128 rows (0 to 127, 128 to 255, ...) at most 80 rows name the same one
- route_weights: float32 [1024, 4], P('ep'), may hold values from 0.2 to 1
- gate_weight: bfloat16 [8, 4096, 1024], P('ep', None, 'tp'), may hold values from -0.09375 to 0.09375
- up_weight: bfloat16 [8, 4096, 1024], P('ep', None, 'tp'), may hold values from -0.09375 to 0.09375
- down_weight: bfloat16 [8, 1024, 4096], P('ep', None, 'tp'), may hold values from -0.1875 to 0.1875
Outputs:
- mixer_out: bfloat16 [2048, 4096], P(('ep', 'tp'))
- moe_out: bfloat16 [1024, 4096], P('ep', 'tp')
The draws below stay inside these ranges and needn't reach their ends.
Inputs may be any that keep to these rules, and one draw needn't show every extreme that they name: `routes`: A row names 4 different experts. Among the 128 rows that one index of ep holds, no expert is named by more than 80 rows, and in every draw some expert is named by exactly 80 of them.
All inputs are finite; a program needn't handle non-finite values.
Results may differ from the reference program's by a relative error of at most 0.025.
Values may be sent and summed in bfloat16 or wider, within the bound.
A program may use at most 64 MiB of HBM per device.

```python
import math
import jax
import jax.numpy as jnp
import numpy as np
from jax import lax

D = 4096
HEADS = 32
HD = 64
FE = 1024
TOPK = 4
TOK_DEV = 256
R_DEV = 128
WIDTH = 2048
TOKENS = 2048
MOE_ROWS = 1024
EXPERTS = 8
CAP = 80
N_EP = 8
N_TP = 4


def slow_heads(key):
    chance = 0.5
    return jax.random.uniform(jax.random.fold_in(key, 11), (HEADS,)) < chance


def span_offsets(key, salt, reach):
    span_count = TOKENS // TOK_DEV
    offsets = jax.random.uniform(jax.random.fold_in(key, salt), (span_count, HEADS), jnp.float32, -reach, reach)
    return jnp.repeat(offsets, TOK_DEV, axis=0)[:, :, None]


def jitter(key, salt, spread):
    shape = (TOKENS, HEADS, HD)
    return jax.random.normal(jax.random.fold_in(key, salt), shape, jnp.float32) * spread


def draw_decay_in(key, part):
    slow = slow_heads(key)
    level = jnp.where(slow, math.log(0.5 / TOKENS) + 0.5, math.log(1.0 / 40.0) + 0.5).astype(jnp.float32)
    values = level[None, :, None] + span_offsets(key, 12, 1.0) + jitter(key, 13, 0.5)
    return jnp.clip(values, -16.0, 2.0).reshape(TOKENS, HEADS * HD).astype(jnp.bfloat16)


def draw_rate_in(key, part):
    slow = slow_heads(key)
    level = jnp.where(slow, math.log(0.5 * HD / TOKENS), 0.0).astype(jnp.float32)
    spread = jnp.where(slow, 0.5, 1.0).astype(jnp.float32)[None, :, None]
    values = level[None, :, None] + span_offsets(key, 14, 0.7) + jitter(key, 15, 1.0) * spread
    return jnp.clip(values, -12.0, 4.0).reshape(TOKENS, HEADS * HD).astype(jnp.bfloat16)


def block_levels(rng, extent, split, low, high):
    loudness, own = 1.0, jax.random.fold_in(rng, 6)
    for axis_at, parts in split:
        heights = jnp.exp(jax.random.uniform(jax.random.fold_in(own, axis_at), (parts,), jnp.float32, low / len(split), high / len(split)))
        loudness = loudness * jnp.repeat(heights, extent[axis_at] // parts).reshape([-1 if axis == axis_at else 1 for axis in range(len(extent))])
    return loudness


def routed_block(stream_key, own, number, rows, number_of, top, bound, slope):
    sequence = jax.random.permutation(stream_key, number_of)
    heavy_load, common = shares(number_of, rows * top, bound, slope, True), shares(number_of, rows * top, bound, slope, False)
    places = jnp.arange(number_of)

    def named(sizes, rotation):
        used = int((sizes > 0).sum())
        fixed = max(1, used // 4)
        moved = fixed + (places - fixed + rotation * (used - fixed)) % max(1, number_of - fixed)
        return jnp.zeros((number_of,), jnp.int32).at[sequence[jnp.where(places < fixed, places, moved)]].set(jnp.asarray(sizes, jnp.int32))

    sizes = jnp.where(number % 4 == 0, named(heavy_load, number // 4), named(common, number - number // 4 - 1))
    mixed = jax.random.permutation(jax.random.fold_in(own, 3), number_of)
    giver, sink = mixed[0:number_of // 2 * 2:2], mixed[1:number_of // 2 * 2:2]
    margin = jnp.minimum(sizes[giver] - 1, bound - sizes[sink]) // 2
    margin = jnp.where((giver == sequence[0]) | (sink == sequence[0]) | (sizes[sink] == 0), 0, jnp.maximum(margin, 0))
    moved = jax.random.randint(jax.random.fold_in(own, 4), (number_of // 2,), 0, 1 << 20) % (margin + 1)
    sizes = sizes.at[giver].add(-moved).at[sink].add(moved)
    members = jnp.searchsorted(jnp.cumsum(sizes), jnp.arange(rows * top), side="right").astype(jnp.int32)
    table = members.reshape(top, rows).T
    table = table[jax.random.permutation(jax.random.fold_in(own, 1), rows)]
    rotation = jax.random.randint(jax.random.fold_in(own, 2), (rows, 1), 0, top)
    return jnp.take_along_axis(table, (jnp.arange(top)[None, :] + rotation) % top, axis=1)


def shares(count, total, limit, slope, full):
    weights = [(1 << 20) // math.isqrt(rank ** slope) + 1 for rank in range(1, count + 1)]
    largest = limit if full else min(limit, max(-(-total // count), total * weights[0] // sum(weights)))
    least = 1 if total - largest >= count - 1 else 0
    given, surplus = [largest] + [least] * (count - 1), total - largest - least * (count - 1)
    while surplus > 0:
        movable = [i for i in range(1, count) if given[i] < largest] or [i for i in range(1, count) if given[i] < limit]
        pool, remaining = sum([weights[i] for i in movable]), surplus
        for i in movable:
            addition = min(limit - given[i], max(1, remaining * weights[i] // pool), surplus)
            given[i] = given[i] + addition
            surplus = surplus - addition
    return np.array(given)


def scatter_about(rng, dims, width, most, cuts=(), held_as=jnp.bfloat16):
    values = jax.random.normal(rng, dims, jnp.float32) * width
    if len(cuts) > 0:
        values = block_levels(rng, dims, cuts, -0.22, 0.18) * values
    return jnp.clip(values, min=-most, max=most).astype(held_as)


def setup_inputs(seed: int = 0) -> dict:
    seeds = jax.random.split(jax.random.key(seed), 15)
    receptance = scatter_about(seeds[0], (TOKENS, WIDTH), 1.0, 6.0, ((0, 8), (1, 4)))
    key_in = scatter_about(seeds[1], (TOKENS, WIDTH), 1.0, 6.0, ((0, 8), (1, 4)))
    value_in = scatter_about(seeds[2], (TOKENS, WIDTH), 1.0, 6.0, ((0, 8), (1, 4)))
    decay_in = draw_decay_in(jax.random.fold_in(seeds[14], 71), 0)
    rate_in = draw_rate_in(jax.random.fold_in(seeds[14], 71), 0)
    norm_gain = jnp.clip(1.0 + 0.18 * jax.random.normal(seeds[5], (WIDTH,), jnp.float32), 0.1, 1.9)
    out_weight = scatter_about(seeds[6], (WIDTH, D), WIDTH ** -0.5, 0.125, ((0, 4),))
    moe_in = scatter_about(seeds[7], (MOE_ROWS, D), 1.0, 6.0, ((0, 8),))
    ffn_gain = jnp.clip(1.0 + 0.18 * jax.random.normal(seeds[8], (D,), jnp.float32), 0.1, 1.9)
    routes_keys = jax.random.split(jax.random.fold_in(seeds[9], 1), MOE_ROWS // R_DEV)
    routes_turns = jax.random.permutation(jax.random.fold_in(seeds[9], 3), MOE_ROWS // R_DEV)
    routes = jax.vmap(lambda own, number: routed_block(jax.random.fold_in(seeds[9], 2), own, number, R_DEV, EXPERTS, TOPK, CAP, 1))(routes_keys, routes_turns).reshape((MOE_ROWS, TOPK))
    route_weights = jnp.clip(0.2 + 0.8 * jax.random.uniform(seeds[10], (MOE_ROWS, TOPK), jnp.float32) ** block_levels(seeds[10], (MOE_ROWS, TOPK), ((0, 8),), -0.2, 0.2), 0.2, 1.0)
    gate_weight = scatter_about(seeds[11], (EXPERTS, D, FE), D ** -0.5, 0.09375, ((0, 8), (2, 4)))
    up_weight = scatter_about(seeds[12], (EXPERTS, D, FE), D ** -0.5, 0.09375, ((0, 8), (2, 4)))
    down_weight = scatter_about(seeds[13], (EXPERTS, FE, D), FE ** -0.5, 0.1875, ((0, 8), (2, 4)))
    return {"receptance": receptance, "key_in": key_in, "value_in": value_in, "decay_in": decay_in, "rate_in": rate_in, "norm_gain": norm_gain, "out_weight": out_weight, "moe_in": moe_in, "ffn_gain": ffn_gain, "routes": routes, "route_weights": route_weights, "gate_weight": gate_weight, "up_weight": up_weight, "down_weight": down_weight}


EXACT_MATMUL = lax.Precision.HIGHEST

def mixer_reference(receptance, key_in, value_in, decay_in, rate_in, norm_gain, out_weight):
    shape = (TOKENS, HEADS, HD)
    readout = receptance.astype(jnp.float32).reshape(shape)
    key_rows = key_in.astype(jnp.float32).reshape(shape)
    value_rows = value_in.astype(jnp.float32).reshape(shape)
    log_decay = -jnp.exp(-jax.nn.softplus(-decay_in.astype(jnp.float32)) - 0.5).reshape(shape)
    learn_rate = jax.nn.sigmoid(rate_in.astype(jnp.float32)).reshape(shape)
    unit_key = key_rows / jnp.sqrt(lax.optimization_barrier(jnp.sum(key_rows * key_rows, axis=-1, keepdims=True)) + 1.0)

    def advance(passed_state, inputs):
        current_readout, key_now, value_now, decay_now, rate_now, current_unit_key = inputs
        sequence_walk = jnp.einsum('bw,bwo->bo', current_unit_key, passed_state, precision=EXACT_MATMUL)
        passed_state = jnp.exp(decay_now)[:, :, None] * passed_state - (current_unit_key * rate_now)[:, :, None] * sequence_walk[:, None, :] + (key_now * rate_now)[:, :, None] * value_now[:, None, :]
        return (passed_state, jnp.einsum('bw,bwo->bo', current_readout, passed_state, precision=EXACT_MATMUL))
    start = jnp.zeros((HEADS, HD, HD), jnp.float32)
    _, heads_out = lax.scan(advance, start, (readout, key_rows, value_rows, log_decay, learn_rate, unit_key))
    center = heads_out - lax.optimization_barrier(jnp.mean(heads_out, axis=-1, keepdims=True))
    spread = lax.optimization_barrier(jnp.mean(center * center, axis=-1, keepdims=True))
    normed = center * lax.rsqrt(spread + 1.0) * norm_gain.astype(jnp.float32).reshape(HEADS, HD)
    mixed = normed.reshape(TOKENS, WIDTH).astype(jnp.bfloat16)
    group_width = WIDTH // N_TP

    def add_group(running, group_index):
        columns = lax.dynamic_slice_in_dim(mixed, group_index * group_width, group_width, 1)
        weights = lax.dynamic_slice_in_dim(out_weight, group_index * group_width, group_width, 0)
        product = jnp.dot(columns, weights, preferred_element_type=jnp.float32).astype(jnp.bfloat16)
        product = lax.optimization_barrier(product)
        return (running + product.astype(jnp.float32), None)
    summed, _ = lax.scan(add_group, jnp.zeros((TOKENS, D), jnp.float32), jnp.arange(N_TP, dtype=jnp.int32))
    return summed.astype(jnp.bfloat16)

def expert_reference(moe_in, ffn_gain, routes, route_weights, gate_weight, up_weight, down_weight):
    row_values = moe_in.astype(jnp.float32)
    scaled = row_values * lax.rsqrt(lax.optimization_barrier(jnp.mean(row_values * row_values, axis=-1, keepdims=True)) + 1.0) * ffn_gain
    normed_rows = scaled.astype(jnp.bfloat16)
    pairs = routes.reshape(-1).astype(jnp.int32)
    pair_count = pairs.shape[0]
    onehot = (pairs[:, None] == jnp.arange(EXPERTS, dtype=jnp.int32)[None, :]).astype(jnp.int32)
    slot_rank = lax.optimization_barrier(jnp.sum((jnp.cumsum(onehot, axis=0) - onehot) * onehot, axis=1)).astype(jnp.int32)
    capacity = N_EP * CAP
    position = (pairs * capacity + slot_rank).astype(jnp.int32)
    source = jnp.zeros((EXPERTS * capacity,), jnp.int32).at[position].set(jnp.arange(pair_count, dtype=jnp.int32) // TOPK).reshape(EXPERTS, capacity)
    filled = jnp.zeros((EXPERTS * capacity,), jnp.int32).at[position].set(1).reshape(EXPERTS, capacity)

    def one_expert(operands):
        source_rows, live, gate_matrix, up_matrix, down_matrix = operands
        taken = jnp.where(live[:, None] > 0, normed_rows[source_rows], jnp.zeros((), normed_rows.dtype))
        gate = jnp.dot(taken, gate_matrix, preferred_element_type=jnp.float32)
        up_part = jnp.dot(taken, up_matrix, preferred_element_type=jnp.float32)
        hidden = (jax.nn.silu(gate) * up_part).astype(jnp.bfloat16)
        return jnp.dot(hidden, down_matrix, preferred_element_type=jnp.float32).astype(jnp.bfloat16)
    results = lax.map(one_expert, (source, filled, gate_weight, up_weight, down_weight))
    per_pair = results.reshape(EXPERTS * capacity, D)[position].astype(jnp.float32).reshape(MOE_ROWS, TOPK, D)
    portion = route_weights / lax.optimization_barrier(jnp.sum(route_weights, axis=-1, keepdims=True))
    return lax.optimization_barrier(jnp.sum(portion[:, :, None] * per_pair, axis=1)).astype(jnp.bfloat16)

def reference(receptance, key_in, value_in, decay_in, rate_in, norm_gain, out_weight, moe_in, ffn_gain, routes, route_weights, gate_weight, up_weight, down_weight):
    mixer_out = mixer_reference(receptance, key_in, value_in, decay_in, rate_in, norm_gain, out_weight)
    moe_out = expert_reference(moe_in, ffn_gain, routes, route_weights, gate_weight, up_weight, down_weight)
    return (mixer_out, moe_out)
```

```python
import functools

import jax
import jax.numpy as jnp
from jax import lax
from jax.experimental import pallas as pl
from jax.experimental.pallas import tpu as pltpu
from jax.sharding import PartitionSpec as P

HD = 64
BLOCK = 64
F32 = jnp.float32
BF16 = jnp.bfloat16
MESH = pl.DeviceIdType.MESH


def dot(a, b):
    return jnp.dot(a.astype(BF16), b.astype(BF16), preferred_element_type=F32)


def dot_rows(a, b):
    return lax.dot_general(
        a.astype(BF16), b.astype(BF16), (((1,), (1,)), ((), ())), preferred_element_type=F32
    )


def dot_cols(a, b):
    return lax.dot_general(
        a.astype(BF16), b.astype(BF16), (((0,), (0,)), ((), ())), preferred_element_type=F32
    )


def halves(a):
    high = a.astype(BF16)
    return high, (a - high.astype(F32)).astype(BF16)


def dot_left(mask, b):
    high, low = halves(b)
    return dot(mask, high) + dot(mask, low)


def dot_right(a, mask):
    high, low = halves(a)
    return dot(high, mask) + dot(low, mask)


def lane_head(rows, width):
    return lax.broadcasted_iota(jnp.int32, (rows, width), 1) // HD


def spread(packed):
    rows, width = packed.shape
    packed = packed.astype(BF16)
    head = lane_head(rows, width)
    return jnp.concatenate(
        [jnp.where(head == i, packed, jnp.zeros_like(packed)) for i in range(width // HD)], axis=0
    )


def fold(square):
    width = square.shape[1]
    head = lane_head(HD, width)
    out = jnp.zeros((HD, width), F32)
    for i in range(width // HD):
        out = jnp.where(head == i, square[i * HD : (i + 1) * HD], out)
    return out


def head_ones(width):
    row = lax.broadcasted_iota(jnp.int32, (width, width), 0) // HD
    return (row == lane_head(width, width)).astype(BF16)


def group_width(columns):
    return HD * max(g for g in (4, 2, 1) if columns % (g * HD) == 0)


def tables_block(block, mix_in, read_ref, local_ref, total_ref, carry, last):
    columns = read_ref.shape[1]
    width = group_width(columns)
    row = lax.broadcasted_iota(jnp.int32, (BLOCK, width), 0)
    lane = lax.broadcasted_iota(jnp.int32, (BLOCK, width), 1) % HD
    strict = lane < row
    closed = lane <= row
    eye = (lane == row).astype(F32)
    tril = (
        lax.broadcasted_iota(jnp.int32, (BLOCK, BLOCK), 1)
        <= lax.broadcasted_iota(jnp.int32, (BLOCK, BLOCK), 0)
    ).astype(BF16)
    ones = head_ones(width)
    rows = pl.ds(block * BLOCK, BLOCK)
    for group in range(columns // width):
        at = pl.ds(group * width, width)
        readout = mix_in[0, rows, at].astype(F32)
        key = mix_in[1, rows, at].astype(F32)
        value = mix_in[2, rows, at]
        log_decay = jax.nn.sigmoid(mix_in[3, rows, at].astype(F32)) * -0.6065306597126334
        rate = jax.nn.sigmoid(mix_in[4, rows, at].astype(F32))
        unit = key * lax.rsqrt(dot_right(key * key, ones) + 1.0)
        inclusive = dot_left(tril, log_decay)
        total = inclusive[BLOCK - 1 :]
        probe = -unit * jnp.exp(inclusive - log_decay)
        removal = unit * rate
        written = key * rate
        back = jnp.exp(-inclusive)
        tail = jnp.exp(total - inclusive)
        readout = readout * jnp.exp(inclusive)
        left = jnp.concatenate([probe, readout], axis=0)
        on_removal = dot_rows(left, spread(removal * back))
        on_write = dot_rows(left, spread(written * back))
        lower = jnp.where(strict, on_removal[:BLOCK], 0.0)
        reach = jnp.where(closed, on_removal[BLOCK:], 0.0)
        lower_write = jnp.where(strict, on_write[:BLOCK], 0.0)
        reach_write = jnp.where(closed, on_write[BLOCK:], 0.0)
        value_wide = spread(value)
        on_value = dot(jnp.concatenate([lower_write, reach_write], axis=0), value_wide)
        inverse = eye + lower
        power = dot(lower, spread(lower))
        for doubling in range(BLOCK.bit_length() - 2):
            wide = spread(power)
            if doubling < BLOCK.bit_length() - 3:
                both = dot(jnp.concatenate([inverse, power], axis=0), wide)
                inverse = inverse + both[:BLOCK]
                power = both[BLOCK:]
            else:
                inverse = inverse + dot(inverse, wide)
        solved_probe = dot(inverse, spread(probe))
        solved_values = dot(inverse, spread(on_value[:BLOCK]))
        transition = eye * jnp.exp(total) + fold(dot_cols(removal * tail, solved_probe))
        increment = fold(
            dot_cols(
                jnp.concatenate([removal * tail, written * tail], axis=0),
                jnp.concatenate([solved_values.astype(BF16), value], axis=0),
            )
        )
        read_state = readout + dot(reach, spread(solved_probe))
        local_out = dot(reach, spread(solved_values)) + on_value[BLOCK:]
        if block == 0:
            new_map, new_add = transition, increment
            read_ref[rows, at] = read_state.astype(BF16)
            local_ref[rows, at] = local_out
        else:
            left = jnp.concatenate([read_state, transition], axis=0)
            on_map = dot(left, spread(carry[0, group]))
            on_add = dot(left, spread(carry[1, group]))
            read_ref[rows, at] = on_map[:BLOCK].astype(BF16)
            local_ref[rows, at] = on_add[:BLOCK] + local_out
            new_map, new_add = on_map[BLOCK:], on_add[BLOCK:] + increment
        if last:
            total_ref[0, group] = new_map.astype(BF16)
            total_ref[1, group] = new_add.astype(BF16)
        else:
            carry[0, group] = new_map
            carry[1, group] = new_add


def flip(me, bits):
    bit = 1
    while bit <= bits:
        if bits & bit:
            me = me + bit - 2 * bit * ((me // bit) % 2)
        bit *= 2
    return me


def bit_list(count):
    return [1 << b for b in range(count.bit_length() - 1)]


class Exchange:
    def __init__(self, count, slots, sems, unit):
        me = lax.axis_index("tp")
        half = slots.shape[1] // 2
        bits = bit_list(count)
        self.count, self.copies, self.heads, self.relays, self.seen = count, {}, [], [], set()
        for number in range(len(bits)):
            for stream, order in enumerate((bits, bits[::-1])):
                at = pl.ds(stream * half, half)
                known = [0]
                for bit in order[:number]:
                    known += [k ^ bit for k in known]
                for from_delta in known:
                    bit = order[number]
                    key = (stream, from_delta ^ bit)
                    owner = flip(me, from_delta)
                    self.copies[key] = pltpu.make_async_remote_copy(
                        src_ref=slots.at[owner, at],
                        dst_ref=slots.at[owner, at],
                        send_sem=sems.at[unit, 0, stream, key[1]],
                        recv_sem=sems.at[unit, 1, stream, key[1]],
                        device_id={"tp": flip(me, bit)},
                        device_id_type=MESH,
                    )
                    if from_delta:
                        self.relays.append((key, from_delta))
                    else:
                        self.heads.append(key)

    def start(self, streams=(0, 1)):
        for key in self.heads:
            if key[0] in streams:
                self.copies[key].start()

    def arrive(self, stream, delta):
        if (stream, delta) not in self.seen:
            self.seen.add((stream, delta))
            self.copies[stream, delta].wait_recv()

    def relay(self):
        for key, from_delta in self.relays:
            self.arrive(key[0], from_delta)
            self.copies[key].start()

    def wait(self, delta):
        for stream in (0, 1):
            self.arrive(stream, delta)

    def finish(self):
        for copy in self.copies.values():
            copy.wait_send()


class Prefix:
    def __init__(self, count, own, outgoing, incoming, before, sems):
        self.me, self.count = lax.axis_index("ep"), count
        self.own, self.outgoing, self.incoming, self.before = own, outgoing, incoming, before
        self.steps = bit_list(count)
        self.copies = []
        for number, step in enumerate(self.steps):
            source = own if number == 0 else outgoing.at[number - 1]
            target = incoming.at[number]
            if number == len(self.steps) - 1:
                source, target = source.at[1], target.at[1]
            self.copies.append(
                pltpu.make_async_remote_copy(
                    src_ref=source,
                    dst_ref=target,
                    send_sem=sems.at[0, number],
                    recv_sem=sems.at[1, number],
                    device_id={"ep": lax.rem(self.me + step, count)},
                    device_id_type=MESH,
                )
            )

    def begin(self):
        groups, width = self.own.shape[1], self.own.shape[3]
        lane = lax.broadcasted_iota(jnp.int32, (HD, width), 1) % HD
        eye = (lane == lax.broadcasted_iota(jnp.int32, (HD, width), 0)).astype(F32)
        for group in range(groups):
            self.before[0, group] = eye
            self.before[1, group] = jnp.zeros_like(eye)

    def send(self, number):
        pl.when(self.me + self.steps[number] < self.count)(self.copies[number].start)

    def receive(self, number):
        last = number == len(self.steps) - 1
        groups = self.own.shape[1]
        own, before, incoming = self.own, self.before, self.incoming

        @pl.when(self.me >= self.steps[number])
        def _():
            self.copies[number].wait_recv()
            for group in range(groups):
                left = before[0, group]
                before[1, group] += dot(left, spread(incoming[number, 1, group]))
                if not last:
                    before[0, group] = dot(left, spread(incoming[number, 0, group]))

        if not last:
            for group in range(groups):
                left = own[0, group]
                self.outgoing[number, 0, group] = dot(left, spread(before[0, group])).astype(BF16)
                self.outgoing[number, 1, group] = (
                    dot(left, spread(before[1, group])) + own[1, group].astype(F32)
                ).astype(BF16)

    def finish(self):
        for step, copy in zip(self.steps, self.copies):
            pl.when(self.me + step < self.count)(copy.wait_send)


class Reduce:
    def __init__(self, count, parts, landing, sems):
        self.me = lax.axis_index("tp")
        self.parts, self.landing = parts, landing
        self.half = parts.shape[2] // 2
        bits = bit_list(count)
        self.orders = (bits, bits[::-1])
        self.stages, self.copies = [], {}
        left = [list(range(count))] * 2
        for number in range(len(bits)):
            stage = []
            for stream in (0, 1):
                bit = self.orders[stream][number]
                sent = [d for d in left[stream] if d & bit]
                left[stream] = [d for d in left[stream] if not d & bit]
                at = pl.ds(stream * self.half, self.half)
                for delta in sent:
                    owner = flip(self.me, delta)
                    self.copies[stream, delta] = pltpu.make_async_remote_copy(
                        src_ref=parts.at[owner, :, at],
                        dst_ref=landing.at[delta, :, at],
                        send_sem=sems.at[0, stream, delta],
                        recv_sem=sems.at[1, stream, delta],
                        device_id={"tp": flip(self.me, bit)},
                        device_id_type=MESH,
                    )
                    stage.append((stream, delta, bit))
            self.stages.append(stage)

    def start(self, number):
        for stream, delta, _ in self.stages[number]:
            self.copies[stream, delta].start()

    def land(self, number, out=None):
        for stream, delta, bit in self.stages[number]:
            at = pl.ds(stream * self.half, self.half)
            self.copies[stream, delta].wait_recv()
            mine = flip(self.me, delta ^ bit)
            total = self.parts[mine, :, at].astype(F32) + self.landing[delta, :, at].astype(F32)
            if out is None:
                self.parts[mine, :, at] = total.astype(BF16)
            else:
                out[:, at] = total.astype(BF16)

    def finish(self):
        for copy in self.copies.values():
            copy.wait_send()


class Dispatch:
    def __init__(self, chips, tp_count, rows, info, sems, info_sems, pair_sems, pair_info):
        me = lax.axis_index("ep")
        self.tp = lax.axis_index("tp")
        self.tp_count = tp_count
        self.core, self.chip, self.chips = lax.rem(me, 2), me // 2, chips
        self.me, self.partner = me, me + 1 - 2 * self.core
        self.rows, self.info = rows, info
        self.sems, self.info_sems = sems, info_sems
        self.pair_sems, self.pair_info = pair_sems, pair_info
        self.half = rows.shape[2] // 2

    def remote(self, ref, send, recv, to):
        return pltpu.make_async_remote_copy(
            src_ref=ref,
            dst_ref=ref,
            send_sem=send,
            recv_sem=recv,
            device_id={"ep": to},
            device_id_type=MESH,
        )

    def along(self, k, half, way, to):
        to = jnp.clip(to, 0, self.chips - 1)
        ref = self.rows.at[2 * k + self.core, self.tp, pl.ds(half * self.half, self.half)]
        return self.remote(
            ref, self.sems.at[way, k, half], self.sems.at[2, k, half], 2 * to + self.core
        )

    def along_info(self, k, way, to):
        to = jnp.clip(to, 0, self.chips - 1)
        ref = self.info.at[2 * k + self.core]
        return self.remote(
            ref, self.info_sems.at[way, k], self.info_sems.at[2, k], 2 * to + self.core
        )

    def across(self, k, place):
        ref = self.rows.at[2 * k + self.core, place]
        return self.remote(
            ref, self.pair_sems.at[0, k, place], self.pair_sems.at[1, k, place], self.partner
        )

    def from_partner(self, k, place):
        ref = self.rows.at[2 * k + 1 - self.core, place]
        return self.remote(
            ref, self.pair_sems.at[0, k, place], self.pair_sems.at[1, k, place], self.partner
        )

    def across_info(self, k, other=False):
        core = 1 - self.core if other else self.core
        ref = self.info.at[2 * k + core]
        return self.remote(ref, self.pair_info.at[0, k], self.pair_info.at[1, k], self.partner)

    def sides(self):
        return (
            (self.chip + 1 < self.chips, 0, self.chip + 1),
            (self.chip > 0, 1, self.chip - 1),
        )

    def send_own(self):
        for half in (0, 1):
            for inside, way, to in self.sides():
                pl.when(inside)(self.along(self.chip, half, way, to).start)
        for place in range(self.tp_count):
            self.across(self.chip, place).start()

    def send_info(self):
        for inside, way, to in self.sides():
            pl.when(inside)(self.along_info(self.chip, way, to).start)
        self.across_info(self.chip).start()

    def onward(self, k):
        right = k < self.chip
        to = jnp.where(right, self.chip + 1, self.chip - 1)
        return (to >= 0) & (to < self.chips), jnp.where(right, 0, 1), to

    def landed(self, k, exchange):
        moving, way, to = self.onward(k)
        for half in (0, 1):
            self.along(k, half, way, to).wait_recv()
            pl.when(moving)(self.along(k, half, way, to).start)
            exchange.start((half,))
        self.across(k, self.tp).start()
        self.along_info(k, way, to).wait_recv()
        pl.when(moving)(self.along_info(k, way, to).start)
        self.across_info(k).start()

    def shared(self, k, exchange, delta):
        exchange.wait(delta)
        self.across(k, flip(self.tp, delta)).start()

    def finish(self, order):
        for half in (0, 1):
            for inside, way, to in self.sides():
                pl.when(inside)(self.along(self.chip, half, way, to).wait_send)
        for inside, way, to in self.sides():
            pl.when(inside)(self.along_info(self.chip, way, to).wait_send)
        for k in order:
            moving, way, to = self.onward(k)
            for half in (0, 1):
                pl.when(moving)(self.along(k, half, way, to).wait_send)
            pl.when(moving)(self.along_info(k, way, to).wait_send)
        for k in [self.chip] + order:
            for place in range(self.tp_count):
                self.across(k, place).wait_send()
            self.across_info(k).wait_send()


def chip_order(chip, chips):
    table = [
        sorted((k for k in range(chips) if k != at), key=lambda k: (abs(k - at), k))
        for at in range(chips)
    ]
    return [
        sum(jnp.where(chip == at, table[at][number], 0) for at in range(chips))
        for number in range(chips - 1)
    ]


class Back:
    def __init__(self, count, placed, out, pair_in, held, from_left, from_right, sems):
        me = lax.axis_index("ep")
        self.chips = count // 2
        self.core = lax.rem(me, 2)
        self.chip = me // 2
        self.partner = me + 1 - 2 * self.core
        self.half = out.shape[0] // 2
        self.right_to = jnp.minimum(me + 2, count - 2 + self.core)
        self.left_to = jnp.maximum(me - 2, self.core)
        self.placed, self.out, self.pair_in, self.held = placed, out, pair_in, held
        self.from_left, self.from_right, self.sems = from_left, from_right, sems

    def send(self, source, target, kind, item, to):
        at, part = item
        rows = pl.ds(part * self.half, self.half)
        return pltpu.make_async_remote_copy(
            src_ref=source.at[rows],
            dst_ref=target.at[at, rows],
            send_sem=self.sems.at[kind, 0, 2 * at + part],
            recv_sem=self.sems.at[kind, 1, 2 * at + part],
            device_id={"ep": to},
            device_id_type=MESH,
        )

    def pair(self, item):
        source = self.placed.at[2 * item[0] + 1 - self.core]
        return self.send(source, self.pair_in, 0, item, self.partner)

    def right(self, item, source=None):
        source = self.from_left if source is None else source
        return self.send(source.at[item[0]], self.from_left, 1, item, self.right_to)

    def left(self, item, source=None):
        source = self.from_right if source is None else source
        return self.send(source.at[item[0]], self.from_right, 2, item, self.left_to)

    def pair_sum(self, item):
        at, part = item
        rows = pl.ds(part * self.half, self.half)
        self.pair(item).wait_recv()
        self.held[at, rows] = (
            self.placed[2 * at + self.core, rows].astype(F32) + self.pair_in[at, rows].astype(F32)
        ).astype(BF16)

    def forward(self, item, moving, hop, landing, origin):
        at, part = item
        rows = pl.ds(part * self.half, self.half)

        @pl.when(moving & origin)
        def _():
            hop(item, self.held).start()

        @pl.when(moving & jnp.logical_not(origin))
        def _():
            relay = hop(item)
            relay.wait_recv()
            landing[at, rows] = (
                landing[at, rows].astype(F32) + self.held[at, rows].astype(F32)
            ).astype(BF16)
            relay.start()

    def run(self):
        chips, chip = self.chips, self.chip
        ready = []
        for step in range(chips):
            for at in (chips - 1 - step, step):
                if at not in ready:
                    self.pair_sum((at, 0))
                    self.pair_sum((at, 1))
                    ready.append(at)
            for part in (0, 1):

                def rightward(at=chips - 1 - step, part=part):
                    if at > 0:
                        self.forward(
                            (at, part), at > chip, self.right, self.from_left, chip == 0
                        )

                def leftward(at=step, part=part):
                    if at < chips - 1:
                        self.forward(
                            (at, part), at < chip, self.left, self.from_right, chip == chips - 1
                        )

                @pl.when(chip < chips // 2)
                def _():
                    rightward()
                    leftward()

                @pl.when(chip >= chips // 2)
                def _():
                    leftward()
                    rightward()

    def collect(self):
        chip, at = self.chip, self.chip
        for part in (0, 1):
            rows = pl.ds(part * self.half, self.half)
            self.out[rows] = self.held[at, rows]
            for inside, hop, landing in (
                (chip > 0, self.right, self.from_left),
                (chip < self.chips - 1, self.left, self.from_right),
            ):

                @pl.when(inside)
                def _():
                    hop((at, part)).wait_recv()
                    self.out[rows] = (
                        self.out[rows].astype(F32) + landing[at, rows].astype(F32)
                    ).astype(BF16)

    def finish(self):
        for at in range(self.chips):
            for part in (0, 1):
                item = (at, part)
                self.pair(item).wait_send()
                pl.when(at > self.chip)(self.right(item).wait_send)
                pl.when(at < self.chip)(self.left(item).wait_send)


def layer_kernel(
    tp_count,
    ep_count,
    cap,
    expert_count,
    mixer_hbm,
    gain_ref,
    weight_hbm,
    moe_hbm,
    ffn_ref,
    routes_ref,
    route_weights_ref,
    gate_hbm,
    up_hbm,
    down_hbm,
    mixer_out,
    moe_out,
    rows,
    info,
    mix_in,
    gate_w,
    up_w,
    down_w,
    out_w,
    picked,
    hidden,
    read,
    local_out,
    carry,
    total,
    outgoing,
    incoming,
    before,
    mixed,
    product,
    landing,
    placed,
    pair_in,
    held,
    from_left,
    from_right,
    load_sems,
    along_sems,
    along_info_sems,
    pair_sems,
    pair_info_sems,
    row_sems,
    hidden_sems,
    prefix_sems,
    reduce_sems,
    back_sems,
):
    tp = lax.axis_index("tp")
    place = lax.axis_index("ep")
    chips = ep_count // 2
    chip = place // 2
    steps, bits = bit_list(ep_count), bit_list(tp_count)
    row_count, part_width = rows.shape[2], rows.shape[3]
    units = gate_w.shape[1]
    moe_loads = [
        pltpu.make_async_copy(
            moe_hbm.at[:, pl.ds(t * part_width, part_width)], rows.at[place, t], load_sems.at[t]
        )
        for t in range(tp_count)
    ]
    mixer_loads = [
        pltpu.make_async_copy(source, mix_in.at[i], load_sems.at[tp_count + i])
        for i, source in enumerate(mixer_hbm)
    ]
    weight_loads = [
        pltpu.make_async_copy(source, target, load_sems.at[tp_count + 5 + i])
        for i, (source, target) in enumerate(
            ((gate_hbm, gate_w), (up_hbm, up_w), (down_hbm, down_w), (weight_hbm, out_w))
        )
    ]
    for load in moe_loads + mixer_loads + weight_loads:
        load.start()

    barrier = pltpu.get_barrier_semaphore()

    def signal(axis, to):
        pl.semaphore_signal(barrier, inc=1, device_id={axis: to}, device_id_type=MESH)

    for bit in bits:
        signal("tp", flip(tp, bit))
    for step in steps:
        pl.when(place + step < ep_count)(lambda: signal("ep", place + step))
        pl.when(place >= step)(lambda: signal("ep", place - step))
    peers = sum(
        jnp.where(place + step < ep_count, 1, 0) + jnp.where(place >= step, 1, 0)
        for step in steps
    )
    for load in moe_loads:
        load.wait()
    pl.semaphore_wait(barrier, peers + len(bits))

    dispatch = Dispatch(
        chips, tp_count, rows, info, along_sems, along_info_sems, pair_sems, pair_info_sems
    )
    order = chip_order(chip, chips)
    dispatch.send_own()

    squares = jnp.zeros((row_count, 1), F32)
    for t in range(tp_count):
        part = rows[place, t].astype(F32)
        squares += jnp.sum(part * part, axis=1, keepdims=True)
    scale = lax.rsqrt(squares / (tp_count * part_width) + 1.0)
    names = lax.broadcasted_iota(jnp.int32, (row_count, 128), 1)
    portion = route_weights_ref[...]
    portion = portion / jnp.sum(portion, axis=1, keepdims=True)
    named = jnp.zeros((row_count, 128), F32)
    table = jnp.where(names == expert_count, scale, 0.0)
    for choice in range(routes_ref.shape[1]):
        match = routes_ref[:, choice : choice + 1] == names
        named = jnp.where(match, 1.0, named)
        table = jnp.where(match, portion[:, choice : choice + 1], table)
    earlier = (
        lax.broadcasted_iota(jnp.int32, (row_count, row_count), 1)
        < lax.broadcasted_iota(jnp.int32, (row_count, row_count), 0)
    ).astype(BF16)
    rank = jnp.where(named > 0.0, dot(earlier, named), -1.0)
    info[place, :expert_count] = rank.T[:expert_count]
    info[place, expert_count : 2 * expert_count + 8] = table.T[: expert_count + 8]
    dispatch.send_info()

    slot = lax.broadcasted_iota(jnp.int32, (cap, row_count), 0).astype(F32)

    def chosen(source):
        return info[source, pl.ds(place, 1), :] == slot

    def slot_value(pick, source, index):
        return jnp.sum(
            jnp.where(pick, info[source, pl.ds(index, 1), :], 0.0), axis=1, keepdims=True
        )

    sources = [chip] + order
    exchanges = [None] + [
        Exchange(tp_count, rows.at[2 * k + dispatch.core], row_sems, n)
        for n, k in enumerate(order)
    ]
    hidden_exchanges = [
        Exchange(tp_count, hidden.at[n], hidden_sems, n) for n in range(chips)
    ]

    def gate_up(n):
        k = sources[n]
        if n > 0:
            for delta in range(1, tp_count):
                exchanges[n].wait(delta)
        for t in range(tp_count):
            dispatch.from_partner(k, t).wait_recv()
        dispatch.across_info(k, True).wait_recv()
        for core in (0, 1):
            source = 2 * k + core
            pick = chosen(source)
            factor = slot_value(pick, source, 2 * expert_count)
            onehot = pick.astype(BF16)
            for t in range(tp_count):
                part = dot(onehot, rows[source, t]) * factor * ffn_ref[t]
                picked[core * cap : (core + 1) * cap, t * part_width : (t + 1) * part_width] = (
                    part.astype(BF16)
                )
        gate = dot(picked[...], gate_w[...])
        up = dot(picked[...], up_w[...])
        hidden[n, tp] = (jax.nn.silu(gate) * up).astype(BF16)
        hidden_exchanges[n].start()

    back = Back(ep_count, placed, moe_out, pair_in, held, from_left, from_right, back_sems)

    def down(n):
        k = sources[n]
        for delta in range(1, tp_count):
            hidden_exchanges[n].wait(delta)
        result = dot(
            jnp.concatenate([hidden[n, t] for t in range(tp_count)], axis=1), down_w[...]
        )
        for core in (0, 1):
            source = 2 * k + core
            pick = chosen(source)
            share = slot_value(pick, source, expert_count + place)
            mine = result[core * cap : (core + 1) * cap] * share
            placed[source] = dot_cols(pick.astype(BF16), mine).astype(BF16)
        for part in (0, 1):
            back.pair((k, part)).start()

    def landed(n):
        dispatch.landed(sources[n], exchanges[n])

    def relay(n):
        exchanges[n].relay()
        for delta in range(1, tp_count):
            if delta & (delta - 1) == 0:
                dispatch.shared(sources[n], exchanges[n], delta)

    def share_rest(n):
        for delta in range(1, tp_count):
            if delta & (delta - 1):
                dispatch.shared(sources[n], exchanges[n], delta)

    tokens = read.shape[0]
    blocks = tokens // BLOCK

    def tables(b):
        tables_block(b, mix_in, read, local_out, total, carry, b == blocks - 1)

    prefix = Prefix(ep_count, total, outgoing, incoming, before, prefix_sems)

    weight_loads[0].wait()
    weight_loads[1].wait()
    gate_up(0)
    for load in mixer_loads:
        load.wait()
    remote = chips - 1
    landed(1)
    block = 0
    for n in range(1, remote + 1):
        if block < blocks:
            tables(block)
            block += 1
        if n + 1 <= remote:
            landed(n + 1)
        relay(n)
        if n != 2:
            hidden_exchanges[max(n - 2, 0)].relay()
        if n > 1:
            share_rest(n - 1)
            gate_up(n - 1)
    while block < blocks:
        tables(block)
        block += 1
    prefix.begin()
    prefix.send(0)
    share_rest(remote)
    gate_up(remote)
    hidden_exchanges[remote - 1].relay()
    prefix.receive(0)
    prefix.send(1)
    weight_loads[2].wait()
    down(0)
    hidden_exchanges[remote].relay()
    for number in range(1, len(steps)):
        prefix.receive(number)
        if number + 1 < len(steps):
            prefix.send(number + 1)
    for n in range(1, remote):
        down(n)

    columns = read.shape[1]
    groups, width = total.shape[1], total.shape[3]
    ones = head_ones(width)
    for group in range(groups):
        at = pl.ds(group * width, width)
        heads_out = dot(read[:, at], spread(before[1, group])) + local_out[:, at]
        center = heads_out - dot_right(heads_out, ones) / HD
        variance = dot_right(center * center, ones) / HD
        mixed[:, at] = (center * lax.rsqrt(variance + 1.0) * gain_ref[:, at]).astype(BF16)
    weight_loads[3].wait()
    out_rows = tokens // tp_count
    tile = out_w.shape[1] // 4
    for number in range(4):
        at = pl.ds(number * tile, tile)
        part = dot(mixed[...], out_w[:, at]).astype(BF16)
        for t in range(tp_count):
            product[t, :, at] = part[t * out_rows : (t + 1) * out_rows]
    reduce = Reduce(tp_count, product, landing, reduce_sems)
    reduce.start(0)
    down(remote)
    back.run()
    for number in range(len(bits)):
        last = number == len(bits) - 1
        reduce.land(number, mixer_out if last else None)
        if not last:
            reduce.start(number + 1)
    back.collect()

    dispatch.finish(order)
    for exchange in exchanges[1:] + hidden_exchanges:
        exchange.finish()
    prefix.finish()
    reduce.finish()
    back.finish()


def local(
    receptance,
    key_in,
    value_in,
    decay_in,
    rate_in,
    norm_gain,
    out_weight,
    moe_in,
    ffn_gain,
    routes,
    route_weights,
    gate_weight,
    up_weight,
    down_weight,
):
    tp_count, ep_count = lax.axis_size("tp"), lax.axis_size("ep")
    row_count, feature_count = moe_in.shape
    expert_count = gate_weight.shape[0] * ep_count
    cap = 5 * row_count * routes.shape[1] // (4 * expert_count)
    cap = -(-cap // 16) * 16
    chips = ep_count // 2
    part_width = feature_count // tp_count
    units, out_part = gate_weight.shape[2], down_weight.shape[2]
    tokens, columns = receptance.shape
    width = group_width(columns)
    groups = columns // width
    steps = ep_count.bit_length() - 1
    out_rows = tokens // tp_count
    dim = out_weight.shape[1]
    vmem = pl.BlockSpec(memory_space=pltpu.VMEM)
    hbm = pl.BlockSpec(memory_space=pl.ANY)
    state = (2, groups, HD, width)
    dma = pltpu.SemaphoreType.DMA

    def kernel(r, k, v, d, a, *refs):
        layer_kernel(tp_count, ep_count, cap, expert_count, (r, k, v, d, a), *refs)

    return pl.pallas_call(
        kernel,
        out_shape=[
            jax.ShapeDtypeStruct((out_rows, dim), BF16),
            jax.ShapeDtypeStruct((row_count, out_part), BF16),
        ],
        in_specs=[hbm] * 5 + [vmem, hbm, hbm, vmem, vmem, vmem, hbm, hbm, hbm],
        out_specs=[vmem, vmem],
        scratch_shapes=[
            pltpu.VMEM((ep_count, tp_count, row_count, part_width), BF16),
            pltpu.VMEM((ep_count, 2 * expert_count + 8, row_count), F32),
            pltpu.VMEM((5, tokens, columns), BF16),
            pltpu.VMEM((feature_count, units), BF16),
            pltpu.VMEM((feature_count, units), BF16),
            pltpu.VMEM(down_weight.shape[1:], BF16),
            pltpu.VMEM(out_weight.shape, BF16),
            pltpu.VMEM((2 * cap, feature_count), BF16),
            pltpu.VMEM((chips, tp_count, 2 * cap, units), BF16),
            pltpu.VMEM((tokens, columns), BF16),
            pltpu.VMEM((tokens, columns), F32),
            pltpu.VMEM(state, F32),
            pltpu.VMEM(state, BF16),
            pltpu.VMEM((steps, *state), BF16),
            pltpu.VMEM((steps, *state), BF16),
            pltpu.VMEM(state, F32),
            pltpu.VMEM((tokens, columns), BF16),
            pltpu.VMEM((tp_count, out_rows, dim), BF16),
            pltpu.VMEM((tp_count, out_rows, dim), BF16),
            pltpu.VMEM((ep_count, row_count, out_part), BF16),
            pltpu.VMEM((chips, row_count, out_part), BF16),
            pltpu.VMEM((chips, row_count, out_part), BF16),
            pltpu.VMEM((chips, row_count, out_part), BF16),
            pltpu.VMEM((chips, row_count, out_part), BF16),
            dma((tp_count + 9,)),
            dma((3, chips, 2)),
            dma((3, chips)),
            dma((2, chips, tp_count)),
            dma((2, chips)),
            dma((chips - 1, 2, 2, tp_count)),
            dma((chips, 2, 2, tp_count)),
            dma((2, steps)),
            dma((2, 2, tp_count)),
            dma((3, 2, 2 * chips)),
        ],
        compiler_params=pltpu.CompilerParams(
            collective_id=0, has_side_effects=True, vmem_limit_bytes=63 * 1024 * 1024
        ),
        name="layer",
    )(
        receptance,
        key_in,
        value_in,
        decay_in,
        rate_in,
        norm_gain[None],
        out_weight,
        moe_in,
        ffn_gain.reshape(tp_count, 1, part_width),
        routes,
        route_weights,
        gate_weight[0],
        up_weight[0],
        down_weight[0],
    )


def solution(mesh):
    return jax.shard_map(
        local,
        mesh=mesh,
        in_specs=(
            P("ep", "tp"),
            P("ep", "tp"),
            P("ep", "tp"),
            P("ep", "tp"),
            P("ep", "tp"),
            P("tp"),
            P("tp", None),
            P("ep", None),
            P(),
            P("ep", None),
            P("ep", None),
            P("ep", None, "tp"),
            P("ep", None, "tp"),
            P("ep", None, "tp"),
        ),
        out_specs=(P(("ep", "tp"), None), P("ep", "tp")),
        check_vma=False,
    )
```

```python
import jax
import jax.numpy as jnp
from jax import lax
from jax.experimental import pallas as pl
from jax.experimental.pallas import tpu as pltpu
from jax.sharding import PartitionSpec as P

HD = 64
BLOCK = 64
F32 = jnp.float32
BF16 = jnp.bfloat16
MESH = pl.DeviceIdType.MESH


def dot(a, b):
    return jnp.dot(a.astype(BF16), b.astype(BF16), preferred_element_type=F32)


def dot_rows(a, b):
    return lax.dot_general(
        a.astype(BF16), b.astype(BF16), (((1,), (1,)), ((), ())), preferred_element_type=F32
    )


def dot_cols(a, b):
    return lax.dot_general(
        a.astype(BF16), b.astype(BF16), (((0,), (0,)), ((), ())), preferred_element_type=F32
    )


def halves(a):
    high = a.astype(BF16)
    return high, (a - high.astype(F32)).astype(BF16)


def dot_left(mask, b):
    high, low = halves(b)
    return dot(mask, high) + dot(mask, low)


def dot_right(a, mask):
    high, low = halves(a)
    return dot(high, mask) + dot(low, mask)


def lane_head(rows, width):
    return lax.broadcasted_iota(jnp.int32, (rows, width), 1) // HD


def spread(packed):
    rows, width = packed.shape
    packed = packed.astype(BF16)
    head = lane_head(rows, width)
    return jnp.concatenate(
        [jnp.where(head == i, packed, jnp.zeros_like(packed)) for i in range(width // HD)], axis=0
    )


def fold(square):
    width = square.shape[1]
    head = lane_head(HD, width)
    out = jnp.zeros((HD, width), F32)
    for i in range(width // HD):
        out = jnp.where(head == i, square[i * HD : (i + 1) * HD], out)
    return out


def head_ones(width):
    row = lax.broadcasted_iota(jnp.int32, (width, width), 0) // HD
    return (row == lane_head(width, width)).astype(BF16)


def group_width(columns):
    return HD * max(g for g in (4, 2, 1) if columns % (g * HD) == 0)


def tables_block(block, mix_in, read_ref, local_ref, total_ref, carry, last):
    columns = read_ref.shape[1]
    width = group_width(columns)
    row = lax.broadcasted_iota(jnp.int32, (BLOCK, width), 0)
    lane = lax.broadcasted_iota(jnp.int32, (BLOCK, width), 1) % HD
    strict = lane < row
    closed = lane <= row
    eye = (lane == row).astype(F32)
    tril = (
        lax.broadcasted_iota(jnp.int32, (BLOCK, BLOCK), 1)
        <= lax.broadcasted_iota(jnp.int32, (BLOCK, BLOCK), 0)
    ).astype(BF16)
    ones = head_ones(width)
    rows = pl.ds(block * BLOCK, BLOCK)
    for group in range(columns // width):
        at = pl.ds(group * width, width)
        readout = mix_in[0, rows, at].astype(F32)
        key = mix_in[1, rows, at].astype(F32)
        value = mix_in[2, rows, at]
        log_decay = jax.nn.sigmoid(mix_in[3, rows, at].astype(F32)) * -0.6065306597126334
        rate = jax.nn.sigmoid(mix_in[4, rows, at].astype(F32))
        unit = key * lax.rsqrt(dot_right(key * key, ones) + 1.0)
        inclusive = dot_left(tril, log_decay)
        total = inclusive[BLOCK - 1 :]
        probe = -unit * jnp.exp(inclusive - log_decay)
        removal = unit * rate
        written = key * rate
        back = jnp.exp(-inclusive)
        tail = jnp.exp(total - inclusive)
        readout = readout * jnp.exp(inclusive)
        left = jnp.concatenate([probe, readout], axis=0)
        on_removal = dot_rows(left, spread(removal * back))
        on_write = dot_rows(left, spread(written * back))
        lower = jnp.where(strict, on_removal[:BLOCK], 0.0)
        reach = jnp.where(closed, on_removal[BLOCK:], 0.0)
        lower_write = jnp.where(strict, on_write[:BLOCK], 0.0)
        reach_write = jnp.where(closed, on_write[BLOCK:], 0.0)
        value_wide = spread(value)
        on_value = dot(jnp.concatenate([lower_write, reach_write], axis=0), value_wide)
        inverse = eye + lower
        power = dot(lower, spread(lower))
        for doubling in range(BLOCK.bit_length() - 2):
            wide = spread(power)
            if doubling < BLOCK.bit_length() - 3:
                both = dot(jnp.concatenate([inverse, power], axis=0), wide)
                inverse = inverse + both[:BLOCK]
                power = both[BLOCK:]
            else:
                inverse = inverse + dot(inverse, wide)
        solved_probe = dot(inverse, spread(probe))
        solved_values = dot(inverse, spread(on_value[:BLOCK]))
        transition = eye * jnp.exp(total) + fold(dot_cols(removal * tail, solved_probe))
        increment = fold(
            dot_cols(
                jnp.concatenate([removal * tail, written * tail], axis=0),
                jnp.concatenate([solved_values.astype(BF16), value], axis=0),
            )
        )
        read_state = readout + dot(reach, spread(solved_probe))
        local_out = dot(reach, spread(solved_values)) + on_value[BLOCK:]
        if block == 0:
            new_map, new_add = transition, increment
            read_ref[rows, at] = read_state.astype(BF16)
            local_ref[rows, at] = local_out
        else:
            left = jnp.concatenate([read_state, transition], axis=0)
            on_map = dot(left, spread(carry[0, group]))
            on_add = dot(left, spread(carry[1, group]))
            read_ref[rows, at] = on_map[:BLOCK].astype(BF16)
            local_ref[rows, at] = on_add[:BLOCK] + local_out
            new_map, new_add = on_map[BLOCK:], on_add[BLOCK:] + increment
        if last:
            total_ref[0, group] = new_map.astype(BF16)
            total_ref[1, group] = new_add.astype(BF16)
        else:
            carry[0, group] = new_map
            carry[1, group] = new_add


def flip(me, bits):
    bit = 1
    while bit <= bits:
        if bits & bit:
            me = me + bit - 2 * bit * ((me // bit) % 2)
        bit *= 2
    return me


def bit_list(count):
    return [1 << b for b in range(count.bit_length() - 1)]


class Exchange:
    def __init__(self, count, slots, sems, unit, wide=False):
        me = lax.axis_index("tp")
        half = slots.shape[1] // 2
        bits = bit_list(count)
        self.count, self.copies, self.heads, self.relays, self.seen = count, {}, [], [], set()
        self.seconds = []
        for number in range(1 if wide else 0, len(bits)):
            for stream, order in enumerate((bits, bits[::-1])):
                at = pl.ds(stream * half, half)
                known = [0]
                for bit in order[:number]:
                    known += [k ^ bit for k in known]
                for from_delta in known:
                    bit = order[number]
                    key = (stream, from_delta ^ bit)
                    owner = flip(me, from_delta)
                    self.copies[key] = pltpu.make_async_remote_copy(
                        src_ref=slots.at[owner, at],
                        dst_ref=slots.at[owner, at],
                        send_sem=sems.at[unit, 0, stream, key[1]],
                        recv_sem=sems.at[unit, 1, stream, key[1]],
                        device_id={"tp": flip(me, bit)},
                        device_id_type=MESH,
                    )
                    if wide and from_delta == order[0]:
                        self.seconds.append(key)
                    elif from_delta:
                        self.relays.append((key, from_delta))
                    else:
                        self.heads.append(key)

    def start(self, streams=(0, 1)):
        for key in self.heads:
            if key[0] in streams:
                self.copies[key].start()

    def start_seconds(self):
        for key in self.seconds:
            self.copies[key].start()

    def arrive(self, stream, delta):
        if (stream, delta) in self.copies and (stream, delta) not in self.seen:
            self.seen.add((stream, delta))
            self.copies[stream, delta].wait_recv()

    def relay(self):
        for key, from_delta in self.relays:
            self.arrive(key[0], from_delta)
            self.copies[key].start()

    def wait(self, delta):
        for stream in (0, 1):
            self.arrive(stream, delta)

    def finish(self):
        for copy in self.copies.values():
            copy.wait_send()


class Prefix:
    def __init__(self, count, own, outgoing, incoming, before, sems):
        self.me, self.count = lax.axis_index("ep"), count
        self.own, self.outgoing, self.incoming, self.before = own, outgoing, incoming, before
        self.steps = bit_list(count)
        self.copies = []
        for number, step in enumerate(self.steps):
            source = own if number == 0 else outgoing.at[number - 1]
            target = incoming.at[number]
            if number == len(self.steps) - 1:
                source, target = source.at[1], target.at[1]
            self.copies.append(
                pltpu.make_async_remote_copy(
                    src_ref=source,
                    dst_ref=target,
                    send_sem=sems.at[0, number],
                    recv_sem=sems.at[1, number],
                    device_id={"ep": lax.rem(self.me + step, count)},
                    device_id_type=MESH,
                )
            )

    def begin(self):
        groups, width = self.own.shape[1], self.own.shape[3]
        lane = lax.broadcasted_iota(jnp.int32, (HD, width), 1) % HD
        eye = (lane == lax.broadcasted_iota(jnp.int32, (HD, width), 0)).astype(F32)
        for group in range(groups):
            self.before[0, group] = eye
            self.before[1, group] = jnp.zeros_like(eye)

    def send(self, number):
        pl.when(self.me + self.steps[number] < self.count)(self.copies[number].start)

    def receive(self, number):
        last = number == len(self.steps) - 1
        groups = self.own.shape[1]
        own, before, incoming = self.own, self.before, self.incoming

        @pl.when(self.me >= self.steps[number])
        def _():
            self.copies[number].wait_recv()
            for group in range(groups):
                left = before[0, group]
                before[1, group] += dot(left, spread(incoming[number, 1, group]))
                if not last:
                    before[0, group] = dot(left, spread(incoming[number, 0, group]))

        if not last:
            for group in range(groups):
                left = own[0, group]
                self.outgoing[number, 0, group] = dot(left, spread(before[0, group])).astype(BF16)
                self.outgoing[number, 1, group] = (
                    dot(left, spread(before[1, group])) + own[1, group].astype(F32)
                ).astype(BF16)

    def finish(self):
        for step, copy in zip(self.steps, self.copies):
            pl.when(self.me + step < self.count)(copy.wait_send)


class Reduce:
    def __init__(self, count, parts, landing, sems):
        self.me = lax.axis_index("tp")
        self.parts, self.landing = parts, landing
        self.half = parts.shape[2] // 2
        bits = bit_list(count)
        self.orders = (bits, bits[::-1])
        self.stages, self.copies = [], {}
        left = [list(range(count))] * 2
        for number in range(len(bits)):
            stage = []
            for stream in (0, 1):
                bit = self.orders[stream][number]
                sent = [d for d in left[stream] if d & bit]
                left[stream] = [d for d in left[stream] if not d & bit]
                at = pl.ds(stream * self.half, self.half)
                for delta in sent:
                    owner = flip(self.me, delta)
                    self.copies[stream, delta] = pltpu.make_async_remote_copy(
                        src_ref=parts.at[owner, :, at],
                        dst_ref=landing.at[delta, :, at],
                        send_sem=sems.at[0, stream, delta],
                        recv_sem=sems.at[1, stream, delta],
                        device_id={"tp": flip(self.me, bit)},
                        device_id_type=MESH,
                    )
                    stage.append((stream, delta, bit))
            self.stages.append(stage)

    def start(self, number):
        for stream, delta, _ in self.stages[number]:
            self.copies[stream, delta].start()

    def land(self, number, out=None):
        for stream, delta, bit in self.stages[number]:
            at = pl.ds(stream * self.half, self.half)
            self.copies[stream, delta].wait_recv()
            mine = flip(self.me, delta ^ bit)
            total = self.parts[mine, :, at].astype(F32) + self.landing[delta, :, at].astype(F32)
            if out is None:
                self.parts[mine, :, at] = total.astype(BF16)
            else:
                out[:, at] = total.astype(BF16)

    def finish(self):
        for copy in self.copies.values():
            copy.wait_send()


class Dispatch:
    def __init__(
        self, chips, tp_count, rows, info, extra, sems, info_sems, pair_sems, pair_info, extra_sems
    ):
        me = lax.axis_index("ep")
        self.tp = lax.axis_index("tp")
        self.tp_count = tp_count
        self.core, self.chip, self.chips = lax.rem(me, 2), me // 2, chips
        self.me, self.partner = me, me + 1 - 2 * self.core
        self.rows, self.info = rows, info
        self.sems, self.info_sems = sems, info_sems
        self.pair_sems, self.pair_info = pair_sems, pair_info
        self.half = rows.shape[2] // 2
        bits = bit_list(tp_count)
        self.seconds = [flip(self.tp, bits[0]), flip(self.tp, bits[-1])]
        self.extra, self.extra_sems = extra, extra_sems
        self.end = (self.chip == 0) | (self.chip == chips - 1)
        self.last = self.last_of(self.chip)
        self.passed = chips - 1 - self.last

    def last_of(self, chip):
        return jnp.where(chip >= self.chips // 2, 0, self.chips - 1)

    def second(self, k, half):
        return self.rows.at[
            2 * k + self.core, self.seconds[half], pl.ds(half * self.half, self.half)
        ]

    def through(self, half):
        return self.extra.at[pl.ds(half * self.half, self.half)]

    def move(self, source, target, sender, receiver, half, to):
        return pltpu.make_async_remote_copy(
            src_ref=source,
            dst_ref=target,
            send_sem=self.extra_sems.at[0, sender, half],
            recv_sem=self.extra_sems.at[1, receiver, half],
            device_id={"ep": 2 * jnp.clip(to, 0, self.chips - 1) + self.core},
            device_id_type=MESH,
        )

    def origin_moves(self):
        to = jnp.where(self.chip == 0, 1, self.chips - 2)
        for half in (0, 1):
            source = self.second(self.chip, half)
            if self.chips > 2:
                yield self.move(source, self.through(half), 0, 0, half, to)
            else:
                yield self.move(source, source, 0, 1, half, to)

    def away(self, k):
        return jnp.where(k == 0, self.chip + 1, self.chip - 1)

    def send_second(self):
        @pl.when(self.end)
        def _():
            for move in self.origin_moves():
                move.start()

    def pass_moves(self):
        to = self.away(self.passed)
        final = self.last_of(to) == self.passed
        for half in (0, 1):
            source = self.through(half)
            yield final, self.move(source, self.second(self.passed, half), 0, 1, half, to)
            if self.chips > 4:
                yield jnp.logical_not(final), self.move(source, source, 0, 0, half, to)

    def passing(self):
        if self.chips > 2:

            @pl.when(jnp.logical_not(self.end))
            def _():
                for half in (0, 1):
                    source = self.through(half)
                    self.move(source, source, 0, 0, half, self.chip).wait_recv()
                for wanted, move in self.pass_moves():
                    pl.when(wanted)(move.start)

    def last_moves(self):
        to = self.away(self.last)
        for half in (0, 1):
            source = self.second(self.last, half)
            yield (to >= 0) & (to < self.chips), self.move(source, source, 1, 1, half, to)

    def take_second(self, exchange):
        for half, (moving, move) in enumerate(self.last_moves()):
            move.wait_recv()
            pl.when(moving)(move.start)
        exchange.start_seconds()

    def finish_second(self):
        @pl.when(self.end)
        def _():
            for move in self.origin_moves():
                move.wait_send()

        if self.chips > 2:

            @pl.when(jnp.logical_not(self.end))
            def _():
                for wanted, move in self.pass_moves():
                    pl.when(wanted)(move.wait_send)

        for moving, move in self.last_moves():
            pl.when(moving)(move.wait_send)

    def remote(self, ref, send, recv, to):
        return pltpu.make_async_remote_copy(
            src_ref=ref,
            dst_ref=ref,
            send_sem=send,
            recv_sem=recv,
            device_id={"ep": to},
            device_id_type=MESH,
        )

    def along(self, k, half, way, to):
        to = jnp.clip(to, 0, self.chips - 1)
        ref = self.rows.at[2 * k + self.core, self.tp, pl.ds(half * self.half, self.half)]
        return self.remote(
            ref, self.sems.at[way, k, half], self.sems.at[2, k, half], 2 * to + self.core
        )

    def along_info(self, k, way, to):
        to = jnp.clip(to, 0, self.chips - 1)
        ref = self.info.at[2 * k + self.core]
        return self.remote(
            ref, self.info_sems.at[way, k], self.info_sems.at[2, k], 2 * to + self.core
        )

    def across(self, k, place):
        ref = self.rows.at[2 * k + self.core, place]
        return self.remote(
            ref, self.pair_sems.at[0, k, place], self.pair_sems.at[1, k, place], self.partner
        )

    def from_partner(self, k, place):
        ref = self.rows.at[2 * k + 1 - self.core, place]
        return self.remote(
            ref, self.pair_sems.at[0, k, place], self.pair_sems.at[1, k, place], self.partner
        )

    def across_info(self, k, other=False):
        core = 1 - self.core if other else self.core
        ref = self.info.at[2 * k + core]
        return self.remote(ref, self.pair_info.at[0, k], self.pair_info.at[1, k], self.partner)

    def sides(self):
        return (
            (self.chip + 1 < self.chips, 0, self.chip + 1),
            (self.chip > 0, 1, self.chip - 1),
        )

    def send_own(self):
        for half in (0, 1):
            for inside, way, to in self.sides():
                pl.when(inside)(self.along(self.chip, half, way, to).start)
        for place in range(self.tp_count):
            self.across(self.chip, place).start()

    def send_info(self):
        for inside, way, to in self.sides():
            pl.when(inside)(self.along_info(self.chip, way, to).start)
        self.across_info(self.chip).start()
        self.send_second()

    def onward(self, k):
        right = k < self.chip
        to = jnp.where(right, self.chip + 1, self.chip - 1)
        return (to >= 0) & (to < self.chips), jnp.where(right, 0, 1), to

    def landed(self, k, exchange):
        moving, way, to = self.onward(k)
        for half in (0, 1):
            self.along(k, half, way, to).wait_recv()
            pl.when(moving)(self.along(k, half, way, to).start)
            exchange.start((half,))
        self.across(k, self.tp).start()
        self.along_info(k, way, to).wait_recv()
        pl.when(moving)(self.along_info(k, way, to).start)
        self.across_info(k).start()

    def shared(self, k, exchange, delta):
        exchange.wait(delta)
        self.across(k, flip(self.tp, delta)).start()

    def finish(self, order):
        self.finish_second()
        for half in (0, 1):
            for inside, way, to in self.sides():
                pl.when(inside)(self.along(self.chip, half, way, to).wait_send)
        for inside, way, to in self.sides():
            pl.when(inside)(self.along_info(self.chip, way, to).wait_send)
        for k in order:
            moving, way, to = self.onward(k)
            for half in (0, 1):
                pl.when(moving)(self.along(k, half, way, to).wait_send)
            pl.when(moving)(self.along_info(k, way, to).wait_send)
        for k in [self.chip] + order:
            for place in range(self.tp_count):
                self.across(k, place).wait_send()
            self.across_info(k).wait_send()


def chip_order(chip, chips):
    table = [
        sorted((k for k in range(chips) if k != at), key=lambda k: (abs(k - at), abs(k - (0 if at < chips / 2 else chips - 1))))
        for at in range(chips)
    ]
    return [
        sum(jnp.where(chip == at, table[at][number], 0) for at in range(chips))
        for number in range(chips - 1)
    ]


class Back:
    def __init__(self, count, placed, out, pair_in, held, from_left, from_right, sems):
        me = lax.axis_index("ep")
        self.chips = count // 2
        self.core = lax.rem(me, 2)
        self.chip = me // 2
        self.partner = me + 1 - 2 * self.core
        self.half = out.shape[0] // 2
        self.right_to = jnp.minimum(me + 2, count - 2 + self.core)
        self.left_to = jnp.maximum(me - 2, self.core)
        self.placed, self.out, self.pair_in, self.held = placed, out, pair_in, held
        self.from_left, self.from_right, self.sems = from_left, from_right, sems

    def send(self, source, target, kind, item, to):
        at, part = item
        rows = pl.ds(part * self.half, self.half)
        return pltpu.make_async_remote_copy(
            src_ref=source.at[rows],
            dst_ref=target.at[at, rows],
            send_sem=self.sems.at[kind, 0, 2 * at + part],
            recv_sem=self.sems.at[kind, 1, 2 * at + part],
            device_id={"ep": to},
            device_id_type=MESH,
        )

    def pair(self, item):
        source = self.placed.at[2 * item[0] + 1 - self.core]
        return self.send(source, self.pair_in, 0, item, self.partner)

    def right(self, item, source=None):
        source = self.from_left if source is None else source
        return self.send(source.at[item[0]], self.from_left, 1, item, self.right_to)

    def left(self, item, source=None):
        source = self.from_right if source is None else source
        return self.send(source.at[item[0]], self.from_right, 2, item, self.left_to)

    def pair_sum(self, item):
        at, part = item
        rows = pl.ds(part * self.half, self.half)
        self.pair(item).wait_recv()
        self.held[at, rows] = (
            self.placed[2 * at + self.core, rows].astype(F32) + self.pair_in[at, rows].astype(F32)
        ).astype(BF16)

    def forward(self, item, moving, hop, landing, origin):
        at, part = item
        rows = pl.ds(part * self.half, self.half)

        @pl.when(moving & origin)
        def _():
            hop(item, self.held).start()

        @pl.when(moving & jnp.logical_not(origin))
        def _():
            relay = hop(item)
            relay.wait_recv()
            landing[at, rows] = (
                landing[at, rows].astype(F32) + self.held[at, rows].astype(F32)
            ).astype(BF16)
            relay.start()

    def run(self, between):
        chips, chip = self.chips, self.chip
        ready = []
        for step in range(chips):
            for at in (chips - 1 - step, step):
                if at not in ready:
                    self.pair_sum((at, 0))
                    self.pair_sum((at, 1))
                    ready.append(at)
            for part in (0, 1):

                def rightward(at=chips - 1 - step, part=part):
                    if at > 0:
                        self.forward(
                            (at, part), at > chip, self.right, self.from_left, chip == 0
                        )

                def leftward(at=step, part=part):
                    if at < chips - 1:
                        self.forward(
                            (at, part), at < chip, self.left, self.from_right, chip == chips - 1
                        )

                @pl.when(chip < chips // 2)
                def _():
                    rightward()
                    leftward()

                @pl.when(chip >= chips // 2)
                def _():
                    leftward()
                    rightward()

            for action, *given in between.get(step, ()):
                action(*given)

    def collect(self):
        chip, at = self.chip, self.chip
        for part in (0, 1):
            rows = pl.ds(part * self.half, self.half)
            self.out[rows] = self.held[at, rows]
            for inside, hop, landing in (
                (chip > 0, self.right, self.from_left),
                (chip < self.chips - 1, self.left, self.from_right),
            ):

                @pl.when(inside)
                def _():
                    hop((at, part)).wait_recv()
                    self.out[rows] = (
                        self.out[rows].astype(F32) + landing[at, rows].astype(F32)
                    ).astype(BF16)

    def finish(self):
        for at in range(self.chips):
            for part in (0, 1):
                item = (at, part)
                self.pair(item).wait_send()
                pl.when(at > self.chip)(self.right(item).wait_send)
                pl.when(at < self.chip)(self.left(item).wait_send)


def layer_kernel(
    tp_count,
    ep_count,
    cap,
    expert_count,
    mixer_hbm,
    gain_hbm,
    weight_hbm,
    moe_hbm,
    ffn_hbm,
    routes_hbm,
    route_weights_hbm,
    gate_hbm,
    up_hbm,
    down_hbm,
    mixer_hbm_out,
    moe_hbm_out,
    mixer_out,
    moe_out,
    gain_ref,
    ffn_ref,
    routes_ref,
    route_weights_ref,
    rows,
    info,
    extra,
    mix_in,
    gate_w,
    up_w,
    down_w,
    out_w,
    picked,
    hidden,
    read,
    local_out,
    carry,
    total,
    outgoing,
    incoming,
    before,
    mixed,
    product,
    landing,
    placed,
    pair_in,
    held,
    from_left,
    from_right,
    load_sems,
    along_sems,
    along_info_sems,
    pair_sems,
    pair_info_sems,
    extra_sems,
    row_sems,
    hidden_sems,
    prefix_sems,
    reduce_sems,
    back_sems,
):
    tp = lax.axis_index("tp")
    place = lax.axis_index("ep")
    chips = ep_count // 2
    chip = place // 2
    steps, bits = bit_list(ep_count), bit_list(tp_count)
    row_count, part_width = rows.shape[2], rows.shape[3]
    units = gate_w.shape[1]
    moe_loads = [
        pltpu.make_async_copy(
            moe_hbm.at[:, pl.ds(t * part_width, part_width)], rows.at[place, t], load_sems.at[t]
        )
        for t in range(tp_count)
    ]
    mixer_loads = [
        pltpu.make_async_copy(source, mix_in.at[i], load_sems.at[tp_count + i])
        for i, source in enumerate(mixer_hbm)
    ]
    weight_loads = [
        pltpu.make_async_copy(source, target, load_sems.at[tp_count + 5 + i])
        for i, (source, target) in enumerate(
            ((gate_hbm, gate_w), (up_hbm, up_w), (down_hbm, down_w), (weight_hbm, out_w))
        )
    ]
    small_loads = [
        pltpu.make_async_copy(source, target, load_sems.at[tp_count + 9 + i])
        for i, (source, target) in enumerate(
            (
                (routes_hbm, routes_ref),
                (route_weights_hbm, route_weights_ref),
                (ffn_hbm, ffn_ref),
                (gain_hbm, gain_ref),
            )
        )
    ]
    for load in moe_loads + small_loads + mixer_loads + weight_loads:
        load.start()

    barrier = pltpu.get_barrier_semaphore()

    def signal(axis, to):
        pl.semaphore_signal(barrier, inc=1, device_id={axis: to}, device_id_type=MESH)

    for bit in bits:
        signal("tp", flip(tp, bit))
    for step in steps:
        pl.when(place + step < ep_count)(lambda: signal("ep", place + step))
        pl.when(place >= step)(lambda: signal("ep", place - step))
    peers = sum(
        jnp.where(place + step < ep_count, 1, 0) + jnp.where(place >= step, 1, 0)
        for step in steps
    )
    for load in moe_loads:
        load.wait()
    pl.semaphore_wait(barrier, peers + len(bits))

    dispatch = Dispatch(
        chips,
        tp_count,
        rows,
        info,
        extra,
        along_sems,
        along_info_sems,
        pair_sems,
        pair_info_sems,
        extra_sems,
    )
    order = chip_order(chip, chips)
    dispatch.send_own()

    squares = jnp.zeros((row_count, 1), F32)
    for t in range(tp_count):
        part = rows[place, t].astype(F32)
        squares += jnp.sum(part * part, axis=1, keepdims=True)
    scale = lax.rsqrt(squares / (tp_count * part_width) + 1.0)
    for load in small_loads:
        load.wait()
    names = lax.broadcasted_iota(jnp.int32, (expert_count, row_count), 0)
    portion = route_weights_ref[...]
    portion = portion / jnp.sum(portion, axis=0, keepdims=True)
    named = jnp.zeros((expert_count, row_count), F32)
    table = jnp.zeros((expert_count, row_count), F32)
    for choice in range(routes_ref.shape[0]):
        match = routes_ref[choice : choice + 1] == names
        named = jnp.where(match, 1.0, named)
        table = jnp.where(match, portion[choice : choice + 1], table)
    earlier = (
        lax.broadcasted_iota(jnp.int32, (row_count, row_count), 0)
        < lax.broadcasted_iota(jnp.int32, (row_count, row_count), 1)
    ).astype(BF16)
    info[place, :expert_count] = jnp.where(named > 0.0, dot(named, earlier), -1.0)
    info[place, expert_count : 2 * expert_count] = table
    info[place, 2 * expert_count :] = jnp.broadcast_to(scale, (row_count, row_count)).T[:8]
    dispatch.send_info()

    slot = lax.broadcasted_iota(jnp.int32, (cap, row_count), 0).astype(F32)

    def chosen(source):
        return info[source, pl.ds(place, 1), :] == slot

    def slot_value(pick, source, index):
        return jnp.sum(
            jnp.where(pick, info[source, pl.ds(index, 1), :], 0.0), axis=1, keepdims=True
        )

    sources = [chip] + order
    exchanges = [None] + [
        Exchange(tp_count, rows.at[2 * k + dispatch.core], row_sems, n, n == chips - 2)
        for n, k in enumerate(order)
    ]
    hidden_exchanges = [
        Exchange(tp_count, hidden.at[n], hidden_sems, n) for n in range(chips)
    ]

    def gate_up(n):
        k = sources[n]
        if n > 0:
            for delta in range(1, tp_count):
                exchanges[n].wait(delta)
        for t in range(tp_count):
            dispatch.from_partner(k, t).wait_recv()
        dispatch.across_info(k, True).wait_recv()
        for core in (0, 1):
            source = 2 * k + core
            pick = chosen(source)
            factor = slot_value(pick, source, 2 * expert_count)
            onehot = pick.astype(BF16)
            for t in range(tp_count):
                part = dot(onehot, rows[source, t]) * factor * ffn_ref[t]
                picked[core * cap : (core + 1) * cap, t * part_width : (t + 1) * part_width] = (
                    part.astype(BF16)
                )
        gate = dot(picked[...], gate_w[...])
        up = dot(picked[...], up_w[...])
        hidden[n, tp] = (jax.nn.silu(gate) * up).astype(BF16)
        hidden_exchanges[n].start()

    back = Back(ep_count, placed, moe_out, pair_in, held, from_left, from_right, back_sems)

    def down(n):
        k = sources[n]
        for delta in range(1, tp_count):
            hidden_exchanges[n].wait(delta)
        result = dot(
            jnp.concatenate([hidden[n, t] for t in range(tp_count)], axis=1), down_w[...]
        )
        for core in (0, 1):
            source = 2 * k + core
            pick = chosen(source)
            share = slot_value(pick, source, expert_count + place)
            mine = result[core * cap : (core + 1) * cap] * share
            placed[source] = dot_cols(pick.astype(BF16), mine).astype(BF16)
        for part in (0, 1):
            back.pair((k, part)).start()

    def landed(n):
        dispatch.landed(sources[n], exchanges[n])

    def relay(n):
        exchanges[n].relay()
        for delta in range(1, tp_count):
            if delta & (delta - 1) == 0:
                dispatch.shared(sources[n], exchanges[n], delta)

    def share_rest(n):
        for delta in range(1, tp_count):
            if delta & (delta - 1):
                dispatch.shared(sources[n], exchanges[n], delta)

    tokens = read.shape[0]
    blocks = tokens // BLOCK

    def relay_hidden(n):
        hidden_exchanges[n].relay()

    def tables(b):
        tables_block(b, mix_in, read, local_out, total, carry, b == blocks - 1)

    prefix = Prefix(ep_count, total, outgoing, incoming, before, prefix_sems)

    def wait_loads(loads):
        for load in loads:
            load.wait()

    remote = chips - 1
    last_step = len(steps) - 1

    def prefix_step(number):
        prefix.receive(number)
        if number < last_step:
            prefix.send(number + 1)

    def mixer_start():
        prefix.begin()
        prefix.send(0)

    def heads():
        columns = read.shape[1]
        groups, width = total.shape[1], total.shape[3]
        ones = head_ones(width)
        for group in range(groups):
            at = pl.ds(group * width, width)
            heads_out = dot(read[:, at], spread(before[1, group])) + local_out[:, at]
            center = heads_out - dot_right(heads_out, ones) / HD
            variance = dot_right(center * center, ones) / HD
            mixed[:, at] = (center * lax.rsqrt(variance + 1.0) * gain_ref[:, at]).astype(BF16)

    def project():
        weight_loads[3].wait()
        out_rows = tokens // tp_count
        tile = out_w.shape[1] // 4
        for number in range(4):
            at = pl.ds(number * tile, tile)
            part = dot(mixed[...], out_w[:, at]).astype(BF16)
            for t in range(tp_count):
                product[t, :, at] = part[t * out_rows : (t + 1) * out_rows]

    reduce = Reduce(tp_count, product, landing, reduce_sems)

    out_copies = [
        pltpu.make_async_copy(source, target, load_sems.at[tp_count + 13 + i])
        for i, (source, target) in enumerate(
            ((mixer_out, mixer_hbm_out), (moe_out, moe_hbm_out))
        )
    ]

    def reduce_step(number):
        last = number == len(bits) - 1
        reduce.land(number, mixer_out if last else None)
        if last:
            out_copies[0].start()
        else:
            reduce.start(number + 1)

    def collect():
        back.collect()
        out_copies[1].start()

    inner = (chip > 0) & (chip < chips - 1)

    def landed_inner(n):
        pl.when(inner)(lambda: landed(n))

    def landed_outer(n):
        pl.when(jnp.logical_not(inner))(lambda: landed(n))

    def finish_dispatch():
        dispatch.finish(order)
        for exchange in exchanges[1:]:
            exchange.finish()

    def finish_hidden():
        for exchange in hidden_exchanges:
            exchange.finish()
        prefix.finish()

    def take_second():
        dispatch.take_second(exchanges[remote])

    def second_inner():
        pl.when(inner)(take_second)

    def second_outer():
        pl.when(jnp.logical_not(inner))(take_second)

    more = [(tables, b) for b in range(blocks)]
    chain = [(prefix_step, number) for number in range(len(steps))]
    plan = [(wait_loads, mixer_loads), *more[:1], (landed, 1)]
    plan += [(landed_inner, 2)] * (remote > 1)
    plan += [(wait_loads, weight_loads[:2]), (gate_up, 0), *more[1:2]]
    plan += [(relay, 1), (dispatch.passing,)] if remote > 1 else []
    plan += [(landed_inner, 3)] * (remote > 2)
    plan += [(landed_outer, 2)] * (remote > 1)
    plan += more[2:3]
    plan += [(share_rest, 1), (gate_up, 1), (relay_hidden, 0)] if remote > 1 else []
    plan += [(second_inner,)] * (remote == 3)
    plan += [(landed_outer, 3)] * (remote > 2)
    plan += [*more[3:], (mixer_start,)]
    for n in range(2, remote):
        if n > 2:
            plan.append((landed, n + 1))
        plan += [(relay, n), (share_rest, n), *chain[:1], (gate_up, n), (relay_hidden, n - 1)]
        chain = chain[1:]
    plan += [(second_outer,) if remote == 3 else (take_second,)]
    plan += [*chain[:1], (relay, remote), *chain[1:], (heads,), (project,)]
    plan += [(relay_hidden, remote - 1), (share_rest, remote), (gate_up, remote)]
    plan += [(wait_loads, weight_loads[2:3]), (down, 0), (finish_dispatch,)]
    plan += [(down, n) for n in range(1, remote - 1)]
    plan += [(relay_hidden, remote), (reduce.start, 0)]
    plan += [(down, n) for n in range(max(1, remote - 1), remote + 1)]
    plan += [(back.run, {chips // 2: [(reduce_step, 0)]}), (finish_hidden,)]
    plan += [(reduce_step, number) for number in range(1, len(bits))]
    plan += [(collect,)]
    for step, (action, *given) in enumerate(plan):
        with jax.named_scope(f"{action.__name__}#{step}"):
            action(*given)

    reduce.finish()
    back.finish()
    for copy in out_copies:
        copy.wait()


def settle_kernel(*refs):
    sems = refs[-1]
    count = (len(refs) - 1) // 3
    takes, puts = [], []
    for i in range(count):
        held = refs[2 * count + i]
        takes.append(pltpu.make_async_copy(refs[i], held, sems.at[0, i]))
        puts.append(pltpu.make_async_copy(held, refs[count + i], sems.at[1, i]))
    for take in takes:
        take.start()
    for take, put in zip(takes, puts):
        take.wait()
        put.start()
    for put in puts:
        put.wait()


def settle(*arrays):
    hbm = pl.BlockSpec(memory_space=pltpu.HBM)
    return pl.pallas_call(
        settle_kernel,
        out_shape=[jax.ShapeDtypeStruct(a.shape, a.dtype) for a in arrays],
        in_specs=[hbm] * len(arrays),
        out_specs=[hbm] * len(arrays),
        scratch_shapes=[pltpu.VMEM(a.shape, a.dtype) for a in arrays]
        + [pltpu.SemaphoreType.DMA((2, len(arrays)))],
        compiler_params=pltpu.CompilerParams(vmem_limit_bytes=63 * 2**20),
        name="settle",
    )(*arrays)


def local(
    receptance,
    key_in,
    value_in,
    decay_in,
    rate_in,
    norm_gain,
    out_weight,
    moe_in,
    ffn_gain,
    routes,
    route_weights,
    gate_weight,
    up_weight,
    down_weight,
):
    tp_count, ep_count = lax.axis_size("tp"), lax.axis_size("ep")
    row_count, feature_count = moe_in.shape
    expert_count = gate_weight.shape[0] * ep_count
    cap = 5 * row_count * routes.shape[1] // (4 * expert_count)
    cap = -(-cap // 16) * 16
    chips = ep_count // 2
    part_width = feature_count // tp_count
    units, out_part = gate_weight.shape[2], down_weight.shape[2]
    tokens, columns = receptance.shape
    width = group_width(columns)
    groups = columns // width
    steps = ep_count.bit_length() - 1
    out_rows = tokens // tp_count
    dim = out_weight.shape[1]
    hbm = pl.BlockSpec(memory_space=pltpu.HBM)
    state = (2, groups, HD, width)
    dma = pltpu.SemaphoreType.DMA

    buffers = [
        pltpu.VMEM((out_rows, dim), BF16),
        pltpu.VMEM((row_count, out_part), BF16),
        pltpu.VMEM((1, columns), F32),
        pltpu.VMEM((tp_count, 1, part_width), F32),
        pltpu.VMEM((routes.shape[1], row_count), routes.dtype),
        pltpu.VMEM((routes.shape[1], row_count), F32),
        pltpu.VMEM((ep_count, tp_count, row_count, part_width), BF16),
        pltpu.VMEM((ep_count, 2 * expert_count + 8, row_count), F32),
        pltpu.VMEM((row_count, part_width), BF16),
        pltpu.VMEM((5, tokens, columns), BF16),
        pltpu.VMEM((feature_count, units), BF16),
        pltpu.VMEM((feature_count, units), BF16),
        pltpu.VMEM(down_weight.shape[1:], BF16),
        pltpu.VMEM(out_weight.shape, BF16),
        pltpu.VMEM((2 * cap, feature_count), BF16),
        pltpu.VMEM((chips, tp_count, 2 * cap, units), BF16),
        pltpu.VMEM((tokens, columns), BF16),
        pltpu.VMEM((tokens, columns), F32),
        pltpu.VMEM(state, F32),
        pltpu.VMEM(state, BF16),
        pltpu.VMEM((steps, *state), BF16),
        pltpu.VMEM((steps, *state), BF16),
        pltpu.VMEM(state, F32),
        pltpu.VMEM((tokens, columns), BF16),
        pltpu.VMEM((tp_count, out_rows, dim), BF16),
        pltpu.VMEM((tp_count, out_rows, dim), BF16),
        pltpu.VMEM((ep_count, row_count, out_part), BF16),
        pltpu.VMEM((chips, row_count, out_part), BF16),
        pltpu.VMEM((chips, row_count, out_part), BF16),
        pltpu.VMEM((chips, row_count, out_part), BF16),
        pltpu.VMEM((chips, row_count, out_part), BF16),
    ]
    sems = [
        dma((tp_count + 15,)),
        dma((3, chips, 2)),
        dma((3, chips)),
        dma((2, chips, tp_count)),
        dma((2, chips)),
        dma((2, 2, 2)),
        dma((chips - 1, 2, 2, tp_count)),
        dma((chips, 2, 2, tp_count)),
        dma((2, steps)),
        dma((2, 2, tp_count)),
        dma((3, 2, 2 * chips)),
    ]
    def kernel(r, k, v, d, a, *refs):
        layer_kernel(tp_count, ep_count, cap, expert_count, (r, k, v, d, a), *refs)

    results = pl.pallas_call(
        kernel,
        out_shape=[
            jax.ShapeDtypeStruct((out_rows, dim), BF16),
            jax.ShapeDtypeStruct((row_count, out_part), BF16),
        ],
        in_specs=[hbm] * 14,
        out_specs=[hbm, hbm],
        scratch_shapes=buffers + sems,
        compiler_params=pltpu.CompilerParams(
            collective_id=0, has_side_effects=True, vmem_limit_bytes=63 * 2**20
        ),
        name="layer",
    )(
        receptance,
        key_in,
        value_in,
        decay_in,
        rate_in,
        norm_gain[None],
        out_weight,
        moe_in,
        ffn_gain.reshape(tp_count, 1, part_width),
        routes.T,
        route_weights.T,
        gate_weight[0],
        up_weight[0],
        down_weight[0],
    )
    return settle(*results)


def solution(mesh):
    return jax.shard_map(
        local,
        mesh=mesh,
        in_specs=(
            P("ep", "tp"),
            P("ep", "tp"),
            P("ep", "tp"),
            P("ep", "tp"),
            P("ep", "tp"),
            P("tp"),
            P("tp", None),
            P("ep", None),
            P(),
            P("ep", None),
            P("ep", None),
            P("ep", None, "tp"),
            P("ep", None, "tp"),
            P("ep", None, "tp"),
        ),
        out_specs=(P(("ep", "tp"), None), P("ep", "tp")),
        check_vma=False,
    )
```

```python
import jax
import jax.numpy as jnp
from jax import lax
from jax.experimental import pallas as pl
from jax.experimental.pallas import tpu as pltpu
from jax.sharding import PartitionSpec as P

HD = 64
BLOCK = 64
F32 = jnp.float32
BF16 = jnp.bfloat16
MESH = pl.DeviceIdType.MESH


def dot(a, b):
    return jnp.dot(a.astype(BF16), b.astype(BF16), preferred_element_type=F32)


def dot_rows(a, b):
    return lax.dot_general(
        a.astype(BF16), b.astype(BF16), (((1,), (1,)), ((), ())), preferred_element_type=F32
    )


def dot_cols(a, b):
    return lax.dot_general(
        a.astype(BF16), b.astype(BF16), (((0,), (0,)), ((), ())), preferred_element_type=F32
    )


def halves(a):
    high = a.astype(BF16)
    return high, (a - high.astype(F32)).astype(BF16)


def dot_left(mask, b):
    high, low = halves(b)
    return dot(mask, high) + dot(mask, low)


def dot_right(a, mask):
    high, low = halves(a)
    return dot(high, mask) + dot(low, mask)


def lane_head(rows, width):
    return lax.broadcasted_iota(jnp.int32, (rows, width), 1) // HD


def spread(packed):
    rows, width = packed.shape
    packed = packed.astype(BF16)
    head = lane_head(rows, width)
    return jnp.concatenate(
        [jnp.where(head == i, packed, jnp.zeros_like(packed)) for i in range(width // HD)], axis=0
    )


def fold(square):
    width = square.shape[1]
    head = lane_head(HD, width)
    out = jnp.zeros((HD, width), F32)
    for i in range(width // HD):
        out = jnp.where(head == i, square[i * HD : (i + 1) * HD], out)
    return out


def head_ones(width):
    row = lax.broadcasted_iota(jnp.int32, (width, width), 0) // HD
    return (row == lane_head(width, width)).astype(BF16)


def group_width(columns):
    return HD * max(g for g in (4, 2, 1) if columns % (g * HD) == 0)


def tables_block(block, mix_in, read_ref, local_ref, total_ref, carry, last):
    columns = read_ref.shape[1]
    width = group_width(columns)
    row = lax.broadcasted_iota(jnp.int32, (BLOCK, width), 0)
    lane = lax.broadcasted_iota(jnp.int32, (BLOCK, width), 1) % HD
    strict = lane < row
    closed = lane <= row
    eye = (lane == row).astype(F32)
    tril = (
        lax.broadcasted_iota(jnp.int32, (BLOCK, BLOCK), 1)
        <= lax.broadcasted_iota(jnp.int32, (BLOCK, BLOCK), 0)
    ).astype(BF16)
    ones = head_ones(width)
    rows = pl.ds(block * BLOCK, BLOCK)
    for group in range(columns // width):
        at = pl.ds(group * width, width)
        readout = mix_in[0, rows, at].astype(F32)
        key = mix_in[1, rows, at].astype(F32)
        value = mix_in[2, rows, at]
        log_decay = jax.nn.sigmoid(mix_in[3, rows, at].astype(F32)) * -0.6065306597126334
        rate = jax.nn.sigmoid(mix_in[4, rows, at].astype(F32))
        unit = key * lax.rsqrt(dot_right(key * key, ones) + 1.0)
        inclusive = dot_left(tril, log_decay)
        total = inclusive[BLOCK - 1 :]
        probe = -unit * jnp.exp(inclusive - log_decay)
        removal = unit * rate
        written = key * rate
        back = jnp.exp(-inclusive)
        tail = jnp.exp(total - inclusive)
        readout = readout * jnp.exp(inclusive)
        left = jnp.concatenate([probe, readout], axis=0)
        on_removal = dot_rows(left, spread(removal * back))
        on_write = dot_rows(left, spread(written * back))
        lower = jnp.where(strict, on_removal[:BLOCK], 0.0)
        reach = jnp.where(closed, on_removal[BLOCK:], 0.0)
        lower_write = jnp.where(strict, on_write[:BLOCK], 0.0)
        reach_write = jnp.where(closed, on_write[BLOCK:], 0.0)
        value_wide = spread(value)
        on_value = dot(jnp.concatenate([lower_write, reach_write], axis=0), value_wide)
        inverse = eye + lower
        power = dot(lower, spread(lower))
        for doubling in range(BLOCK.bit_length() - 2):
            wide = spread(power)
            if doubling < BLOCK.bit_length() - 3:
                both = dot(jnp.concatenate([inverse, power], axis=0), wide)
                inverse = inverse + both[:BLOCK]
                power = both[BLOCK:]
            else:
                inverse = inverse + dot(inverse, wide)
        solved_probe = dot(inverse, spread(probe))
        solved_values = dot(inverse, spread(on_value[:BLOCK]))
        transition = eye * jnp.exp(total) + fold(dot_cols(removal * tail, solved_probe))
        increment = fold(
            dot_cols(
                jnp.concatenate([removal * tail, written * tail], axis=0),
                jnp.concatenate([solved_values.astype(BF16), value], axis=0),
            )
        )
        read_state = readout + dot(reach, spread(solved_probe))
        local_out = dot(reach, spread(solved_values)) + on_value[BLOCK:]
        if block == 0:
            new_map, new_add = transition, increment
            read_ref[rows, at] = read_state.astype(BF16)
            local_ref[rows, at] = local_out
        else:
            left = jnp.concatenate([read_state, transition], axis=0)
            on_map = dot(left, spread(carry[0, group]))
            on_add = dot(left, spread(carry[1, group]))
            read_ref[rows, at] = on_map[:BLOCK].astype(BF16)
            local_ref[rows, at] = on_add[:BLOCK] + local_out
            new_map, new_add = on_map[BLOCK:], on_add[BLOCK:] + increment
        if last:
            total_ref[0, group] = new_map.astype(BF16)
            total_ref[1, group] = new_add.astype(BF16)
        else:
            carry[0, group] = new_map
            carry[1, group] = new_add


def flip(me, bits):
    bit = 1
    while bit <= bits:
        if bits & bit:
            me = me + bit - 2 * bit * ((me // bit) % 2)
        bit *= 2
    return me


def bit_list(count):
    return [1 << b for b in range(count.bit_length() - 1)]


class Exchange:
    def __init__(self, count, slots, sems, unit, wide=False):
        me = lax.axis_index("tp")
        half = slots.shape[1] // 2
        bits = bit_list(count)
        self.count, self.copies, self.heads, self.relays, self.seen = count, {}, [], [], set()
        whole = slots.at[pl.ds(0, count - 2 if wide else count - 1)]
        self.sent = pltpu.make_async_remote_copy(
            src_ref=whole,
            dst_ref=whole,
            send_sem=sems.at[unit, 2 * (count - 1)],
            recv_sem=sems.at[unit, 0],
            device_id={"tp": flip(me, bits[0])},
            device_id_type=MESH,
        )
        self.seconds = []
        for number in range(1 if wide else 0, len(bits)):
            for stream, order in enumerate((bits, bits[::-1])):
                at = pl.ds(stream * half, half)
                known = [0]
                for bit in order[:number]:
                    known += [k ^ bit for k in known]
                for from_delta in known:
                    bit = order[number]
                    key = (stream, from_delta ^ bit)
                    owner = flip(me, from_delta)
                    self.copies[key] = pltpu.make_async_remote_copy(
                        src_ref=slots.at[owner, at],
                        dst_ref=slots.at[owner, at],
                        send_sem=sems.at[unit, 2 * (count - 1)],
                        recv_sem=sems.at[unit, stream * (count - 1) + key[1] - 1],
                        device_id={"tp": flip(me, bit)},
                        device_id_type=MESH,
                    )
                    if wide and from_delta == order[0]:
                        self.seconds.append(key)
                    elif from_delta:
                        self.relays.append((key, from_delta))
                    else:
                        self.heads.append(key)

    def start(self, streams=(0, 1)):
        for key in self.heads:
            if key[0] in streams:
                self.copies[key].start()

    def start_seconds(self):
        for key in self.seconds:
            self.copies[key].start()

    def arrive(self, stream, delta):
        if (stream, delta) in self.copies and (stream, delta) not in self.seen:
            self.seen.add((stream, delta))
            self.copies[stream, delta].wait_recv()

    def relay(self):
        for key, from_delta in self.relays:
            self.arrive(key[0], from_delta)
            self.copies[key].start()

    def wait(self, delta):
        for stream in (0, 1):
            self.arrive(stream, delta)

    def finish(self):
        self.sent.wait_send()


class Prefix:
    def __init__(self, count, own, outgoing, incoming, before, sems):
        self.me, self.count = lax.axis_index("ep"), count
        self.own, self.outgoing, self.incoming, self.before = own, outgoing, incoming, before
        self.steps = bit_list(count)
        self.copies = []
        for number, step in enumerate(self.steps):
            source = own if number == 0 else outgoing.at[number - 1]
            target = incoming.at[number]
            if number == len(self.steps) - 1:
                source, target = source.at[1], target.at[1]
            self.copies.append(
                pltpu.make_async_remote_copy(
                    src_ref=source,
                    dst_ref=target,
                    send_sem=sems.at[0, number],
                    recv_sem=sems.at[1, number],
                    device_id={"ep": lax.rem(self.me + step, count)},
                    device_id_type=MESH,
                )
            )

    def begin(self):
        groups, width = self.own.shape[1], self.own.shape[3]
        lane = lax.broadcasted_iota(jnp.int32, (HD, width), 1) % HD
        eye = (lane == lax.broadcasted_iota(jnp.int32, (HD, width), 0)).astype(F32)
        for group in range(groups):
            self.before[0, group] = eye
            self.before[1, group] = jnp.zeros_like(eye)

    def send(self, number):
        pl.when(self.me + self.steps[number] < self.count)(self.copies[number].start)

    def receive(self, number):
        last = number == len(self.steps) - 1
        groups = self.own.shape[1]
        own, before, incoming = self.own, self.before, self.incoming

        @pl.when(self.me >= self.steps[number])
        def _():
            self.copies[number].wait_recv()
            for group in range(groups):
                left = before[0, group]
                before[1, group] += dot(left, spread(incoming[number, 1, group]))
                if not last:
                    before[0, group] = dot(left, spread(incoming[number, 0, group]))

        if not last:
            for group in range(groups):
                left = own[0, group]
                self.outgoing[number, 0, group] = dot(left, spread(before[0, group])).astype(BF16)
                self.outgoing[number, 1, group] = (
                    dot(left, spread(before[1, group])) + own[1, group].astype(F32)
                ).astype(BF16)

    def finish(self):
        for step, copy in zip(self.steps, self.copies):
            pl.when(self.me + step < self.count)(copy.wait_send)


class Reduce:
    def __init__(self, count, parts, landing, sems):
        self.me = lax.axis_index("tp")
        self.parts, self.landing = parts, landing
        self.half = parts.shape[2] // 2
        bits = bit_list(count)
        orders = (bits, bits[::-1])
        self.stages, self.finals, self.copies = [], [], {}
        left = [list(range(count))] * 2
        for number in range(len(bits)):
            passed, finals = [], []
            for stream in (0, 1):
                bit = orders[stream][number]
                sent = [d for d in left[stream] if d & bit]
                left[stream] = [d for d in left[stream] if not d & bit]
                at = pl.ds(stream * self.half, self.half)
                for delta in sent:
                    owner = flip(self.me, delta)
                    self.copies[stream, delta] = pltpu.make_async_remote_copy(
                        src_ref=parts.at[owner, :, at],
                        dst_ref=landing.at[delta, :, at],
                        send_sem=sems.at[0, stream, delta - 1],
                        recv_sem=sems.at[1, stream, delta - 1],
                        device_id={"tp": flip(self.me, bit)},
                        device_id_type=MESH,
                    )
                    (finals if delta == bit else passed).append((stream, delta, bit))
            self.stages.append(passed)
            self.finals.append(finals)

    def start_passed(self, number):
        for stream, delta, _ in self.stages[number]:
            self.copies[stream, delta].start()

    def start_finals(self, number):
        for stream, delta, _ in self.finals[number]:
            self.copies[stream, delta].start()

    def land(self, number):
        for stream, delta, bit in self.stages[number]:
            at = pl.ds(stream * self.half, self.half)
            self.copies[stream, delta].wait_recv()
            mine = flip(self.me, delta ^ bit)
            total = self.parts[mine, :, at].astype(F32) + self.landing[delta, :, at].astype(F32)
            self.parts[mine, :, at] = total.astype(BF16)

    def last(self, out):
        for stream in (0, 1):
            at = pl.ds(stream * self.half, self.half)
            total = self.parts[self.me, :, at].astype(F32)
            for finals in self.finals:
                for owner, delta, _ in finals:
                    if owner == stream:
                        self.copies[stream, delta].wait_recv()
                        total += self.landing[delta, :, at].astype(F32)
            out[:, at] = total.astype(BF16)

    def finish(self):
        for copy in self.copies.values():
            copy.wait_send()


class Dispatch:
    def __init__(
        self, chips, tp_count, rows, info, extra, sems, info_sems, pair_sems, pair_info, extra_sems
    ):
        me = lax.axis_index("ep")
        self.tp = lax.axis_index("tp")
        self.tp_count = tp_count
        self.core, self.chip, self.chips = lax.rem(me, 2), me // 2, chips
        self.me, self.partner = me, me + 1 - 2 * self.core
        self.rows, self.info = rows, info
        self.sems, self.info_sems = sems, info_sems
        self.pair_sems, self.pair_info = pair_sems, pair_info
        self.half = rows.shape[2] // 2
        bits = bit_list(tp_count)
        self.seconds = [flip(self.tp, bits[0]), flip(self.tp, bits[-1])]
        self.extra, self.extra_sems = extra, extra_sems
        self.end = (self.chip == 0) | (self.chip == chips - 1)
        self.last = self.last_of(self.chip)
        self.passed = chips - 1 - self.last

    def last_of(self, chip):
        return jnp.where(chip >= self.chips // 2, 0, self.chips - 1)

    def second(self, k, half):
        return self.rows.at[
            2 * k + self.core, self.seconds[half], pl.ds(half * self.half, self.half)
        ]

    def through(self, half):
        return self.extra.at[pl.ds(half * self.half, self.half)]

    def move(self, source, target, sender, receiver, half, to):
        return pltpu.make_async_remote_copy(
            src_ref=source,
            dst_ref=target,
            send_sem=self.extra_sems.at[0, sender, half],
            recv_sem=self.extra_sems.at[1, receiver, half],
            device_id={"ep": 2 * jnp.clip(to, 0, self.chips - 1) + self.core},
            device_id_type=MESH,
        )

    def origin_moves(self):
        to = jnp.where(self.chip == 0, 1, self.chips - 2)
        for half in (0, 1):
            source = self.second(self.chip, half)
            if self.chips > 2:
                yield self.move(source, self.through(half), 0, 0, half, to)
            else:
                yield self.move(source, source, 0, 1, half, to)

    def away(self, k):
        return jnp.where(k == 0, self.chip + 1, self.chip - 1)

    def send_second(self):
        @pl.when(self.end)
        def _():
            for move in self.origin_moves():
                move.start()

    def pass_moves(self):
        to = self.away(self.passed)
        final = self.last_of(to) == self.passed
        for half in (0, 1):
            source = self.through(half)
            yield final, self.move(source, self.second(self.passed, half), 0, 1, half, to)
            if self.chips > 4:
                yield jnp.logical_not(final), self.move(source, source, 0, 0, half, to)

    def passing(self):
        if self.chips > 2:

            @pl.when(jnp.logical_not(self.end))
            def _():
                for half in (0, 1):
                    source = self.through(half)
                    self.move(source, source, 0, 0, half, self.chip).wait_recv()
                for wanted, move in self.pass_moves():
                    pl.when(wanted)(move.start)

    def last_moves(self):
        to = self.away(self.last)
        for half in (0, 1):
            source = self.second(self.last, half)
            yield (to >= 0) & (to < self.chips), self.move(source, source, 1, 1, half, to)

    def take_second(self, exchange):
        for half, (moving, move) in enumerate(self.last_moves()):
            move.wait_recv()
            pl.when(moving)(move.start)
        exchange.start_seconds()

    def finish_second(self):
        @pl.when(self.end)
        def _():
            for move in self.origin_moves():
                move.wait_send()

        if self.chips > 2:

            @pl.when(jnp.logical_not(self.end))
            def _():
                for wanted, move in self.pass_moves():
                    pl.when(wanted)(move.wait_send)

        for moving, move in self.last_moves():
            pl.when(moving)(move.wait_send)

    def remote(self, ref, send, recv, to):
        return pltpu.make_async_remote_copy(
            src_ref=ref,
            dst_ref=ref,
            send_sem=send,
            recv_sem=recv,
            device_id={"ep": to},
            device_id_type=MESH,
        )

    def along(self, k, half, way, to):
        to = jnp.clip(to, 0, self.chips - 1)
        ref = self.rows.at[2 * k + self.core, self.tp, pl.ds(half * self.half, self.half)]
        return self.remote(
            ref, self.sems.at[way, k, half], self.sems.at[2, k, half], 2 * to + self.core
        )

    def along_info(self, k, way, to):
        to = jnp.clip(to, 0, self.chips - 1)
        ref = self.info.at[2 * k + self.core]
        return self.remote(
            ref, self.info_sems.at[way, k], self.info_sems.at[2, k], 2 * to + self.core
        )

    def across(self, k, place):
        ref = self.rows.at[2 * k + self.core, place]
        return self.remote(ref, self.pair_sems.at[0, k], self.pair_sems.at[1, k], self.partner)

    def all_across(self, k, other=False):
        ref = self.rows.at[2 * k + (1 - self.core if other else self.core)]
        return self.remote(ref, self.pair_sems.at[0, k], self.pair_sems.at[1, k], self.partner)

    def across_info(self, k, other=False):
        core = 1 - self.core if other else self.core
        ref = self.info.at[2 * k + core]
        return self.remote(ref, self.pair_info.at[0, k], self.pair_info.at[1, k], self.partner)

    def sides(self):
        return (
            (self.chip + 1 < self.chips, 0, self.chip + 1),
            (self.chip > 0, 1, self.chip - 1),
        )

    def send_own(self):
        for half in (0, 1):
            for inside, way, to in self.sides():
                pl.when(inside)(self.along(self.chip, half, way, to).start)
        for place in range(self.tp_count):
            self.across(self.chip, place).start()

    def send_info(self):
        for inside, way, to in self.sides():
            pl.when(inside)(self.along_info(self.chip, way, to).start)
        self.across_info(self.chip).start()
        self.send_second()

    def onward(self, k):
        right = k < self.chip
        to = jnp.where(right, self.chip + 1, self.chip - 1)
        return (to >= 0) & (to < self.chips), jnp.where(right, 0, 1), to

    def landed(self, k, exchange):
        moving, way, to = self.onward(k)
        for half in (0, 1):
            self.along(k, half, way, to).wait_recv()
            pl.when(moving)(self.along(k, half, way, to).start)
            exchange.start((half,))
        self.across(k, self.tp).start()
        self.along_info(k, way, to).wait_recv()
        pl.when(moving)(self.along_info(k, way, to).start)
        self.across_info(k).start()

    def shared(self, k, exchange, delta):
        exchange.wait(delta)
        self.across(k, flip(self.tp, delta)).start()

    def finish(self, order):
        self.finish_second()
        for half in (0, 1):
            for inside, way, to in self.sides():
                pl.when(inside)(self.along(self.chip, half, way, to).wait_send)
        for inside, way, to in self.sides():
            pl.when(inside)(self.along_info(self.chip, way, to).wait_send)
        for k in order:
            moving, way, to = self.onward(k)
            for half in (0, 1):
                pl.when(moving)(self.along(k, half, way, to).wait_send)
            pl.when(moving)(self.along_info(k, way, to).wait_send)
        for k in [self.chip] + order:
            self.all_across(k).wait_send()
            self.across_info(k).wait_send()


def chip_order(chip, chips):
    table = [
        sorted((k for k in range(chips) if k != at), key=lambda k: (abs(k - at), abs(k - (0 if at < chips / 2 else chips - 1))))
        for at in range(chips)
    ]
    return [
        sum(jnp.where(chip == at, table[at][number], 0) for at in range(chips))
        for number in range(chips - 1)
    ]


class Back:
    def __init__(self, count, placed, out, pair_in, held, from_left, from_right, sems):
        me = lax.axis_index("ep")
        self.chips = count // 2
        self.core = lax.rem(me, 2)
        self.chip = me // 2
        self.partner = me + 1 - 2 * self.core
        self.half = out.shape[0] // 2
        self.right_to = jnp.minimum(me + 2, count - 2 + self.core)
        self.left_to = jnp.maximum(me - 2, self.core)
        self.placed, self.out, self.pair_in, self.held = placed, out, pair_in, held
        self.from_left, self.from_right, self.sems = from_left, from_right, sems

    def send(self, source, target, kind, item, to):
        at, part = item
        rows = pl.ds(part * self.half, self.half)
        return pltpu.make_async_remote_copy(
            src_ref=source.at[rows],
            dst_ref=target.at[at, rows],
            send_sem=self.sems.at[2 * self.chips + 2 * at + part],
            recv_sem=self.sems.at[2 * self.chips * (kind + 1) + 2 * at + part],
            device_id={"ep": to},
            device_id_type=MESH,
        )

    def pair(self, at):
        return pltpu.make_async_remote_copy(
            src_ref=self.placed.at[2 * at + 1 - self.core],
            dst_ref=self.pair_in.at[at],
            send_sem=self.sems.at[at],
            recv_sem=self.sems.at[self.chips + at],
            device_id={"ep": self.partner},
            device_id_type=MESH,
        )

    def right(self, item, source=None):
        source = self.from_left if source is None else source
        return self.send(source.at[item[0]], self.from_left, 1, item, self.right_to)

    def left(self, item, source=None):
        source = self.from_right if source is None else source
        return self.send(source.at[item[0]], self.from_right, 2, item, self.left_to)

    def pair_sum(self, at):
        self.pair(at).wait_recv()
        self.held[at] = (
            self.placed[2 * at + self.core].astype(F32) + self.pair_in[at].astype(F32)
        ).astype(BF16)

    def forward(self, item, moving, hop, landing):
        at, part = item
        rows = pl.ds(part * self.half, self.half)

        @pl.when(moving)
        def _():
            relay = hop(item)
            relay.wait_recv()
            landing[at, rows] = (
                landing[at, rows].astype(F32) + self.held[at, rows].astype(F32)
            ).astype(BF16)
            relay.start()

    def origin(self, at):
        self.pair_sum(at)
        for part in (0, 1):
            item = (at, part)
            pl.when(self.chip == 0)(self.right(item, self.held).start)
            pl.when(self.chip > 0)(self.left(item, self.held).start)

    def run(self):
        chips, chip = self.chips, self.chip
        order = [1, *range(chips - 1, 1, -1)]
        ready = set()

        def summed(at):
            if at not in ready:
                ready.add(at)
                self.pair_sum(at)

        def step(near, number):
            part = number % 2
            right_at = order[number // 2]
            left_at = chips - 1 - right_at

            def rightward():
                self.forward((right_at, part), right_at > chip, self.right, self.from_left)

            def leftward():
                self.forward((left_at, part), left_at < chip, self.left, self.from_right)

            first, second = (rightward, leftward) if near else (leftward, rightward)
            pl.when(chip < chips // 2)(first)
            pl.when(chip >= chips // 2)(second)

        lead = 2
        items = 2 * len(order)
        for number in range(items + lead):
            if number < items:
                summed(order[number // 2])
                summed(chips - 1 - order[number // 2])
                step(True, number)
            if number >= lead:
                step(False, number - lead)

    def collect(self):
        chip, at = self.chip, self.chip

        @pl.when((chip == 0) | (chip == self.chips - 1))
        def _():
            self.pair_sum(at)

        for part in (0, 1):
            rows = pl.ds(part * self.half, self.half)
            self.out[rows] = self.held[at, rows]
            for inside, hop, landing in (
                (chip > 0, self.right, self.from_left),
                (chip < self.chips - 1, self.left, self.from_right),
            ):

                @pl.when(inside)
                def _():
                    hop((at, part)).wait_recv()
                    self.out[rows] = (
                        self.out[rows].astype(F32) + landing[at, rows].astype(F32)
                    ).astype(BF16)

    def finish(self):
        for at in range(self.chips):
            self.pair(at).wait_send()
            for part in (0, 1):
                item = (at, part)
                pl.when(at > self.chip)(self.right(item).wait_send)
                pl.when(at < self.chip)(self.left(item).wait_send)


def layer_kernel(
    tp_count,
    ep_count,
    cap,
    expert_count,
    mixer_hbm,
    gain_hbm,
    weight_hbm,
    moe_hbm,
    ffn_hbm,
    routes_hbm,
    route_weights_hbm,
    gate_hbm,
    up_hbm,
    down_hbm,
    mixer_hbm_out,
    moe_hbm_out,
    mixer_out,
    moe_out,
    gain_ref,
    ffn_ref,
    routes_ref,
    route_weights_ref,
    rows,
    info,
    extra,
    mix_in,
    gate_w,
    up_w,
    down_w,
    out_w,
    picked,
    hidden,
    read,
    local_out,
    carry,
    total,
    outgoing,
    incoming,
    before,
    mixed,
    product,
    landing,
    placed,
    pair_in,
    held,
    from_left,
    from_right,
    load_sems,
    along_sems,
    along_info_sems,
    pair_sems,
    pair_info_sems,
    extra_sems,
    row_sems,
    hidden_sems,
    prefix_sems,
    reduce_sems,
    back_sems,
):
    tp = lax.axis_index("tp")
    place = lax.axis_index("ep")
    chips = ep_count // 2
    chip = place // 2
    steps, bits = bit_list(ep_count), bit_list(tp_count)
    row_count, part_width = rows.shape[2], rows.shape[3]
    units = gate_w.shape[1]
    moe_loads = [
        pltpu.make_async_copy(
            moe_hbm.at[:, pl.ds(t * part_width, part_width)], rows.at[place, t], load_sems.at[0]
        )
        for t in range(tp_count)
    ]
    mixer_loads = [
        pltpu.make_async_copy(source, mix_in.at[i], load_sems.at[1])
        for i, source in enumerate(mixer_hbm)
    ]
    weight_loads = [
        pltpu.make_async_copy(source, target, load_sems.at[2 + i])
        for i, (source, target) in enumerate(
            ((gate_hbm, gate_w), (up_hbm, up_w), (down_hbm, down_w), (weight_hbm, out_w))
        )
    ]
    small_loads = [
        pltpu.make_async_copy(source, target, load_sems.at[6 + i])
        for i, (source, target) in enumerate(
            (
                (routes_hbm, routes_ref),
                (route_weights_hbm, route_weights_ref),
                (ffn_hbm, ffn_ref),
                (gain_hbm, gain_ref),
            )
        )
    ]
    for load in moe_loads + small_loads + mixer_loads + weight_loads:
        load.start()

    barrier = pltpu.get_barrier_semaphore()

    def signal(axis, to):
        pl.semaphore_signal(barrier, inc=1, device_id={axis: to}, device_id_type=MESH)

    for bit in bits:
        signal("tp", flip(tp, bit))
    for step in steps:
        pl.when(place + step < ep_count)(lambda: signal("ep", place + step))
        pl.when(place >= step)(lambda: signal("ep", place - step))
    peers = sum(
        jnp.where(place + step < ep_count, 1, 0) + jnp.where(place >= step, 1, 0)
        for step in steps
    )
    pltpu.make_async_copy(rows.at[place], rows.at[place], load_sems.at[0]).wait()
    pl.semaphore_wait(barrier, peers + len(bits))

    dispatch = Dispatch(
        chips,
        tp_count,
        rows,
        info,
        extra,
        along_sems,
        along_info_sems,
        pair_sems,
        pair_info_sems,
        extra_sems,
    )
    order = chip_order(chip, chips)
    dispatch.send_own()

    squares = jnp.zeros((row_count, 1), F32)
    for t in range(tp_count):
        part = rows[place, t].astype(F32)
        squares += jnp.sum(part * part, axis=1, keepdims=True)
    scale = lax.rsqrt(squares / (tp_count * part_width) + 1.0)
    for load in small_loads:
        load.wait()
    names = lax.broadcasted_iota(jnp.int32, (expert_count, row_count), 0)
    portion = route_weights_ref[...]
    portion = portion / jnp.sum(portion, axis=0, keepdims=True)
    named = jnp.zeros((expert_count, row_count), F32)
    table = jnp.zeros((expert_count, row_count), F32)
    for choice in range(routes_ref.shape[0]):
        match = routes_ref[choice : choice + 1] == names
        named = jnp.where(match, 1.0, named)
        table = jnp.where(match, portion[choice : choice + 1], table)
    earlier = (
        lax.broadcasted_iota(jnp.int32, (row_count, row_count), 0)
        < lax.broadcasted_iota(jnp.int32, (row_count, row_count), 1)
    ).astype(BF16)
    info[place, :expert_count] = jnp.where(named > 0.0, dot(named, earlier), -1.0)
    info[place, expert_count : 2 * expert_count] = table
    info[place, 2 * expert_count :] = jnp.broadcast_to(scale, (row_count, row_count)).T[:8]
    dispatch.send_info()

    slot = lax.broadcasted_iota(jnp.int32, (cap, row_count), 0).astype(F32)

    def chosen(source):
        return info[source, pl.ds(place, 1), :] == slot

    def slot_value(pick, source, index):
        return jnp.sum(
            jnp.where(pick, info[source, pl.ds(index, 1), :], 0.0), axis=1, keepdims=True
        )

    sources = [chip] + order
    exchanges = [None] + [
        Exchange(tp_count, rows.at[2 * k + dispatch.core], row_sems, n, n == chips - 2)
        for n, k in enumerate(order)
    ]
    hidden_exchanges = [
        Exchange(tp_count, hidden.at[n], hidden_sems, n) for n in range(chips)
    ]

    def gate_up(n):
        k = sources[n]
        if n > 0:
            for delta in range(1, tp_count):
                exchanges[n].wait(delta)
        dispatch.all_across(k, True).wait_recv()
        dispatch.across_info(k, True).wait_recv()
        for core in (0, 1):
            source = 2 * k + core
            pick = chosen(source)
            factor = slot_value(pick, source, 2 * expert_count)
            onehot = pick.astype(BF16)
            for t in range(tp_count):
                part = dot(onehot, rows[source, t]) * factor * ffn_ref[t]
                picked[core * cap : (core + 1) * cap, t * part_width : (t + 1) * part_width] = (
                    part.astype(BF16)
                )
        gate = dot(picked[...], gate_w[...])
        up = dot(picked[...], up_w[...])
        hidden[n, tp] = (jax.nn.silu(gate) * up).astype(BF16)
        hidden_exchanges[n].start()

    back = Back(ep_count, placed, moe_out, pair_in, held, from_left, from_right, back_sems)

    def down(n):
        k = sources[n]
        for delta in range(1, tp_count):
            hidden_exchanges[n].wait(delta)
        result = dot(
            jnp.concatenate([hidden[n, t] for t in range(tp_count)], axis=1), down_w[...]
        )
        for core in (0, 1):
            source = 2 * k + core
            pick = chosen(source)
            share = slot_value(pick, source, expert_count + place)
            mine = result[core * cap : (core + 1) * cap] * share
            placed[source] = dot_cols(pick.astype(BF16), mine).astype(BF16)
        back.pair(k).start()

    def landed(n):
        dispatch.landed(sources[n], exchanges[n])

    def relay(n):
        exchanges[n].relay()
        for delta in range(1, tp_count):
            if delta & (delta - 1) == 0:
                dispatch.shared(sources[n], exchanges[n], delta)

    def share_rest(n):
        for delta in range(1, tp_count):
            if delta & (delta - 1):
                dispatch.shared(sources[n], exchanges[n], delta)

    tokens = read.shape[0]
    blocks = tokens // BLOCK

    def relay_hidden(n):
        hidden_exchanges[n].relay()

    def tables(b):
        tables_block(b, mix_in, read, local_out, total, carry, b == blocks - 1)

    prefix = Prefix(ep_count, total, outgoing, incoming, before, prefix_sems)

    def wait_loads(loads):
        for load in loads:
            load.wait()

    remote = chips - 1
    last_step = len(steps) - 1

    def prefix_step(number):
        prefix.receive(number)
        if number < last_step:
            prefix.send(number + 1)

    def mixer_start():
        prefix.begin()
        prefix.send(0)

    def heads():
        columns = read.shape[1]
        groups, width = total.shape[1], total.shape[3]
        ones = head_ones(width)
        for group in range(groups):
            at = pl.ds(group * width, width)
            heads_out = dot(read[:, at], spread(before[1, group])) + local_out[:, at]
            center = heads_out - dot_right(heads_out, ones) / HD
            variance = dot_right(center * center, ones) / HD
            mixed[:, at] = (center * lax.rsqrt(variance + 1.0) * gain_ref[:, at]).astype(BF16)

    def project():
        weight_loads[3].wait()
        out_rows = tokens // tp_count
        tile = out_w.shape[1] // 4
        for number in range(4):
            at = pl.ds(number * tile, tile)
            part = dot(mixed[...], out_w[:, at]).astype(BF16)
            for t in range(tp_count):
                product[t, :, at] = part[t * out_rows : (t + 1) * out_rows]

    reduce = Reduce(tp_count, product, landing, reduce_sems)

    out_copies = [
        pltpu.make_async_copy(source, target, load_sems.at[10 + i])
        for i, (source, target) in enumerate(
            ((mixer_out, mixer_hbm_out), (moe_out, moe_hbm_out))
        )
    ]

    def reduce_pass():
        for number in range(len(bits) - 1):
            reduce.land(number)
            reduce.start_passed(number + 1)
            reduce.start_finals(number + 1)

    def reduce_last():
        reduce.last(mixer_out)
        out_copies[0].start()

    def origin(n):
        pl.when(jnp.logical_not(inner))(lambda: back.origin(sources[n]))

    def run():
        pl.when(inner)(back.run)

    def relay_inner(n):
        seen = set(exchanges[n].seen)
        pl.when(inner)(lambda: relay(n))
        exchanges[n].seen = seen

    def relay_outer(n):
        pl.when(jnp.logical_not(inner))(lambda: relay(n))

    def collect():
        back.collect()
        out_copies[1].start()

    inner = (chip > 0) & (chip < chips - 1)

    def landed_inner(n):
        pl.when(inner)(lambda: landed(n))

    def landed_outer(n):
        pl.when(jnp.logical_not(inner))(lambda: landed(n))

    def finish_dispatch():
        dispatch.finish(order)
        for exchange in exchanges[1:]:
            exchange.finish()

    def finish_hidden():
        for exchange in hidden_exchanges:
            exchange.finish()
        prefix.finish()

    def take_second():
        dispatch.take_second(exchanges[remote])

    def second_inner():
        pl.when(inner)(take_second)

    def second_outer():
        pl.when(jnp.logical_not(inner))(take_second)

    more = [(tables, b) for b in range(blocks)]
    chain = [(prefix_step, number) for number in range(len(steps))]
    all_mixer = pltpu.make_async_copy(mix_in, mix_in, load_sems.at[1])
    plan = [(wait_loads, [all_mixer]), *more[:1], (landed, 1)]
    plan += [(landed_inner, 2)] * (remote > 1)
    plan += [(wait_loads, weight_loads[:2]), (gate_up, 0), *more[1:2]]
    plan += [(relay, 1), (dispatch.passing,)] if remote > 1 else []
    plan += [(landed_inner, 3)] * (remote > 2)
    plan += [(landed_outer, 2)] * (remote > 1)
    plan += more[2:3]
    plan += [(second_inner,)] * (remote == 3)
    plan += [(share_rest, 1)] if remote > 1 else []
    plan += [(relay_inner, 2)] if remote > 2 else []
    plan += [(gate_up, 1), (relay_hidden, 0)] if remote > 1 else []
    plan += [(landed_outer, 3)] * (remote > 2)
    plan += [*more[3:], (mixer_start,)]
    for n in range(2, remote):
        if n > 2:
            plan.append((landed, n + 1))
        plan.append((relay_outer if n == 2 else relay, n))
        plan += [(second_outer,)] * (remote == 3)
        plan += [(share_rest, n), *chain[:1], (gate_up, n), (relay_hidden, n - 1)]
        chain = chain[1:]
    plan += [(take_second,)] * (remote != 3)
    plan += [*chain[:1], (relay, remote), *chain[1:]]
    plan += [(share_rest, remote), (gate_up, remote), (relay_hidden, remote - 1), (heads,)]
    plan += [(wait_loads, weight_loads[2:3])]
    plan += [(down, 1)] if remote > 1 else []
    plan += [(project,)]
    plan += [(origin, 1)] if remote > 1 else []
    plan += [(relay_hidden, remote), (reduce.start_passed, 0), (reduce.start_finals, 0)]
    plan += [(finish_dispatch,)]
    plan += [(down, n) for n in range(2, remote)]
    plan += [(down, 0), (down, remote)]
    plan += [(origin, n) for n in [remote, *range(remote - 1, 1, -1)]]
    plan += [(reduce_pass,), (run,), (finish_hidden,), (reduce_last,), (collect,)]
    for step, (action, *given) in enumerate(plan):
        with jax.named_scope(f"{action.__name__}#{step}"):
            action(*given)

    reduce.finish()
    back.finish()
    for copy in out_copies:
        copy.wait()


def settle_kernel(*refs):
    sems = refs[-1]
    count = (len(refs) - 1) // 3
    takes, puts = [], []
    for i in range(count):
        held = refs[2 * count + i]
        takes.append(pltpu.make_async_copy(refs[i], held, sems.at[0, i]))
        puts.append(pltpu.make_async_copy(held, refs[count + i], sems.at[1, i]))
    for take in takes:
        take.start()
    for take, put in zip(takes, puts):
        take.wait()
        put.start()
    for put in puts:
        put.wait()


def settle(*arrays):
    hbm = pl.BlockSpec(memory_space=pltpu.HBM)
    return pl.pallas_call(
        settle_kernel,
        out_shape=[jax.ShapeDtypeStruct(a.shape, a.dtype) for a in arrays],
        in_specs=[hbm] * len(arrays),
        out_specs=[hbm] * len(arrays),
        scratch_shapes=[pltpu.VMEM(a.shape, a.dtype) for a in arrays]
        + [pltpu.SemaphoreType.DMA((2, len(arrays)))],
        compiler_params=pltpu.CompilerParams(vmem_limit_bytes=63 * 2**20),
        name="settle",
    )(*arrays)


def local(
    receptance,
    key_in,
    value_in,
    decay_in,
    rate_in,
    norm_gain,
    out_weight,
    moe_in,
    ffn_gain,
    routes,
    route_weights,
    gate_weight,
    up_weight,
    down_weight,
):
    tp_count, ep_count = lax.axis_size("tp"), lax.axis_size("ep")
    row_count, feature_count = moe_in.shape
    expert_count = gate_weight.shape[0] * ep_count
    cap = 5 * row_count * routes.shape[1] // (4 * expert_count)
    cap = -(-cap // 16) * 16
    chips = ep_count // 2
    part_width = feature_count // tp_count
    units, out_part = gate_weight.shape[2], down_weight.shape[2]
    tokens, columns = receptance.shape
    width = group_width(columns)
    groups = columns // width
    steps = ep_count.bit_length() - 1
    out_rows = tokens // tp_count
    dim = out_weight.shape[1]
    hbm = pl.BlockSpec(memory_space=pltpu.HBM)
    state = (2, groups, HD, width)
    dma = pltpu.SemaphoreType.DMA

    buffers = [
        pltpu.VMEM((out_rows, dim), BF16),
        pltpu.VMEM((row_count, out_part), BF16),
        pltpu.VMEM((1, columns), F32),
        pltpu.VMEM((tp_count, 1, part_width), F32),
        pltpu.VMEM((routes.shape[1], row_count), routes.dtype),
        pltpu.VMEM((routes.shape[1], row_count), F32),
        pltpu.VMEM((ep_count, tp_count, row_count, part_width), BF16),
        pltpu.VMEM((ep_count, 2 * expert_count + 8, row_count), F32),
        pltpu.VMEM((row_count, part_width), BF16),
        pltpu.VMEM((5, tokens, columns), BF16),
        pltpu.VMEM((feature_count, units), BF16),
        pltpu.VMEM((feature_count, units), BF16),
        pltpu.VMEM(down_weight.shape[1:], BF16),
        pltpu.VMEM(out_weight.shape, BF16),
        pltpu.VMEM((2 * cap, feature_count), BF16),
        pltpu.VMEM((chips, tp_count, 2 * cap, units), BF16),
        pltpu.VMEM((tokens, columns), BF16),
        pltpu.VMEM((tokens, columns), F32),
        pltpu.VMEM(state, F32),
        pltpu.VMEM(state, BF16),
        pltpu.VMEM((steps, *state), BF16),
        pltpu.VMEM((steps, *state), BF16),
        pltpu.VMEM(state, F32),
        pltpu.VMEM((tokens, columns), BF16),
        pltpu.VMEM((tp_count, out_rows, dim), BF16),
        pltpu.VMEM((tp_count, out_rows, dim), BF16),
        pltpu.VMEM((ep_count, row_count, out_part), BF16),
        pltpu.VMEM((chips, row_count, out_part), BF16),
        pltpu.VMEM((chips, row_count, out_part), BF16),
        pltpu.VMEM((chips, row_count, out_part), BF16),
        pltpu.VMEM((chips, row_count, out_part), BF16),
    ]
    sems = [
        dma((12,)),
        dma((3, chips, 2)),
        dma((3, chips)),
        dma((2, chips)),
        dma((2, chips)),
        dma((2, 2, 2)),
        dma((chips - 1, 2 * tp_count - 1)),
        dma((chips, 2 * tp_count - 1)),
        dma((2, steps)),
        dma((2, 2, tp_count - 1)),
        dma((8 * chips,)),
    ]
    def kernel(r, k, v, d, a, *refs):
        layer_kernel(tp_count, ep_count, cap, expert_count, (r, k, v, d, a), *refs)

    results = pl.pallas_call(
        kernel,
        out_shape=[
            jax.ShapeDtypeStruct((out_rows, dim), BF16),
            jax.ShapeDtypeStruct((row_count, out_part), BF16),
        ],
        in_specs=[hbm] * 14,
        out_specs=[hbm, hbm],
        scratch_shapes=buffers + sems,
        compiler_params=pltpu.CompilerParams(
            collective_id=0, has_side_effects=True, vmem_limit_bytes=63 * 2**20
        ),
        name="layer",
    )(
        receptance,
        key_in,
        value_in,
        decay_in,
        rate_in,
        norm_gain[None],
        out_weight,
        moe_in,
        ffn_gain.reshape(tp_count, 1, part_width),
        routes.T,
        route_weights.T,
        gate_weight[0],
        up_weight[0],
        down_weight[0],
    )
    return settle(*results)


def solution(mesh):
    return jax.shard_map(
        local,
        mesh=mesh,
        in_specs=(
            P("ep", "tp"),
            P("ep", "tp"),
            P("ep", "tp"),
            P("ep", "tp"),
            P("ep", "tp"),
            P("tp"),
            P("tp", None),
            P("ep", None),
            P(),
            P("ep", None),
            P("ep", None),
            P("ep", None, "tp"),
            P("ep", None, "tp"),
            P("ep", None, "tp"),
        ),
        out_specs=(P(("ep", "tp"), None), P("ep", "tp")),
        check_vma=False,
    )
```

```python
import itertools

import jax
import jax.numpy as jnp
from jax import lax
from jax.experimental import pallas as pl
from jax.experimental.pallas import tpu as pltpu
from jax.sharding import PartitionSpec as P

HD = 64
BLOCK = 64
F32 = jnp.float32
BF16 = jnp.bfloat16
MESH = pl.DeviceIdType.MESH


def dot(a, b):
    return jnp.dot(a.astype(BF16), b.astype(BF16), preferred_element_type=F32)


def dot_rows(a, b):
    return lax.dot_general(
        a.astype(BF16), b.astype(BF16), (((1,), (1,)), ((), ())), preferred_element_type=F32
    )


def dot_cols(a, b):
    return lax.dot_general(
        a.astype(BF16), b.astype(BF16), (((0,), (0,)), ((), ())), preferred_element_type=F32
    )


def halves(a):
    high = a.astype(BF16)
    return high, (a - high.astype(F32)).astype(BF16)


def dot_left(mask, b):
    high, low = halves(b)
    return dot(mask, high) + dot(mask, low)


def dot_right(a, mask):
    high, low = halves(a)
    return dot(high, mask) + dot(low, mask)


def lane_head(rows, width):
    return lax.broadcasted_iota(jnp.int32, (rows, width), 1) // HD


def spread(packed):
    rows, width = packed.shape
    packed = packed.astype(BF16)
    head = lane_head(rows, width)
    return jnp.concatenate(
        [jnp.where(head == i, packed, jnp.zeros_like(packed)) for i in range(width // HD)], axis=0
    )


def fold(square):
    width = square.shape[1]
    head = lane_head(HD, width)
    out = jnp.zeros((HD, width), F32)
    for i in range(width // HD):
        out = jnp.where(head == i, square[i * HD : (i + 1) * HD], out)
    return out


def head_ones(width):
    row = lax.broadcasted_iota(jnp.int32, (width, width), 0) // HD
    return (row == lane_head(width, width)).astype(BF16)


def group_width(columns):
    return HD * max(g for g in (4, 2, 1) if columns % (g * HD) == 0)


def tables_block(block, mix_in, read_ref, local_ref, total_ref, carry, last):
    columns = read_ref.shape[1]
    width = group_width(columns)
    row = lax.broadcasted_iota(jnp.int32, (BLOCK, width), 0)
    lane = lax.broadcasted_iota(jnp.int32, (BLOCK, width), 1) % HD
    strict = lane < row
    closed = lane <= row
    eye = (lane == row).astype(F32)
    tril = (
        lax.broadcasted_iota(jnp.int32, (BLOCK, BLOCK), 1)
        <= lax.broadcasted_iota(jnp.int32, (BLOCK, BLOCK), 0)
    ).astype(BF16)
    ones = head_ones(width)
    rows = pl.ds(block * BLOCK, BLOCK)
    for group in range(columns // width):
        at = pl.ds(group * width, width)
        readout = mix_in[0, rows, at].astype(F32)
        key = mix_in[1, rows, at].astype(F32)
        value = mix_in[2, rows, at]
        log_decay = jax.nn.sigmoid(mix_in[3, rows, at].astype(F32)) * -0.6065306597126334
        rate = jax.nn.sigmoid(mix_in[4, rows, at].astype(F32))
        unit = key * lax.rsqrt(dot_right(key * key, ones) + 1.0)
        inclusive = dot_left(tril, log_decay)
        total = inclusive[BLOCK - 1 :]
        probe = -unit * jnp.exp(inclusive - log_decay)
        removal = unit * rate
        written = key * rate
        back = jnp.exp(-inclusive)
        tail = jnp.exp(total - inclusive)
        readout = readout * jnp.exp(inclusive)
        left = jnp.concatenate([probe, readout], axis=0)
        on_removal = dot_rows(left, spread(removal * back))
        on_write = dot_rows(left, spread(written * back))
        lower = jnp.where(strict, on_removal[:BLOCK], 0.0)
        reach = jnp.where(closed, on_removal[BLOCK:], 0.0)
        lower_write = jnp.where(strict, on_write[:BLOCK], 0.0)
        reach_write = jnp.where(closed, on_write[BLOCK:], 0.0)
        value_wide = spread(value)
        on_value = dot(jnp.concatenate([lower_write, reach_write], axis=0), value_wide)
        inverse = eye + lower
        power = dot(lower, spread(lower))
        for doubling in range(BLOCK.bit_length() - 2):
            wide = spread(power)
            if doubling < BLOCK.bit_length() - 3:
                both = dot(jnp.concatenate([inverse, power], axis=0), wide)
                inverse = inverse + both[:BLOCK]
                power = both[BLOCK:]
            else:
                inverse = inverse + dot(inverse, wide)
        solved_probe = dot(inverse, spread(probe))
        solved_values = dot(inverse, spread(on_value[:BLOCK]))
        transition = eye * jnp.exp(total) + fold(dot_cols(removal * tail, solved_probe))
        increment = fold(
            dot_cols(
                jnp.concatenate([removal * tail, written * tail], axis=0),
                jnp.concatenate([solved_values.astype(BF16), value], axis=0),
            )
        )
        read_state = readout + dot(reach, spread(solved_probe))
        local_out = dot(reach, spread(solved_values)) + on_value[BLOCK:]
        if block == 0:
            new_map, new_add = transition, increment
            read_ref[rows, at] = read_state.astype(BF16)
            local_ref[rows, at] = local_out
        else:
            left = jnp.concatenate([read_state, transition], axis=0)
            on_map = dot(left, spread(carry[0, group]))
            on_add = dot(left, spread(carry[1, group]))
            read_ref[rows, at] = on_map[:BLOCK].astype(BF16)
            local_ref[rows, at] = on_add[:BLOCK] + local_out
            new_map, new_add = on_map[BLOCK:], on_add[BLOCK:] + increment
        if last:
            total_ref[0, group] = new_map.astype(BF16)
            total_ref[1, group] = new_add.astype(BF16)
        else:
            carry[0, group] = new_map
            carry[1, group] = new_add


def flip(me, bits):
    bit = 1
    while bit <= bits:
        if bits & bit:
            me = me + bit - 2 * bit * ((me // bit) % 2)
        bit *= 2
    return me


def bit_list(count):
    return [1 << b for b in range(count.bit_length() - 1)]


class Exchange:
    def __init__(self, count, slots, sems, unit, wide=False):
        me = lax.axis_index("tp")
        half = slots.shape[1] // 2
        bits = bit_list(count)
        self.count, self.copies, self.heads, self.relays, self.seen = count, {}, [], [], set()
        whole = slots.at[pl.ds(0, count - 2 if wide else count - 1)]
        self.sent = pltpu.make_async_remote_copy(
            src_ref=whole,
            dst_ref=whole,
            send_sem=sems.at[unit, 2 * (count - 1)],
            recv_sem=sems.at[unit, 0],
            device_id={"tp": flip(me, bits[0])},
            device_id_type=MESH,
        )
        self.seconds = []
        for number in range(1 if wide else 0, len(bits)):
            for stream, order in enumerate((bits, bits[::-1])):
                at = pl.ds(stream * half, half)
                known = [0]
                for bit in order[:number]:
                    known += [k ^ bit for k in known]
                for from_delta in known:
                    bit = order[number]
                    key = (stream, from_delta ^ bit)
                    owner = flip(me, from_delta)
                    self.copies[key] = pltpu.make_async_remote_copy(
                        src_ref=slots.at[owner, at],
                        dst_ref=slots.at[owner, at],
                        send_sem=sems.at[unit, 2 * (count - 1)],
                        recv_sem=sems.at[unit, stream * (count - 1) + key[1] - 1],
                        device_id={"tp": flip(me, bit)},
                        device_id_type=MESH,
                    )
                    if wide and from_delta == order[0]:
                        self.seconds.append(key)
                    elif from_delta:
                        self.relays.append((key, from_delta))
                    else:
                        self.heads.append(key)

    def start(self, streams=(0, 1)):
        for key in self.heads:
            if key[0] in streams:
                self.copies[key].start()

    def start_seconds(self):
        for key in self.seconds:
            self.copies[key].start()

    def arrive(self, stream, delta):
        if (stream, delta) in self.copies and (stream, delta) not in self.seen:
            self.seen.add((stream, delta))
            self.copies[stream, delta].wait_recv()

    def relay(self):
        for key, from_delta in self.relays:
            self.arrive(key[0], from_delta)
            self.copies[key].start()

    def wait(self, delta):
        for stream in (0, 1):
            self.arrive(stream, delta)

    def finish(self):
        self.sent.wait_send()


class Prefix:
    def __init__(self, count, own, outgoing, incoming, before, sems):
        self.me, self.count = lax.axis_index("ep"), count
        self.own, self.outgoing, self.incoming, self.before = own, outgoing, incoming, before
        self.steps = bit_list(count)
        self.copies = []
        for number, step in enumerate(self.steps):
            source = own if number == 0 else outgoing.at[number - 1]
            target = incoming.at[number]
            if number == len(self.steps) - 1:
                source, target = source.at[1], target.at[1]
            self.copies.append(
                pltpu.make_async_remote_copy(
                    src_ref=source,
                    dst_ref=target,
                    send_sem=sems.at[0, number],
                    recv_sem=sems.at[1, number],
                    device_id={"ep": lax.rem(self.me + step, count)},
                    device_id_type=MESH,
                )
            )

    def begin(self):
        groups, width = self.own.shape[1], self.own.shape[3]
        lane = lax.broadcasted_iota(jnp.int32, (HD, width), 1) % HD
        eye = (lane == lax.broadcasted_iota(jnp.int32, (HD, width), 0)).astype(F32)
        for group in range(groups):
            self.before[0, group] = eye
            self.before[1, group] = jnp.zeros_like(eye)

    def send(self, number):
        pl.when(self.me + self.steps[number] < self.count)(self.copies[number].start)

    def receive(self, number):
        last = number == len(self.steps) - 1
        groups = self.own.shape[1]
        own, before, incoming = self.own, self.before, self.incoming

        @pl.when(self.me >= self.steps[number])
        def _():
            self.copies[number].wait_recv()
            for group in range(groups):
                left = before[0, group]
                before[1, group] += dot(left, spread(incoming[number, 1, group]))
                if not last:
                    before[0, group] = dot(left, spread(incoming[number, 0, group]))

        if not last:
            for group in range(groups):
                left = own[0, group]
                self.outgoing[number, 0, group] = dot(left, spread(before[0, group])).astype(BF16)
                self.outgoing[number, 1, group] = (
                    dot(left, spread(before[1, group])) + own[1, group].astype(F32)
                ).astype(BF16)

    def finish(self):
        for step, copy in zip(self.steps, self.copies):
            pl.when(self.me + step < self.count)(copy.wait_send)


class Reduce:
    def __init__(self, count, parts, landing, sems):
        self.me = lax.axis_index("tp")
        self.parts, self.landing = parts, landing
        self.half = parts.shape[2] // 2
        bits = bit_list(count)
        orders = (bits, bits[::-1])
        self.stages, self.finals, self.copies = [], [], {}
        left = [list(range(count))] * 2
        for number in range(len(bits)):
            passed, finals = [], []
            for stream in (0, 1):
                bit = orders[stream][number]
                sent = [d for d in left[stream] if d & bit]
                left[stream] = [d for d in left[stream] if not d & bit]
                at = pl.ds(stream * self.half, self.half)
                for delta in sent:
                    owner = flip(self.me, delta)
                    self.copies[stream, delta] = pltpu.make_async_remote_copy(
                        src_ref=parts.at[owner, :, at],
                        dst_ref=landing.at[delta, :, at],
                        send_sem=sems.at[0, stream, delta - 1],
                        recv_sem=sems.at[1, stream, delta - 1],
                        device_id={"tp": flip(self.me, bit)},
                        device_id_type=MESH,
                    )
                    (finals if delta == bit else passed).append((stream, delta, bit))
            self.stages.append(passed)
            self.finals.append(finals)

    def start_passed(self, number):
        for stream, delta, _ in self.stages[number]:
            self.copies[stream, delta].start()

    def start_finals(self, number):
        for stream, delta, _ in self.finals[number]:
            self.copies[stream, delta].start()

    def land(self, number):
        for stream, delta, bit in self.stages[number]:
            at = pl.ds(stream * self.half, self.half)
            self.copies[stream, delta].wait_recv()
            mine = flip(self.me, delta ^ bit)
            total = self.parts[mine, :, at].astype(F32) + self.landing[delta, :, at].astype(F32)
            self.parts[mine, :, at] = total.astype(BF16)

    def last(self, out):
        for stream in (0, 1):
            at = pl.ds(stream * self.half, self.half)
            total = self.parts[self.me, :, at].astype(F32)
            for finals in self.finals:
                for owner, delta, _ in finals:
                    if owner == stream:
                        self.copies[stream, delta].wait_recv()
                        total += self.landing[delta, :, at].astype(F32)
            out[:, at] = total.astype(BF16)

    def finish(self):
        for copy in self.copies.values():
            copy.wait_send()


class Dispatch:
    def __init__(
        self, chips, tp_count, rows, info, extra, sems, info_sems, pair_sems, pair_info, extra_sems
    ):
        me = lax.axis_index("ep")
        self.tp = lax.axis_index("tp")
        self.tp_count = tp_count
        self.core, self.chip, self.chips = lax.rem(me, 2), me // 2, chips
        self.me, self.partner = me, me + 1 - 2 * self.core
        self.rows, self.info = rows, info
        self.sems, self.info_sems = sems, info_sems
        self.pair_sems, self.pair_info = pair_sems, pair_info
        self.half = rows.shape[2] // 2
        bits = bit_list(tp_count)
        self.seconds = [flip(self.tp, bits[0]), flip(self.tp, bits[-1])]
        self.extra, self.extra_sems = extra, extra_sems
        self.end = (self.chip == 0) | (self.chip == chips - 1)
        self.last = self.last_of(self.chip)
        self.passed = chips - 1 - self.last

    def last_of(self, chip):
        return jnp.where(chip >= self.chips // 2, 0, self.chips - 1)

    def second(self, k, half):
        return self.rows.at[
            2 * k + self.core, self.seconds[half], pl.ds(half * self.half, self.half)
        ]

    def through(self, half):
        return self.extra.at[pl.ds(half * self.half, self.half)]

    def move(self, source, target, sender, receiver, half, to):
        return pltpu.make_async_remote_copy(
            src_ref=source,
            dst_ref=target,
            send_sem=self.extra_sems.at[0, sender, half],
            recv_sem=self.extra_sems.at[1, receiver, half],
            device_id={"ep": 2 * jnp.clip(to, 0, self.chips - 1) + self.core},
            device_id_type=MESH,
        )

    def origin_moves(self):
        to = jnp.where(self.chip == 0, 1, self.chips - 2)
        for half in (0, 1):
            source = self.second(self.chip, half)
            if self.chips > 2:
                yield self.move(source, self.through(half), 0, 0, half, to)
            else:
                yield self.move(source, source, 0, 1, half, to)

    def away(self, k):
        return jnp.where(k == 0, self.chip + 1, self.chip - 1)

    def send_second(self):
        @pl.when(self.end)
        def _():
            for move in self.origin_moves():
                move.start()

    def pass_moves(self):
        to = self.away(self.passed)
        final = self.last_of(to) == self.passed
        for half in (0, 1):
            source = self.through(half)
            yield final, self.move(source, self.second(self.passed, half), 0, 1, half, to)
            if self.chips > 4:
                yield jnp.logical_not(final), self.move(source, source, 0, 0, half, to)

    def passing(self):
        if self.chips > 2:

            @pl.when(jnp.logical_not(self.end))
            def _():
                for half in (0, 1):
                    source = self.through(half)
                    self.move(source, source, 0, 0, half, self.chip).wait_recv()
                for wanted, move in self.pass_moves():
                    pl.when(wanted)(move.start)

    def last_moves(self):
        to = self.away(self.last)
        for half in (0, 1):
            source = self.second(self.last, half)
            yield (to >= 0) & (to < self.chips), self.move(source, source, 1, 1, half, to)

    def take_second(self, exchange):
        for half, (moving, move) in enumerate(self.last_moves()):
            move.wait_recv()
            pl.when(moving)(move.start)
        exchange.start_seconds()

    def finish_second(self):
        @pl.when(self.end)
        def _():
            for move in self.origin_moves():
                move.wait_send()

        if self.chips > 2:

            @pl.when(jnp.logical_not(self.end))
            def _():
                for wanted, move in self.pass_moves():
                    pl.when(wanted)(move.wait_send)

        for moving, move in self.last_moves():
            pl.when(moving)(move.wait_send)

    def remote(self, ref, send, recv, to):
        return pltpu.make_async_remote_copy(
            src_ref=ref,
            dst_ref=ref,
            send_sem=send,
            recv_sem=recv,
            device_id={"ep": to},
            device_id_type=MESH,
        )

    def along(self, k, half, way, to):
        to = jnp.clip(to, 0, self.chips - 1)
        ref = self.rows.at[2 * k + self.core, self.tp, pl.ds(half * self.half, self.half)]
        return self.remote(
            ref, self.sems.at[way, k, half], self.sems.at[2, k, half], 2 * to + self.core
        )

    def along_info(self, k, way, to):
        to = jnp.clip(to, 0, self.chips - 1)
        ref = self.info.at[2 * k + self.core]
        return self.remote(
            ref, self.info_sems.at[way, k], self.info_sems.at[2, k], 2 * to + self.core
        )

    def across(self, k, place):
        ref = self.rows.at[2 * k + self.core, place]
        return self.remote(ref, self.pair_sems.at[0, k], self.pair_sems.at[1, k], self.partner)

    def all_across(self, k, other=False):
        ref = self.rows.at[2 * k + (1 - self.core if other else self.core)]
        return self.remote(ref, self.pair_sems.at[0, k], self.pair_sems.at[1, k], self.partner)

    def across_info(self, k, other=False):
        core = 1 - self.core if other else self.core
        ref = self.info.at[2 * k + core]
        return self.remote(ref, self.pair_info.at[0, k], self.pair_info.at[1, k], self.partner)

    def sides(self):
        return (
            (self.chip + 1 < self.chips, 0, self.chip + 1),
            (self.chip > 0, 1, self.chip - 1),
        )

    def send_own(self):
        for half in (0, 1):
            for inside, way, to in self.sides():
                pl.when(inside)(self.along(self.chip, half, way, to).start)
        for place in range(self.tp_count):
            self.across(self.chip, place).start()

    def send_info(self):
        for inside, way, to in self.sides():
            pl.when(inside)(self.along_info(self.chip, way, to).start)
        self.across_info(self.chip).start()
        self.send_second()

    def onward(self, k):
        right = k < self.chip
        to = jnp.where(right, self.chip + 1, self.chip - 1)
        return (to >= 0) & (to < self.chips), jnp.where(right, 0, 1), to

    def landed(self, k, exchange):
        moving, way, to = self.onward(k)
        for half in (0, 1):
            self.along(k, half, way, to).wait_recv()
            pl.when(moving)(self.along(k, half, way, to).start)
            exchange.start((half,))
        self.across(k, self.tp).start()
        self.along_info(k, way, to).wait_recv()
        pl.when(moving)(self.along_info(k, way, to).start)
        self.across_info(k).start()

    def shared(self, k, exchange, delta):
        exchange.wait(delta)
        self.across(k, flip(self.tp, delta)).start()

    def finish(self, order):
        self.finish_second()
        for half in (0, 1):
            for inside, way, to in self.sides():
                pl.when(inside)(self.along(self.chip, half, way, to).wait_send)
        for inside, way, to in self.sides():
            pl.when(inside)(self.along_info(self.chip, way, to).wait_send)
        for k in order:
            moving, way, to = self.onward(k)
            for half in (0, 1):
                pl.when(moving)(self.along(k, half, way, to).wait_send)
            pl.when(moving)(self.along_info(k, way, to).wait_send)
        for k in [self.chip] + order:
            self.all_across(k).wait_send()
            self.across_info(k).wait_send()


def chip_order(chip, chips):
    table = [
        sorted((k for k in range(chips) if k != at), key=lambda k: (abs(k - at), abs(k - (0 if at < chips / 2 else chips - 1))))
        for at in range(chips)
    ]
    return [
        sum(jnp.where(chip == at, table[at][number], 0) for at in range(chips))
        for number in range(chips - 1)
    ]


class Back:
    def __init__(self, count, placed, out, pair_in, held, from_left, from_right, sems):
        me = lax.axis_index("ep")
        self.chips = count // 2
        self.core = lax.rem(me, 2)
        self.chip = me // 2
        self.partner = me + 1 - 2 * self.core
        self.parts = 4
        self.half = out.shape[0] // self.parts
        self.right_to = jnp.minimum(me + 2, count - 2 + self.core)
        self.left_to = jnp.maximum(me - 2, self.core)
        self.placed, self.out, self.pair_in, self.held = placed, out, pair_in, held
        self.from_left, self.from_right, self.sems = from_left, from_right, sems

    def send(self, source, target, kind, item, to):
        at, part = item
        rows = pl.ds(part * self.half, self.half)
        return pltpu.make_async_remote_copy(
            src_ref=source.at[rows],
            dst_ref=target.at[at, rows],
            send_sem=self.sems.at[2 * self.chips + self.parts * at + part],
            recv_sem=self.sems.at[self.chips * (2 + self.parts * kind) + self.parts * at + part],
            device_id={"ep": to},
            device_id_type=MESH,
        )

    def pair(self, at):
        return pltpu.make_async_remote_copy(
            src_ref=self.placed.at[2 * at + 1 - self.core],
            dst_ref=self.pair_in.at[at],
            send_sem=self.sems.at[at],
            recv_sem=self.sems.at[self.chips + at],
            device_id={"ep": self.partner},
            device_id_type=MESH,
        )

    def right(self, item, source=None):
        source = self.from_left if source is None else source
        return self.send(source.at[item[0]], self.from_left, 1, item, self.right_to)

    def left(self, item, source=None):
        source = self.from_right if source is None else source
        return self.send(source.at[item[0]], self.from_right, 2, item, self.left_to)

    def pair_sum(self, at):
        self.pair(at).wait_recv()
        self.held[at] = (
            self.placed[2 * at + self.core].astype(F32) + self.pair_in[at].astype(F32)
        ).astype(BF16)

    def forward(self, item, moving, hop, landing):
        at, part = item
        rows = pl.ds(part * self.half, self.half)

        @pl.when(moving)
        def _():
            relay = hop(item)
            relay.wait_recv()
            landing[at, rows] = (
                landing[at, rows].astype(F32) + self.held[at, rows].astype(F32)
            ).astype(BF16)
            relay.start()

    def origin(self, at):
        self.pair_sum(at)
        for part in range(self.parts):
            item = (at, part)
            pl.when(self.chip == 0)(self.right(item, self.held).start)
            pl.when(self.chip > 0)(self.left(item, self.held).start)

    def relays(self):
        chips, chip, parts = self.chips, self.chip, self.parts
        ready = set()

        def summed(at):
            if at not in ready:
                ready.add(at)
                self.pair_sum(at)

        def step(near, number):
            part = number % parts
            right_at = 1 + number // parts
            left_at = chips - 1 - right_at

            def rightward():
                self.forward((right_at, part), right_at > chip, self.right, self.from_left)

            def leftward():
                self.forward((left_at, part), left_at < chip, self.left, self.from_right)

            first, second = (rightward, leftward) if near else (leftward, rightward)
            pl.when(chip < chips // 2)(first)
            pl.when(chip >= chips // 2)(second)

        items = parts * (chips - 1)
        for number in range(items + parts):
            if number < items:
                summed(1 + number // parts)
                summed(chips - 2 - number // parts)
                step(True, number)
            if number >= parts:
                step(False, number - parts)
            yield

    def collect(self):
        chip, at = self.chip, self.chip

        @pl.when((chip == 0) | (chip == self.chips - 1))
        def _():
            self.pair_sum(at)

        for part in range(self.parts):
            rows = pl.ds(part * self.half, self.half)
            self.out[rows] = self.held[at, rows]
            for inside, hop, landing in (
                (chip > 0, self.right, self.from_left),
                (chip < self.chips - 1, self.left, self.from_right),
            ):

                @pl.when(inside)
                def _():
                    hop((at, part)).wait_recv()
                    self.out[rows] = (
                        self.out[rows].astype(F32) + landing[at, rows].astype(F32)
                    ).astype(BF16)

    def finish(self):
        for at in range(self.chips):
            self.pair(at).wait_send()
            for part in range(self.parts):
                item = (at, part)
                pl.when(at > self.chip)(self.right(item).wait_send)
                pl.when(at < self.chip)(self.left(item).wait_send)


def layer_kernel(
    tp_count,
    ep_count,
    cap,
    expert_count,
    mixer_hbm,
    gain_hbm,
    weight_hbm,
    moe_hbm,
    ffn_hbm,
    routes_hbm,
    route_weights_hbm,
    gate_hbm,
    up_hbm,
    down_hbm,
    mixer_hbm_out,
    moe_hbm_out,
    mixer_out,
    moe_out,
    gain_ref,
    ffn_ref,
    routes_ref,
    route_weights_ref,
    rows,
    info,
    extra,
    mix_in,
    gate_w,
    up_w,
    down_w,
    out_w,
    picked,
    hidden,
    read,
    local_out,
    carry,
    total,
    outgoing,
    incoming,
    before,
    mixed,
    product,
    landing,
    placed,
    pair_in,
    held,
    from_left,
    from_right,
    load_sems,
    along_sems,
    along_info_sems,
    pair_sems,
    pair_info_sems,
    extra_sems,
    row_sems,
    hidden_sems,
    prefix_sems,
    reduce_sems,
    back_sems,
):
    tp = lax.axis_index("tp")
    place = lax.axis_index("ep")
    chips = ep_count // 2
    chip = place // 2
    steps, bits = bit_list(ep_count), bit_list(tp_count)
    row_count, part_width = rows.shape[2], rows.shape[3]
    units = gate_w.shape[1]
    moe_loads = [
        pltpu.make_async_copy(
            moe_hbm.at[:, pl.ds(t * part_width, part_width)], rows.at[place, t], load_sems.at[0]
        )
        for t in range(tp_count)
    ]
    mixer_loads = [
        pltpu.make_async_copy(source, mix_in.at[i], load_sems.at[1])
        for i, source in enumerate(mixer_hbm)
    ]
    weight_loads = [
        pltpu.make_async_copy(source, target, load_sems.at[2 + i])
        for i, (source, target) in enumerate(
            ((gate_hbm, gate_w), (up_hbm, up_w), (down_hbm, down_w), (weight_hbm, out_w))
        )
    ]
    small_loads = [
        pltpu.make_async_copy(source, target, load_sems.at[6 + i])
        for i, (source, target) in enumerate(
            (
                (routes_hbm, routes_ref),
                (route_weights_hbm, route_weights_ref),
                (ffn_hbm, ffn_ref),
                (gain_hbm, gain_ref),
            )
        )
    ]
    for load in moe_loads + small_loads + mixer_loads + weight_loads:
        load.start()

    barrier = pltpu.get_barrier_semaphore()

    def signal(axis, to):
        pl.semaphore_signal(barrier, inc=1, device_id={axis: to}, device_id_type=MESH)

    for bit in bits:
        signal("tp", flip(tp, bit))
    for step in steps:
        pl.when(place + step < ep_count)(lambda: signal("ep", place + step))
        pl.when(place >= step)(lambda: signal("ep", place - step))
    peers = sum(
        jnp.where(place + step < ep_count, 1, 0) + jnp.where(place >= step, 1, 0)
        for step in steps
    )
    pltpu.make_async_copy(rows.at[place], rows.at[place], load_sems.at[0]).wait()
    pl.semaphore_wait(barrier, peers + len(bits))

    dispatch = Dispatch(
        chips,
        tp_count,
        rows,
        info,
        extra,
        along_sems,
        along_info_sems,
        pair_sems,
        pair_info_sems,
        extra_sems,
    )
    order = chip_order(chip, chips)
    dispatch.send_own()

    squares = jnp.zeros((row_count, 1), F32)
    for t in range(tp_count):
        part = rows[place, t].astype(F32)
        squares += jnp.sum(part * part, axis=1, keepdims=True)
    scale = lax.rsqrt(squares / (tp_count * part_width) + 1.0)
    for load in small_loads:
        load.wait()
    names = lax.broadcasted_iota(jnp.int32, (expert_count, row_count), 0)
    portion = route_weights_ref[...]
    portion = portion / jnp.sum(portion, axis=0, keepdims=True)
    named = jnp.zeros((expert_count, row_count), F32)
    table = jnp.zeros((expert_count, row_count), F32)
    for choice in range(routes_ref.shape[0]):
        match = routes_ref[choice : choice + 1] == names
        named = jnp.where(match, 1.0, named)
        table = jnp.where(match, portion[choice : choice + 1], table)
    earlier = (
        lax.broadcasted_iota(jnp.int32, (row_count, row_count), 0)
        < lax.broadcasted_iota(jnp.int32, (row_count, row_count), 1)
    ).astype(BF16)
    info[place, :expert_count] = jnp.where(named > 0.0, dot(named, earlier), -1.0)
    info[place, expert_count : 2 * expert_count] = table
    info[place, 2 * expert_count :] = jnp.broadcast_to(scale, (row_count, row_count)).T[:8]
    dispatch.send_info()

    slot = lax.broadcasted_iota(jnp.int32, (cap, row_count), 0).astype(F32)

    def chosen(source):
        return info[source, pl.ds(place, 1), :] == slot

    def slot_value(pick, source, index):
        return jnp.sum(
            jnp.where(pick, info[source, pl.ds(index, 1), :], 0.0), axis=1, keepdims=True
        )

    sources = [chip] + order
    exchanges = [None] + [
        Exchange(tp_count, rows.at[2 * k + dispatch.core], row_sems, n, n == chips - 2)
        for n, k in enumerate(order)
    ]
    hidden_exchanges = [
        Exchange(tp_count, hidden.at[n], hidden_sems, n) for n in range(chips)
    ]

    def gate_up(n):
        k = sources[n]
        if n > 0:
            for delta in range(1, tp_count):
                exchanges[n].wait(delta)
        dispatch.all_across(k, True).wait_recv()
        dispatch.across_info(k, True).wait_recv()
        for core in (0, 1):
            source = 2 * k + core
            pick = chosen(source)
            factor = slot_value(pick, source, 2 * expert_count)
            onehot = pick.astype(BF16)
            for t in range(tp_count):
                part = dot(onehot, rows[source, t]) * factor * ffn_ref[t]
                picked[core * cap : (core + 1) * cap, t * part_width : (t + 1) * part_width] = (
                    part.astype(BF16)
                )
        gate = dot(picked[...], gate_w[...])
        up = dot(picked[...], up_w[...])
        hidden[n, tp] = (jax.nn.silu(gate) * up).astype(BF16)
        hidden_exchanges[n].start()

    back = Back(ep_count, placed, moe_out, pair_in, held, from_left, from_right, back_sems)

    def down(n):
        k = sources[n]
        for delta in range(1, tp_count):
            hidden_exchanges[n].wait(delta)
        result = dot(
            jnp.concatenate([hidden[n, t] for t in range(tp_count)], axis=1), down_w[...]
        )
        for core in (0, 1):
            source = 2 * k + core
            pick = chosen(source)
            share = slot_value(pick, source, expert_count + place)
            mine = result[core * cap : (core + 1) * cap] * share
            placed[source] = dot_cols(pick.astype(BF16), mine).astype(BF16)
        back.pair(k).start()

    def landed(n):
        dispatch.landed(sources[n], exchanges[n])

    def relay(n):
        exchanges[n].relay()
        for delta in range(1, tp_count):
            if delta & (delta - 1) == 0:
                dispatch.shared(sources[n], exchanges[n], delta)

    def share_rest(n):
        for delta in range(1, tp_count):
            if delta & (delta - 1):
                dispatch.shared(sources[n], exchanges[n], delta)

    tokens = read.shape[0]
    blocks = tokens // BLOCK

    def relay_hidden(n):
        hidden_exchanges[n].relay()

    def tables(b):
        tables_block(b, mix_in, read, local_out, total, carry, b == blocks - 1)

    prefix = Prefix(ep_count, total, outgoing, incoming, before, prefix_sems)

    def wait_loads(loads):
        for load in loads:
            load.wait()

    remote = chips - 1
    last_step = len(steps) - 1

    def prefix_step(number):
        prefix.receive(number)
        if number < last_step:
            prefix.send(number + 1)

    def mixer_start():
        prefix.begin()
        prefix.send(0)

    def heads():
        columns = read.shape[1]
        groups, width = total.shape[1], total.shape[3]
        ones = head_ones(width)
        for group in range(groups):
            at = pl.ds(group * width, width)
            heads_out = dot(read[:, at], spread(before[1, group])) + local_out[:, at]
            center = heads_out - dot_right(heads_out, ones) / HD
            variance = dot_right(center * center, ones) / HD
            mixed[:, at] = (center * lax.rsqrt(variance + 1.0) * gain_ref[:, at]).astype(BF16)

    def project():
        weight_loads[3].wait()
        out_rows = tokens // tp_count
        tile = out_w.shape[1] // 4
        for number in range(4):
            at = pl.ds(number * tile, tile)
            part = dot(mixed[...], out_w[:, at]).astype(BF16)
            for t in range(tp_count):
                product[t, :, at] = part[t * out_rows : (t + 1) * out_rows]

    reduce = Reduce(tp_count, product, landing, reduce_sems)

    out_copies = [
        pltpu.make_async_copy(source, target, load_sems.at[10 + i])
        for i, (source, target) in enumerate(
            ((mixer_out, mixer_hbm_out), (moe_out, moe_hbm_out))
        )
    ]

    def reduce_pass():
        for number in range(len(bits) - 1):
            reduce.land(number)
            reduce.start_passed(number + 1)
            reduce.start_finals(number + 1)

    def reduce_last():
        reduce.last(mixer_out)
        out_copies[0].start()

    def origin(n):
        pl.when(jnp.logical_not(inner))(lambda: back.origin(sources[n]))

    relays = back.relays()

    def run(count):
        @pl.when(inner)
        def _():
            for _ in itertools.islice(relays, count):
                pass

    def relay_inner(n):
        seen = set(exchanges[n].seen)
        pl.when(inner)(lambda: relay(n))
        exchanges[n].seen = seen

    def relay_outer(n):
        pl.when(jnp.logical_not(inner))(lambda: relay(n))

    def collect():
        back.collect()
        out_copies[1].start()

    inner = (chip > 0) & (chip < chips - 1)

    def landed_inner(n):
        pl.when(inner)(lambda: landed(n))

    def landed_outer(n):
        pl.when(jnp.logical_not(inner))(lambda: landed(n))

    def finish_dispatch():
        dispatch.finish(order)
        for exchange in exchanges[1:]:
            exchange.finish()

    def finish_hidden():
        for exchange in hidden_exchanges:
            exchange.finish()
        prefix.finish()

    def take_second():
        dispatch.take_second(exchanges[remote])

    def second_inner():
        pl.when(inner)(take_second)

    def second_outer():
        pl.when(jnp.logical_not(inner))(take_second)

    more = [(tables, b) for b in range(blocks)]
    chain = [(prefix_step, number) for number in range(len(steps))]
    all_mixer = pltpu.make_async_copy(mix_in, mix_in, load_sems.at[1])
    plan = [(wait_loads, [all_mixer]), *more[:1], (landed, 1)]
    plan += [(landed_inner, 2)] * (remote > 1)
    plan += [(wait_loads, weight_loads[:2]), (gate_up, 0), *more[1:2]]
    plan += [(relay, 1), (dispatch.passing,)] if remote > 1 else []
    plan += [(landed_inner, 3)] * (remote > 2)
    plan += [(landed_outer, 2)] * (remote > 1)
    plan += more[2:3]
    plan += [(second_inner,)] * (remote == 3)
    plan += [(share_rest, 1)] if remote > 1 else []
    plan += [(relay_inner, 2)] if remote > 2 else []
    plan += [(gate_up, 1), (relay_hidden, 0)] if remote > 1 else []
    plan += [(landed_outer, 3), (relay_outer, 2)] if remote > 2 else []
    plan += [*more[3:], (mixer_start,)]
    plan += [(second_outer,)] * (remote == 3)
    for n in range(2, remote):
        if n > 2:
            plan += [(landed, n + 1), (relay, n)]
        plan += [(share_rest, n), *chain[:1], (relay_hidden, n - 1), (gate_up, n)]
        chain = chain[1:] if n == 2 else chain
    plan += [(take_second,)] * (remote != 3)
    plan += [(relay, remote), (share_rest, remote), (gate_up, remote)]
    plan += [(wait_loads, weight_loads[2:3])]
    plan += [(down, 1)] if remote > 2 else []
    plan += [*chain[:1], (relay_hidden, remote - 1)]
    plan += [(origin, 1)] if remote > 2 else []
    plan += [*chain[1:], (heads,), (relay_hidden, remote)]
    for n in range(2 if remote > 2 else 1, remote):
        plan += [(down, n), (project,), (origin, n)] if n == remote - 1 else [(down, n), (origin, n)]
    plan += [(reduce.start_passed, 0), (reduce.start_finals, 0), (finish_dispatch,)]
    plan += [(down, 0), (down, remote), (origin, remote)]
    plan += [(run, back.parts * (remote - 1)), (reduce_pass,), (run, None)]
    plan += [(finish_hidden,), (reduce_last,), (collect,)]
    for step, (action, *given) in enumerate(plan):
        with jax.named_scope(f"{action.__name__}#{step}"):
            action(*given)

    reduce.finish()
    back.finish()
    for copy in out_copies:
        copy.wait()


def settle_kernel(*refs):
    sems = refs[-1]
    count = (len(refs) - 1) // 3
    takes, puts = [], []
    for i in range(count):
        held = refs[2 * count + i]
        takes.append(pltpu.make_async_copy(refs[i], held, sems.at[0, i]))
        puts.append(pltpu.make_async_copy(held, refs[count + i], sems.at[1, i]))
    for take in takes:
        take.start()
    for take, put in zip(takes, puts):
        take.wait()
        put.start()
    for put in puts:
        put.wait()


def settle(*arrays):
    hbm = pl.BlockSpec(memory_space=pltpu.HBM)
    return pl.pallas_call(
        settle_kernel,
        out_shape=[jax.ShapeDtypeStruct(a.shape, a.dtype) for a in arrays],
        in_specs=[hbm] * len(arrays),
        out_specs=[hbm] * len(arrays),
        scratch_shapes=[pltpu.VMEM(a.shape, a.dtype) for a in arrays]
        + [pltpu.SemaphoreType.DMA((2, len(arrays)))],
        compiler_params=pltpu.CompilerParams(vmem_limit_bytes=63 * 2**20),
        name="settle",
    )(*arrays)


def local(
    receptance,
    key_in,
    value_in,
    decay_in,
    rate_in,
    norm_gain,
    out_weight,
    moe_in,
    ffn_gain,
    routes,
    route_weights,
    gate_weight,
    up_weight,
    down_weight,
):
    tp_count, ep_count = lax.axis_size("tp"), lax.axis_size("ep")
    row_count, feature_count = moe_in.shape
    expert_count = gate_weight.shape[0] * ep_count
    cap = 5 * row_count * routes.shape[1] // (4 * expert_count)
    cap = -(-cap // 16) * 16
    chips = ep_count // 2
    part_width = feature_count // tp_count
    units, out_part = gate_weight.shape[2], down_weight.shape[2]
    tokens, columns = receptance.shape
    width = group_width(columns)
    groups = columns // width
    steps = ep_count.bit_length() - 1
    out_rows = tokens // tp_count
    dim = out_weight.shape[1]
    hbm = pl.BlockSpec(memory_space=pltpu.HBM)
    state = (2, groups, HD, width)
    dma = pltpu.SemaphoreType.DMA

    buffers = [
        pltpu.VMEM((out_rows, dim), BF16),
        pltpu.VMEM((row_count, out_part), BF16),
        pltpu.VMEM((1, columns), F32),
        pltpu.VMEM((tp_count, 1, part_width), F32),
        pltpu.VMEM((routes.shape[1], row_count), routes.dtype),
        pltpu.VMEM((routes.shape[1], row_count), F32),
        pltpu.VMEM((ep_count, tp_count, row_count, part_width), BF16),
        pltpu.VMEM((ep_count, 2 * expert_count + 8, row_count), F32),
        pltpu.VMEM((row_count, part_width), BF16),
        pltpu.VMEM((5, tokens, columns), BF16),
        pltpu.VMEM((feature_count, units), BF16),
        pltpu.VMEM((feature_count, units), BF16),
        pltpu.VMEM(down_weight.shape[1:], BF16),
        pltpu.VMEM(out_weight.shape, BF16),
        pltpu.VMEM((2 * cap, feature_count), BF16),
        pltpu.VMEM((chips, tp_count, 2 * cap, units), BF16),
        pltpu.VMEM((tokens, columns), BF16),
        pltpu.VMEM((tokens, columns), F32),
        pltpu.VMEM(state, F32),
        pltpu.VMEM(state, BF16),
        pltpu.VMEM((steps, *state), BF16),
        pltpu.VMEM((steps, *state), BF16),
        pltpu.VMEM(state, F32),
        pltpu.VMEM((tokens, columns), BF16),
        pltpu.VMEM((tp_count, out_rows, dim), BF16),
        pltpu.VMEM((tp_count, out_rows, dim), BF16),
        pltpu.VMEM((ep_count, row_count, out_part), BF16),
        pltpu.VMEM((chips, row_count, out_part), BF16),
        pltpu.VMEM((chips, row_count, out_part), BF16),
        pltpu.VMEM((chips, row_count, out_part), BF16),
        pltpu.VMEM((chips, row_count, out_part), BF16),
    ]
    sems = [
        dma((12,)),
        dma((3, chips, 2)),
        dma((3, chips)),
        dma((2, chips)),
        dma((2, chips)),
        dma((2, 2, 2)),
        dma((chips - 1, 2 * tp_count - 1)),
        dma((chips, 2 * tp_count - 1)),
        dma((2, steps)),
        dma((2, 2, tp_count - 1)),
        dma((14 * chips,)),
    ]
    def kernel(r, k, v, d, a, *refs):
        layer_kernel(tp_count, ep_count, cap, expert_count, (r, k, v, d, a), *refs)

    results = pl.pallas_call(
        kernel,
        out_shape=[
            jax.ShapeDtypeStruct((out_rows, dim), BF16),
            jax.ShapeDtypeStruct((row_count, out_part), BF16),
        ],
        in_specs=[hbm] * 14,
        out_specs=[hbm, hbm],
        scratch_shapes=buffers + sems,
        compiler_params=pltpu.CompilerParams(
            collective_id=0, has_side_effects=True, vmem_limit_bytes=63 * 2**20
        ),
        name="layer",
    )(
        receptance,
        key_in,
        value_in,
        decay_in,
        rate_in,
        norm_gain[None],
        out_weight,
        moe_in,
        ffn_gain.reshape(tp_count, 1, part_width),
        routes.T,
        route_weights.T,
        gate_weight[0],
        up_weight[0],
        down_weight[0],
    )
    return settle(*results)


def solution(mesh):
    return jax.shard_map(
        local,
        mesh=mesh,
        in_specs=(
            P("ep", "tp"),
            P("ep", "tp"),
            P("ep", "tp"),
            P("ep", "tp"),
            P("ep", "tp"),
            P("tp"),
            P("tp", None),
            P("ep", None),
            P(),
            P("ep", None),
            P("ep", None),
            P("ep", None, "tp"),
            P("ep", None, "tp"),
            P("ep", None, "tp"),
        ),
        out_specs=(P(("ep", "tp"), None), P("ep", "tp")),
        check_vma=False,
    )
```

```python
import itertools

import jax
import jax.numpy as jnp
from jax import lax
from jax.experimental import pallas as pl
from jax.experimental.pallas import tpu as pltpu
from jax.sharding import PartitionSpec as P

HD = 64
BLOCK = 64
F32 = jnp.float32
BF16 = jnp.bfloat16
MESH = pl.DeviceIdType.MESH


def dot(a, b):
    return jnp.dot(a.astype(BF16), b.astype(BF16), preferred_element_type=F32)


def dot_rows(a, b):
    return lax.dot_general(
        a.astype(BF16), b.astype(BF16), (((1,), (1,)), ((), ())), preferred_element_type=F32
    )


def dot_cols(a, b):
    return lax.dot_general(
        a.astype(BF16), b.astype(BF16), (((0,), (0,)), ((), ())), preferred_element_type=F32
    )


def halves(a):
    high = a.astype(BF16)
    return high, (a - high.astype(F32)).astype(BF16)


def dot_left(mask, b):
    high, low = halves(b)
    return dot(mask, high) + dot(mask, low)


def dot_right(a, mask):
    high, low = halves(a)
    return dot(high, mask) + dot(low, mask)


def lane_head(rows, width):
    return lax.broadcasted_iota(jnp.int32, (rows, width), 1) // HD


def spread(packed):
    rows, width = packed.shape
    packed = packed.astype(BF16)
    head = lane_head(rows, width)
    return jnp.concatenate(
        [jnp.where(head == i, packed, jnp.zeros_like(packed)) for i in range(width // HD)], axis=0
    )


def fold(square):
    width = square.shape[1]
    head = lane_head(HD, width)
    out = jnp.zeros((HD, width), F32)
    for i in range(width // HD):
        out = jnp.where(head == i, square[i * HD : (i + 1) * HD], out)
    return out


def head_ones(width):
    row = lax.broadcasted_iota(jnp.int32, (width, width), 0) // HD
    return (row == lane_head(width, width)).astype(BF16)


def group_width(columns):
    return HD * max(g for g in (4, 2, 1) if columns % (g * HD) == 0)


def tables_block(block, mix_in, read_ref, local_ref, total_ref, carry, last):
    columns = read_ref.shape[1]
    width = group_width(columns)
    row = lax.broadcasted_iota(jnp.int32, (BLOCK, width), 0)
    lane = lax.broadcasted_iota(jnp.int32, (BLOCK, width), 1) % HD
    strict = lane < row
    closed = lane <= row
    eye = (lane == row).astype(F32)
    tril = (
        lax.broadcasted_iota(jnp.int32, (BLOCK, BLOCK), 1)
        <= lax.broadcasted_iota(jnp.int32, (BLOCK, BLOCK), 0)
    ).astype(BF16)
    ones = head_ones(width)
    rows = pl.ds(block * BLOCK, BLOCK)
    for group in range(columns // width):
        at = pl.ds(group * width, width)
        readout = mix_in[0, rows, at].astype(F32)
        key = mix_in[1, rows, at].astype(F32)
        value = mix_in[2, rows, at]
        log_decay = jax.nn.sigmoid(mix_in[3, rows, at].astype(F32)) * -0.6065306597126334
        rate = jax.nn.sigmoid(mix_in[4, rows, at].astype(F32))
        unit = key * lax.rsqrt(dot_right(key * key, ones) + 1.0)
        inclusive = dot_left(tril, log_decay)
        total = inclusive[BLOCK - 1 :]
        probe = -unit * jnp.exp(inclusive - log_decay)
        removal = unit * rate
        written = key * rate
        back = jnp.exp(-inclusive)
        tail = jnp.exp(total - inclusive)
        readout = readout * jnp.exp(inclusive)
        left = jnp.concatenate([probe, readout], axis=0)
        on_removal = dot_rows(left, spread(removal * back))
        on_write = dot_rows(left, spread(written * back))
        lower = jnp.where(strict, on_removal[:BLOCK], 0.0)
        reach = jnp.where(closed, on_removal[BLOCK:], 0.0)
        lower_write = jnp.where(strict, on_write[:BLOCK], 0.0)
        reach_write = jnp.where(closed, on_write[BLOCK:], 0.0)
        value_wide = spread(value)
        on_value = dot(jnp.concatenate([lower_write, reach_write], axis=0), value_wide)
        inverse = eye + lower
        power = dot(lower, spread(lower))
        for doubling in range(BLOCK.bit_length() - 2):
            wide = spread(power)
            if doubling < BLOCK.bit_length() - 3:
                both = dot(jnp.concatenate([inverse, power], axis=0), wide)
                inverse = inverse + both[:BLOCK]
                power = both[BLOCK:]
            else:
                inverse = inverse + dot(inverse, wide)
        solved_probe = dot(inverse, spread(probe))
        solved_values = dot(inverse, spread(on_value[:BLOCK]))
        transition = eye * jnp.exp(total) + fold(dot_cols(removal * tail, solved_probe))
        increment = fold(
            dot_cols(
                jnp.concatenate([removal * tail, written * tail], axis=0),
                jnp.concatenate([solved_values.astype(BF16), value], axis=0),
            )
        )
        read_state = readout + dot(reach, spread(solved_probe))
        local_out = dot(reach, spread(solved_values)) + on_value[BLOCK:]
        if block == 0:
            new_map, new_add = transition, increment
            read_ref[rows, at] = read_state.astype(BF16)
            local_ref[rows, at] = local_out
        else:
            left = jnp.concatenate([read_state, transition], axis=0)
            on_map = dot(left, spread(carry[0, group]))
            on_add = dot(left, spread(carry[1, group]))
            read_ref[rows, at] = on_map[:BLOCK].astype(BF16)
            local_ref[rows, at] = on_add[:BLOCK] + local_out
            new_map, new_add = on_map[BLOCK:], on_add[BLOCK:] + increment
        if last:
            total_ref[0, group] = new_map.astype(BF16)
            total_ref[1, group] = new_add.astype(BF16)
        else:
            carry[0, group] = new_map
            carry[1, group] = new_add


def flip(me, bits):
    bit = 1
    while bit <= bits:
        if bits & bit:
            me = me + bit - 2 * bit * ((me // bit) % 2)
        bit *= 2
    return me


def bit_list(count):
    return [1 << b for b in range(count.bit_length() - 1)]


class Exchange:
    def __init__(self, count, slots, sems, unit, wide=False):
        me = lax.axis_index("tp")
        half = slots.shape[1] // 2
        bits = bit_list(count)
        self.count, self.copies, self.heads, self.relays, self.seen = count, {}, [], [], set()
        whole = slots.at[pl.ds(0, count - 2 if wide else count - 1)]
        self.sent = pltpu.make_async_remote_copy(
            src_ref=whole,
            dst_ref=whole,
            send_sem=sems.at[unit, 2 * (count - 1)],
            recv_sem=sems.at[unit, 0],
            device_id={"tp": flip(me, bits[0])},
            device_id_type=MESH,
        )
        self.seconds = []
        for number in range(1 if wide else 0, len(bits)):
            for stream, order in enumerate((bits, bits[::-1])):
                at = pl.ds(stream * half, half)
                known = [0]
                for bit in order[:number]:
                    known += [k ^ bit for k in known]
                for from_delta in known:
                    bit = order[number]
                    key = (stream, from_delta ^ bit)
                    owner = flip(me, from_delta)
                    self.copies[key] = pltpu.make_async_remote_copy(
                        src_ref=slots.at[owner, at],
                        dst_ref=slots.at[owner, at],
                        send_sem=sems.at[unit, 2 * (count - 1)],
                        recv_sem=sems.at[unit, stream * (count - 1) + key[1] - 1],
                        device_id={"tp": flip(me, bit)},
                        device_id_type=MESH,
                    )
                    if wide and from_delta == order[0]:
                        self.seconds.append(key)
                    elif from_delta:
                        self.relays.append((key, from_delta))
                    else:
                        self.heads.append(key)

    def start(self, streams=(0, 1)):
        for key in self.heads:
            if key[0] in streams:
                self.copies[key].start()

    def start_seconds(self):
        for key in self.seconds:
            self.copies[key].start()

    def arrive(self, stream, delta):
        if (stream, delta) in self.copies and (stream, delta) not in self.seen:
            self.seen.add((stream, delta))
            self.copies[stream, delta].wait_recv()

    def relay(self):
        for key, from_delta in self.relays:
            self.arrive(key[0], from_delta)
            self.copies[key].start()

    def wait(self, delta):
        for stream in (0, 1):
            self.arrive(stream, delta)

    def finish(self):
        self.sent.wait_send()


class Prefix:
    def __init__(self, count, own, outgoing, incoming, before, sems):
        self.me, self.count = lax.axis_index("ep"), count
        self.own, self.outgoing, self.incoming, self.before = own, outgoing, incoming, before
        self.steps = bit_list(count)
        self.copies = []
        for number, step in enumerate(self.steps):
            source = own if number == 0 else outgoing.at[number - 1]
            target = incoming.at[number]
            if number == len(self.steps) - 1:
                source, target = source.at[1], target.at[1]
            self.copies.append(
                pltpu.make_async_remote_copy(
                    src_ref=source,
                    dst_ref=target,
                    send_sem=sems.at[0, number],
                    recv_sem=sems.at[1, number],
                    device_id={"ep": lax.rem(self.me + step, count)},
                    device_id_type=MESH,
                )
            )

    def begin(self):
        groups, width = self.own.shape[1], self.own.shape[3]
        lane = lax.broadcasted_iota(jnp.int32, (HD, width), 1) % HD
        eye = (lane == lax.broadcasted_iota(jnp.int32, (HD, width), 0)).astype(F32)
        for group in range(groups):
            self.before[0, group] = eye
            self.before[1, group] = jnp.zeros_like(eye)

    def send(self, number):
        pl.when(self.me + self.steps[number] < self.count)(self.copies[number].start)

    def receive(self, number):
        last = number == len(self.steps) - 1
        groups = self.own.shape[1]
        own, before, incoming = self.own, self.before, self.incoming

        @pl.when(self.me >= self.steps[number])
        def _():
            self.copies[number].wait_recv()
            for group in range(groups):
                left = before[0, group]
                before[1, group] += dot(left, spread(incoming[number, 1, group]))
                if not last:
                    before[0, group] = dot(left, spread(incoming[number, 0, group]))

        if not last:
            for group in range(groups):
                left = own[0, group]
                self.outgoing[number, 0, group] = dot(left, spread(before[0, group])).astype(BF16)
                self.outgoing[number, 1, group] = (
                    dot(left, spread(before[1, group])) + own[1, group].astype(F32)
                ).astype(BF16)

    def finish(self):
        for step, copy in zip(self.steps, self.copies):
            pl.when(self.me + step < self.count)(copy.wait_send)


class Reduce:
    def __init__(self, count, parts, landing, sems):
        self.me = lax.axis_index("tp")
        self.parts, self.landing = parts, landing
        self.half = parts.shape[2] // 2
        bits = bit_list(count)
        whole = landing.at[pl.ds(0, count - 1)]
        self.sent = pltpu.make_async_remote_copy(
            src_ref=whole,
            dst_ref=whole,
            send_sem=sems.at[2 * (count - 1)],
            recv_sem=sems.at[0],
            device_id={"tp": flip(self.me, bits[0])},
            device_id_type=MESH,
        )
        orders = (bits, bits[::-1])
        self.stages, self.finals, self.copies = [], [], {}
        left = [list(range(count))] * 2
        for number in range(len(bits)):
            passed, finals = [], []
            for stream in (0, 1):
                bit = orders[stream][number]
                sent = [d for d in left[stream] if d & bit]
                left[stream] = [d for d in left[stream] if not d & bit]
                at = pl.ds(stream * self.half, self.half)
                for delta in sent:
                    owner = flip(self.me, delta)
                    self.copies[stream, delta] = pltpu.make_async_remote_copy(
                        src_ref=parts.at[owner, :, at],
                        dst_ref=landing.at[delta, :, at],
                        send_sem=sems.at[2 * (count - 1)],
                        recv_sem=sems.at[stream * (count - 1) + delta - 1],
                        device_id={"tp": flip(self.me, bit)},
                        device_id_type=MESH,
                    )
                    (finals if delta == bit else passed).append((stream, delta, bit))
            self.stages.append(passed)
            self.finals.append(finals)

    def start_passed(self, number):
        for stream, delta, _ in self.stages[number]:
            self.copies[stream, delta].start()

    def start_finals(self, number):
        for stream, delta, _ in self.finals[number]:
            self.copies[stream, delta].start()

    def land(self, number):
        for stream, delta, bit in self.stages[number]:
            at = pl.ds(stream * self.half, self.half)
            self.copies[stream, delta].wait_recv()
            mine = flip(self.me, delta ^ bit)
            total = self.parts[mine, :, at].astype(F32) + self.landing[delta, :, at].astype(F32)
            self.parts[mine, :, at] = total.astype(BF16)

    def last(self, out):
        for stream in (0, 1):
            at = pl.ds(stream * self.half, self.half)
            total = self.parts[self.me, :, at].astype(F32)
            for finals in self.finals:
                for owner, delta, _ in finals:
                    if owner == stream:
                        self.copies[stream, delta].wait_recv()
                        total += self.landing[delta, :, at].astype(F32)
            out[:, at] = total.astype(BF16)

    def finish(self):
        self.sent.wait_send()


class Dispatch:
    def __init__(
        self, chips, tp_count, rows, info, extra, sems, info_sems, pair_sems, pair_info, extra_sems
    ):
        me = lax.axis_index("ep")
        self.tp = lax.axis_index("tp")
        self.tp_count = tp_count
        self.core, self.chip, self.chips = lax.rem(me, 2), me // 2, chips
        self.me, self.partner = me, me + 1 - 2 * self.core
        self.rows, self.info = rows, info
        self.sems, self.info_sems = sems, info_sems
        self.pair_sems, self.pair_info = pair_sems, pair_info
        self.half = rows.shape[2] // 2
        bits = bit_list(tp_count)
        self.seconds = [flip(self.tp, bits[0]), flip(self.tp, bits[-1])]
        self.extra, self.extra_sems = extra, extra_sems
        self.end = (self.chip == 0) | (self.chip == chips - 1)
        self.last = self.last_of(self.chip)
        self.passed = chips - 1 - self.last

    def last_of(self, chip):
        return jnp.where(chip >= self.chips // 2, 0, self.chips - 1)

    def second(self, k, half):
        return self.rows.at[
            2 * k + self.core, self.seconds[half], pl.ds(half * self.half, self.half)
        ]

    def through(self, half):
        return self.extra.at[pl.ds(half * self.half, self.half)]

    def move(self, source, target, sender, receiver, half, to):
        return pltpu.make_async_remote_copy(
            src_ref=source,
            dst_ref=target,
            send_sem=self.extra_sems.at[0, sender, half],
            recv_sem=self.extra_sems.at[1, receiver, half],
            device_id={"ep": 2 * jnp.clip(to, 0, self.chips - 1) + self.core},
            device_id_type=MESH,
        )

    def origin_moves(self):
        to = jnp.where(self.chip == 0, 1, self.chips - 2)
        for half in (0, 1):
            source = self.second(self.chip, half)
            if self.chips > 2:
                yield self.move(source, self.through(half), 0, 0, half, to)
            else:
                yield self.move(source, source, 0, 1, half, to)

    def away(self, k):
        return jnp.where(k == 0, self.chip + 1, self.chip - 1)

    def send_second(self):
        @pl.when(self.end)
        def _():
            for move in self.origin_moves():
                move.start()

    def pass_moves(self):
        to = self.away(self.passed)
        final = self.last_of(to) == self.passed
        for half in (0, 1):
            source = self.through(half)
            yield final, self.move(source, self.second(self.passed, half), 0, 1, half, to)
            if self.chips > 4:
                yield jnp.logical_not(final), self.move(source, source, 0, 0, half, to)

    def passing(self):
        if self.chips > 2:

            @pl.when(jnp.logical_not(self.end))
            def _():
                for half in (0, 1):
                    source = self.through(half)
                    self.move(source, source, 0, 0, half, self.chip).wait_recv()
                for wanted, move in self.pass_moves():
                    pl.when(wanted)(move.start)

    def last_moves(self):
        to = self.away(self.last)
        for half in (0, 1):
            source = self.second(self.last, half)
            yield (to >= 0) & (to < self.chips), self.move(source, source, 1, 1, half, to)

    def take_second(self, exchange):
        for half, (moving, move) in enumerate(self.last_moves()):
            move.wait_recv()
            pl.when(moving)(move.start)
        exchange.start_seconds()

    def finish_second(self):
        @pl.when(self.end)
        def _():
            for move in self.origin_moves():
                move.wait_send()

        if self.chips > 2:

            @pl.when(jnp.logical_not(self.end))
            def _():
                for wanted, move in self.pass_moves():
                    pl.when(wanted)(move.wait_send)

        for moving, move in self.last_moves():
            pl.when(moving)(move.wait_send)

    def remote(self, ref, send, recv, to):
        return pltpu.make_async_remote_copy(
            src_ref=ref,
            dst_ref=ref,
            send_sem=send,
            recv_sem=recv,
            device_id={"ep": to},
            device_id_type=MESH,
        )

    def along(self, k, half, way, to):
        to = jnp.clip(to, 0, self.chips - 1)
        ref = self.rows.at[2 * k + self.core, self.tp, pl.ds(half * self.half, self.half)]
        return self.remote(
            ref, self.sems.at[way, k, half], self.sems.at[2, k, half], 2 * to + self.core
        )

    def along_info(self, k, way, to):
        to = jnp.clip(to, 0, self.chips - 1)
        ref = self.info.at[2 * k + self.core]
        return self.remote(
            ref, self.info_sems.at[way, k], self.info_sems.at[2, k], 2 * to + self.core
        )

    def across(self, k, place):
        ref = self.rows.at[2 * k + self.core, place]
        return self.remote(ref, self.pair_sems.at[self.chips], self.pair_sems.at[k], self.partner)

    def all_across(self, k, other=False):
        ref = self.rows.at[2 * k + (1 - self.core if other else self.core)]
        return self.remote(ref, self.pair_sems.at[self.chips], self.pair_sems.at[k], self.partner)

    def across_info(self, k, other=False):
        core = 1 - self.core if other else self.core
        ref = self.info.at[2 * k + core]
        return self.remote(ref, self.pair_info.at[self.chips], self.pair_info.at[k], self.partner)

    def sides(self):
        return (
            (self.chip + 1 < self.chips, 0, self.chip + 1),
            (self.chip > 0, 1, self.chip - 1),
        )

    def send_own(self):
        for half in (0, 1):
            for inside, way, to in self.sides():
                pl.when(inside)(self.along(self.chip, half, way, to).start)
        for place in range(self.tp_count):
            self.across(self.chip, place).start()

    def send_info(self):
        for inside, way, to in self.sides():
            pl.when(inside)(self.along_info(self.chip, way, to).start)
        self.across_info(self.chip).start()
        self.send_second()

    def onward(self, k):
        right = k < self.chip
        to = jnp.where(right, self.chip + 1, self.chip - 1)
        return (to >= 0) & (to < self.chips), jnp.where(right, 0, 1), to

    def landed(self, k, exchange):
        moving, way, to = self.onward(k)
        for half in (0, 1):
            self.along(k, half, way, to).wait_recv()
            pl.when(moving)(self.along(k, half, way, to).start)
            exchange.start((half,))
        self.across(k, self.tp).start()
        self.along_info(k, way, to).wait_recv()
        pl.when(moving)(self.along_info(k, way, to).start)
        self.across_info(k).start()

    def shared(self, k, exchange, delta):
        exchange.wait(delta)
        self.across(k, flip(self.tp, delta)).start()

    def finish(self, order):
        self.finish_second()
        for half in (0, 1):
            for inside, way, to in self.sides():
                pl.when(inside)(self.along(self.chip, half, way, to).wait_send)
        for inside, way, to in self.sides():
            pl.when(inside)(self.along_info(self.chip, way, to).wait_send)
        for k in order:
            moving, way, to = self.onward(k)
            for half in (0, 1):
                pl.when(moving)(self.along(k, half, way, to).wait_send)
            pl.when(moving)(self.along_info(k, way, to).wait_send)
        for ref, sems in ((self.rows, self.pair_sems), (self.info, self.pair_info)):
            whole = ref.at[pl.ds(0, self.chips)]
            self.remote(whole, sems.at[self.chips], sems.at[0], self.partner).wait_send()


def chip_order(chip, chips):
    table = [
        sorted((k for k in range(chips) if k != at), key=lambda k: (abs(k - at), abs(k - (0 if at < chips / 2 else chips - 1))))
        for at in range(chips)
    ]
    return [
        sum(jnp.where(chip == at, table[at][number], 0) for at in range(chips))
        for number in range(chips - 1)
    ]


class Back:
    def __init__(self, count, placed, out, pair_in, held, from_left, from_right, sems):
        me = lax.axis_index("ep")
        self.chips = count // 2
        self.core = lax.rem(me, 2)
        self.chip = me // 2
        self.partner = me + 1 - 2 * self.core
        self.parts = 4
        self.half = out.shape[0] // self.parts
        self.right_to = jnp.minimum(me + 2, count - 2 + self.core)
        self.left_to = jnp.maximum(me - 2, self.core)
        self.placed, self.out, self.pair_in, self.held = placed, out, pair_in, held
        self.from_left, self.from_right, self.sems = from_left, from_right, sems

    def send(self, source, target, kind, item, to):
        at, part = item
        rows = pl.ds(part * self.half, self.half)
        return pltpu.make_async_remote_copy(
            src_ref=source.at[rows],
            dst_ref=target.at[at, rows],
            send_sem=self.sems.at[0],
            recv_sem=self.sems.at[
                2 + self.chips + self.parts * (self.chips * (kind - 1) + at) + part
            ],
            device_id={"ep": to},
            device_id_type=MESH,
        )

    def pair(self, at):
        return pltpu.make_async_remote_copy(
            src_ref=self.placed.at[2 * at + 1 - self.core],
            dst_ref=self.pair_in.at[at],
            send_sem=self.sems.at[1],
            recv_sem=self.sems.at[2 + at],
            device_id={"ep": self.partner},
            device_id_type=MESH,
        )

    def right(self, item, source=None):
        source = self.from_left if source is None else source
        return self.send(source.at[item[0]], self.from_left, 1, item, self.right_to)

    def left(self, item, source=None):
        source = self.from_right if source is None else source
        return self.send(source.at[item[0]], self.from_right, 2, item, self.left_to)

    def pair_sum(self, at):
        self.pair(at).wait_recv()
        self.held[at] = (
            self.placed[2 * at + self.core].astype(F32) + self.pair_in[at].astype(F32)
        ).astype(BF16)

    def forward(self, item, moving, hop, landing):
        at, part = item
        rows = pl.ds(part * self.half, self.half)

        @pl.when(moving)
        def _():
            relay = hop(item)
            relay.wait_recv()
            landing[at, rows] = (
                landing[at, rows].astype(F32) + self.held[at, rows].astype(F32)
            ).astype(BF16)
            relay.start()

    def origin(self, at):
        self.pair_sum(at)
        for part in range(self.parts):
            item = (at, part)
            pl.when(self.chip == 0)(self.right(item, self.held).start)
            pl.when(self.chip > 0)(self.left(item, self.held).start)

    def relays(self):
        chips, chip, parts = self.chips, self.chip, self.parts
        order = [1, *range(chips - 1, 1, -1)]
        ready = set()

        def summed(at):
            if at not in ready:
                ready.add(at)
                self.pair_sum(at)

        def step(near, number):
            part = number % parts
            right_at = order[number // parts]
            left_at = chips - 1 - right_at

            def rightward():
                self.forward((right_at, part), right_at > chip, self.right, self.from_left)

            def leftward():
                self.forward((left_at, part), left_at < chip, self.left, self.from_right)

            first, second = (rightward, leftward) if near else (leftward, rightward)
            pl.when(chip < chips // 2)(first)
            pl.when(chip >= chips // 2)(second)

        items = parts * (chips - 1)
        for number in range(items + parts):
            if number < items:
                summed(order[number // parts])
                summed(chips - 1 - order[number // parts])
                step(True, number)
            if number >= parts:
                step(False, number - parts)
            yield

    def collect(self):
        chip, at = self.chip, self.chip

        @pl.when((chip == 0) | (chip == self.chips - 1))
        def _():
            self.pair_sum(at)

        for part in range(self.parts):
            rows = pl.ds(part * self.half, self.half)
            self.out[rows] = self.held[at, rows]
            for inside, hop, landing in (
                (chip > 0, self.right, self.from_left),
                (chip < self.chips - 1, self.left, self.from_right),
            ):

                @pl.when(inside)
                def _():
                    hop((at, part)).wait_recv()
                    self.out[rows] = (
                        self.out[rows].astype(F32) + landing[at, rows].astype(F32)
                    ).astype(BF16)

    def finish(self):
        for whole, sem in (
            (self.from_left.at[pl.ds(0, self.chips - 1)], 0),
            (self.placed.at[pl.ds(0, self.chips)], 1),
        ):
            pltpu.make_async_remote_copy(
                src_ref=whole,
                dst_ref=whole,
                send_sem=self.sems.at[sem],
                recv_sem=self.sems.at[2],
                device_id={"ep": self.partner},
                device_id_type=MESH,
            ).wait_send()


def layer_kernel(
    tp_count,
    ep_count,
    cap,
    expert_count,
    mixer_hbm,
    gain_hbm,
    weight_hbm,
    moe_hbm,
    ffn_hbm,
    routes_hbm,
    route_weights_hbm,
    gate_hbm,
    up_hbm,
    down_hbm,
    mixer_hbm_out,
    moe_hbm_out,
    mixer_out,
    moe_out,
    gain_ref,
    ffn_ref,
    routes_ref,
    route_weights_ref,
    rows,
    info,
    extra,
    mix_in,
    gate_w,
    up_w,
    down_w,
    out_w,
    picked,
    hidden,
    read,
    local_out,
    carry,
    total,
    outgoing,
    incoming,
    before,
    mixed,
    product,
    landing,
    placed,
    pair_in,
    held,
    from_left,
    from_right,
    load_sems,
    along_sems,
    along_info_sems,
    pair_sems,
    pair_info_sems,
    extra_sems,
    row_sems,
    hidden_sems,
    prefix_sems,
    reduce_sems,
    back_sems,
):
    tp = lax.axis_index("tp")
    place = lax.axis_index("ep")
    chips = ep_count // 2
    chip = place // 2
    steps, bits = bit_list(ep_count), bit_list(tp_count)
    row_count, part_width = rows.shape[2], rows.shape[3]
    units = gate_w.shape[1]
    moe_loads = [
        pltpu.make_async_copy(
            moe_hbm.at[:, pl.ds(t * part_width, part_width)], rows.at[place, t], load_sems.at[0]
        )
        for t in range(tp_count)
    ]
    mixer_loads = [
        pltpu.make_async_copy(source, mix_in.at[i], load_sems.at[1])
        for i, source in enumerate(mixer_hbm)
    ]
    weight_loads = [
        pltpu.make_async_copy(source, target, load_sems.at[2 + i])
        for i, (source, target) in enumerate(
            ((gate_hbm, gate_w), (up_hbm, up_w), (down_hbm, down_w), (weight_hbm, out_w))
        )
    ]
    small_loads = [
        pltpu.make_async_copy(source, target, load_sems.at[6 + i])
        for i, (source, target) in enumerate(
            (
                (routes_hbm, routes_ref),
                (route_weights_hbm, route_weights_ref),
                (ffn_hbm, ffn_ref),
                (gain_hbm, gain_ref),
            )
        )
    ]
    for load in moe_loads:
        load.start()

    barrier = pltpu.get_barrier_semaphore()

    def signal(axis, to):
        pl.semaphore_signal(barrier, inc=1, device_id={axis: to}, device_id_type=MESH)

    for bit in bits:
        signal("tp", flip(tp, bit))
    for step in steps:
        pl.when(place + step < ep_count)(lambda: signal("ep", place + step))
        pl.when(place >= step)(lambda: signal("ep", place - step))
    for load in small_loads + weight_loads[:2] + mixer_loads + weight_loads[2:]:
        load.start()
    peers = sum(
        jnp.where(place + step < ep_count, 1, 0) + jnp.where(place >= step, 1, 0)
        for step in steps
    )
    pltpu.make_async_copy(rows.at[place], rows.at[place], load_sems.at[0]).wait()
    pl.semaphore_wait(barrier, peers + len(bits))

    dispatch = Dispatch(
        chips,
        tp_count,
        rows,
        info,
        extra,
        along_sems,
        along_info_sems,
        pair_sems,
        pair_info_sems,
        extra_sems,
    )
    order = chip_order(chip, chips)
    dispatch.send_own()

    squares = jnp.zeros((row_count, 1), F32)
    for t in range(tp_count):
        part = rows[place, t].astype(F32)
        squares += jnp.sum(part * part, axis=1, keepdims=True)
    scale = lax.rsqrt(squares / (tp_count * part_width) + 1.0)
    for load in small_loads:
        load.wait()
    names = lax.broadcasted_iota(jnp.int32, (expert_count, row_count), 0)
    portion = route_weights_ref[...]
    portion = portion / jnp.sum(portion, axis=0, keepdims=True)
    named = jnp.zeros((expert_count, row_count), F32)
    table = jnp.zeros((expert_count, row_count), F32)
    for choice in range(routes_ref.shape[0]):
        match = routes_ref[choice : choice + 1] == names
        named = jnp.where(match, 1.0, named)
        table = jnp.where(match, portion[choice : choice + 1], table)
    earlier = (
        lax.broadcasted_iota(jnp.int32, (row_count, row_count), 0)
        < lax.broadcasted_iota(jnp.int32, (row_count, row_count), 1)
    ).astype(BF16)
    info[place, :expert_count] = jnp.where(named > 0.0, dot(named, earlier), -1.0)
    info[place, expert_count : 2 * expert_count] = table
    info[place, 2 * expert_count :] = jnp.broadcast_to(scale, (row_count, row_count)).T[:8]
    dispatch.send_info()

    slot = lax.broadcasted_iota(jnp.int32, (cap, row_count), 0).astype(F32)

    def chosen(source):
        return info[source, pl.ds(place, 1), :] == slot

    def slot_value(pick, source, index):
        return jnp.sum(
            jnp.where(pick, info[source, pl.ds(index, 1), :], 0.0), axis=1, keepdims=True
        )

    sources = [chip] + order
    exchanges = [None] + [
        Exchange(tp_count, rows.at[2 * k + dispatch.core], row_sems, n, n == chips - 2)
        for n, k in enumerate(order)
    ]
    hidden_exchanges = [
        Exchange(tp_count, hidden.at[n], hidden_sems, n) for n in range(chips)
    ]

    def gate_up(n):
        k = sources[n]
        if n > 0:
            for delta in range(1, tp_count):
                exchanges[n].wait(delta)
        dispatch.all_across(k, True).wait_recv()
        dispatch.across_info(k, True).wait_recv()
        for core in (0, 1):
            source = 2 * k + core
            pick = chosen(source)
            factor = slot_value(pick, source, 2 * expert_count)
            onehot = pick.astype(BF16)
            for t in range(tp_count):
                part = dot(onehot, rows[source, t]) * factor * ffn_ref[t]
                picked[core * cap : (core + 1) * cap, t * part_width : (t + 1) * part_width] = (
                    part.astype(BF16)
                )
        gate = dot(picked[...], gate_w[...])
        up = dot(picked[...], up_w[...])
        hidden[n, tp] = (jax.nn.silu(gate) * up).astype(BF16)
        hidden_exchanges[n].start()

    back = Back(ep_count, placed, moe_out, pair_in, held, from_left, from_right, back_sems)

    def down(n):
        k = sources[n]
        for delta in range(1, tp_count):
            hidden_exchanges[n].wait(delta)
        result = dot(
            jnp.concatenate([hidden[n, t] for t in range(tp_count)], axis=1), down_w[...]
        )
        for core in (0, 1):
            source = 2 * k + core
            pick = chosen(source)
            share = slot_value(pick, source, expert_count + place)
            mine = result[core * cap : (core + 1) * cap] * share
            placed[source] = dot_cols(pick.astype(BF16), mine).astype(BF16)
        back.pair(k).start()

    def landed(n):
        dispatch.landed(sources[n], exchanges[n])

    def relay(n):
        exchanges[n].relay()
        for delta in range(1, tp_count):
            if delta & (delta - 1) == 0:
                dispatch.shared(sources[n], exchanges[n], delta)

    def share_rest(n):
        for delta in range(1, tp_count):
            if delta & (delta - 1):
                dispatch.shared(sources[n], exchanges[n], delta)

    tokens = read.shape[0]
    blocks = tokens // BLOCK

    def relay_hidden(n):
        hidden_exchanges[n].relay()

    def tables(b):
        tables_block(b, mix_in, read, local_out, total, carry, b == blocks - 1)

    prefix = Prefix(ep_count, total, outgoing, incoming, before, prefix_sems)

    def wait_loads(loads):
        for load in loads:
            load.wait()

    remote = chips - 1
    last_step = len(steps) - 1

    def prefix_step(number):
        prefix.receive(number)
        if number < last_step:
            prefix.send(number + 1)

    def mixer_start():
        prefix.begin()
        prefix.send(0)

    def heads():
        columns = read.shape[1]
        groups, width = total.shape[1], total.shape[3]
        ones = head_ones(width)
        for group in range(groups):
            at = pl.ds(group * width, width)
            heads_out = dot(read[:, at], spread(before[1, group])) + local_out[:, at]
            center = heads_out - dot_right(heads_out, ones) / HD
            variance = dot_right(center * center, ones) / HD
            mixed[:, at] = (center * lax.rsqrt(variance + 1.0) * gain_ref[:, at]).astype(BF16)

    def project():
        weight_loads[3].wait()
        out_rows = tokens // tp_count
        tile = out_w.shape[1] // 4
        for number in range(4):
            at = pl.ds(number * tile, tile)
            part = dot(mixed[...], out_w[:, at]).astype(BF16)
            for t in range(tp_count):
                product[t, :, at] = part[t * out_rows : (t + 1) * out_rows]

    reduce = Reduce(tp_count, product, landing, reduce_sems)

    out_copies = [
        pltpu.make_async_copy(source, target, load_sems.at[10 + i])
        for i, (source, target) in enumerate(
            ((mixer_out, mixer_hbm_out), (moe_out, moe_hbm_out))
        )
    ]

    def reduce_pass():
        for number in range(len(bits) - 1):
            reduce.land(number)
            reduce.start_passed(number + 1)
            reduce.start_finals(number + 1)

    def reduce_last():
        reduce.last(mixer_out)
        out_copies[0].start()

    def origin(n):
        pl.when(jnp.logical_not(inner))(lambda: back.origin(sources[n]))

    relays = back.relays()

    def run(count):
        @pl.when(inner)
        def _():
            for _ in itertools.islice(relays, count):
                pass

    def relay_inner(n):
        seen = set(exchanges[n].seen)
        pl.when(inner)(lambda: relay(n))
        exchanges[n].seen = seen

    def relay_outer(n):
        pl.when(jnp.logical_not(inner))(lambda: relay(n))

    def collect():
        back.collect()
        out_copies[1].start()

    inner = (chip > 0) & (chip < chips - 1)

    def landed_inner(n):
        pl.when(inner)(lambda: landed(n))

    def landed_outer(n):
        pl.when(jnp.logical_not(inner))(lambda: landed(n))

    def finish_dispatch():
        dispatch.finish(order)
        for exchange in exchanges[1:]:
            exchange.finish()

    def finish_hidden():
        for exchange in hidden_exchanges:
            exchange.finish()
        prefix.finish()

    def take_second():
        dispatch.take_second(exchanges[remote])

    def second_inner():
        pl.when(inner)(take_second)

    def second_outer():
        pl.when(jnp.logical_not(inner))(take_second)

    more = [(tables, b) for b in range(blocks)]
    chain = [(prefix_step, number) for number in range(len(steps))]
    all_mixer = pltpu.make_async_copy(mix_in, mix_in, load_sems.at[1])
    plan = [(wait_loads, [all_mixer]), *more[:1], (landed, 1)]
    plan += [(landed_inner, 2)] * (remote > 1)
    plan += [(wait_loads, weight_loads[:2]), (gate_up, 0), *more[1:2]]
    plan += [(relay, 1), (dispatch.passing,)] if remote > 1 else []
    plan += [(landed_inner, 3)] * (remote > 2)
    plan += [(landed_outer, 2)] * (remote > 1)
    plan += more[2:3]
    plan += [(second_inner,)] * (remote == 3)
    plan += [(share_rest, 1)] if remote > 1 else []
    plan += [(relay_inner, 2)] if remote > 2 else []
    plan += [(gate_up, 1), (relay_hidden, 0)] if remote > 1 else []
    plan += [(landed_outer, 3), (relay_outer, 2)] if remote > 2 else []
    plan += [*more[3:], (mixer_start,)]
    plan += [(second_outer,)] * (remote == 3)
    for n in range(2, remote):
        if n > 2:
            plan += [(landed, n + 1), (relay, n)]
        plan += [(share_rest, n), *chain[:1], (relay_hidden, n - 1), (gate_up, n)]
        chain = chain[1:] if n == 2 else chain
    plan += [(take_second,)] * (remote != 3)
    plan += [(relay, remote), (share_rest, remote), (gate_up, remote)]
    plan += [(wait_loads, weight_loads[2:3])]
    plan += [(down, 1)] if remote > 2 else []
    plan += [*chain[:1], (relay_hidden, remote - 1)]
    plan += [(origin, 1)] if remote > 2 else []
    plan += [*chain[1:], (heads,), (relay_hidden, remote), (project,)]
    plan += [(reduce.start_passed, 0), (reduce.start_finals, 0)]
    plan += [(down, n) for n in range(2 if remote > 2 else 1, remote + 1)]
    plan += [(origin, n) for n in range(remote, 1 if remote > 2 else 0, -1)]
    plan += [(finish_dispatch,), (down, 0)]
    plan += [(run, back.parts + 2), (reduce_pass,), (run, None)]
    plan += [(finish_hidden,), (reduce_last,), (collect,)]
    for step, (action, *given) in enumerate(plan):
        with jax.named_scope(f"{action.__name__}#{step}"):
            action(*given)

    reduce.finish()
    back.finish()
    for copy in out_copies:
        copy.wait()


def settle_kernel(*refs):
    sems = refs[-1]
    count = (len(refs) - 1) // 3
    takes, puts = [], []
    for i in range(count):
        held = refs[2 * count + i]
        takes.append(pltpu.make_async_copy(refs[i], held, sems.at[0, i]))
        puts.append(pltpu.make_async_copy(held, refs[count + i], sems.at[1, i]))
    for take in takes:
        take.start()
    for take, put in zip(takes, puts):
        take.wait()
        put.start()
    for put in puts:
        put.wait()


def settle(*arrays):
    hbm = pl.BlockSpec(memory_space=pltpu.HBM)
    return pl.pallas_call(
        settle_kernel,
        out_shape=[jax.ShapeDtypeStruct(a.shape, a.dtype) for a in arrays],
        in_specs=[hbm] * len(arrays),
        out_specs=[hbm] * len(arrays),
        scratch_shapes=[pltpu.VMEM(a.shape, a.dtype) for a in arrays]
        + [pltpu.SemaphoreType.DMA((2, len(arrays)))],
        compiler_params=pltpu.CompilerParams(vmem_limit_bytes=63 * 2**20),
        name="settle",
    )(*arrays)


def local(
    receptance,
    key_in,
    value_in,
    decay_in,
    rate_in,
    norm_gain,
    out_weight,
    moe_in,
    ffn_gain,
    routes,
    route_weights,
    gate_weight,
    up_weight,
    down_weight,
):
    tp_count, ep_count = lax.axis_size("tp"), lax.axis_size("ep")
    row_count, feature_count = moe_in.shape
    expert_count = gate_weight.shape[0] * ep_count
    cap = 5 * row_count * routes.shape[1] // (4 * expert_count)
    cap = -(-cap // 16) * 16
    chips = ep_count // 2
    part_width = feature_count // tp_count
    units, out_part = gate_weight.shape[2], down_weight.shape[2]
    tokens, columns = receptance.shape
    width = group_width(columns)
    groups = columns // width
    steps = ep_count.bit_length() - 1
    out_rows = tokens // tp_count
    dim = out_weight.shape[1]
    hbm = pl.BlockSpec(memory_space=pltpu.HBM)
    state = (2, groups, HD, width)
    dma = pltpu.SemaphoreType.DMA

    buffers = [
        pltpu.VMEM((out_rows, dim), BF16),
        pltpu.VMEM((row_count, out_part), BF16),
        pltpu.VMEM((1, columns), F32),
        pltpu.VMEM((tp_count, 1, part_width), F32),
        pltpu.VMEM((routes.shape[1], row_count), routes.dtype),
        pltpu.VMEM((routes.shape[1], row_count), F32),
        pltpu.VMEM((ep_count, tp_count, row_count, part_width), BF16),
        pltpu.VMEM((ep_count, 2 * expert_count + 8, row_count), F32),
        pltpu.VMEM((row_count, part_width), BF16),
        pltpu.VMEM((5, tokens, columns), BF16),
        pltpu.VMEM((feature_count, units), BF16),
        pltpu.VMEM((feature_count, units), BF16),
        pltpu.VMEM(down_weight.shape[1:], BF16),
        pltpu.VMEM(out_weight.shape, BF16),
        pltpu.VMEM((2 * cap, feature_count), BF16),
        pltpu.VMEM((chips, tp_count, 2 * cap, units), BF16),
        pltpu.VMEM((tokens, columns), BF16),
        pltpu.VMEM((tokens, columns), F32),
        pltpu.VMEM(state, F32),
        pltpu.VMEM(state, BF16),
        pltpu.VMEM((steps, *state), BF16),
        pltpu.VMEM((steps, *state), BF16),
        pltpu.VMEM(state, F32),
        pltpu.VMEM((tokens, columns), BF16),
        pltpu.VMEM((tp_count, out_rows, dim), BF16),
        pltpu.VMEM((tp_count, out_rows, dim), BF16),
        pltpu.VMEM((ep_count, row_count, out_part), BF16),
        pltpu.VMEM((chips, row_count, out_part), BF16),
        pltpu.VMEM((chips, row_count, out_part), BF16),
        pltpu.VMEM((chips, row_count, out_part), BF16),
        pltpu.VMEM((chips, row_count, out_part), BF16),
    ]
    sems = [
        dma((12,)),
        dma((3, chips, 2)),
        dma((3, chips)),
        dma((chips + 1,)),
        dma((chips + 1,)),
        dma((2, 2, 2)),
        dma((chips - 1, 2 * tp_count - 1)),
        dma((chips, 2 * tp_count - 1)),
        dma((2, steps)),
        dma((2 * tp_count - 1,)),
        dma((2 + 9 * chips,)),
    ]
    def kernel(r, k, v, d, a, *refs):
        layer_kernel(tp_count, ep_count, cap, expert_count, (r, k, v, d, a), *refs)

    results = pl.pallas_call(
        kernel,
        out_shape=[
            jax.ShapeDtypeStruct((out_rows, dim), BF16),
            jax.ShapeDtypeStruct((row_count, out_part), BF16),
        ],
        in_specs=[hbm] * 14,
        out_specs=[hbm, hbm],
        scratch_shapes=buffers + sems,
        compiler_params=pltpu.CompilerParams(
            collective_id=0, has_side_effects=True, vmem_limit_bytes=63 * 2**20
        ),
        name="layer",
    )(
        receptance,
        key_in,
        value_in,
        decay_in,
        rate_in,
        norm_gain[None],
        out_weight,
        moe_in,
        ffn_gain.reshape(tp_count, 1, part_width),
        routes.T,
        route_weights.T,
        gate_weight[0],
        up_weight[0],
        down_weight[0],
    )
    return settle(*results)


def solution(mesh):
    return jax.shard_map(
        local,
        mesh=mesh,
        in_specs=(
            P("ep", "tp"),
            P("ep", "tp"),
            P("ep", "tp"),
            P("ep", "tp"),
            P("ep", "tp"),
            P("tp"),
            P("tp", None),
            P("ep", None),
            P(),
            P("ep", None),
            P("ep", None),
            P("ep", None, "tp"),
            P("ep", None, "tp"),
            P("ep", None, "tp"),
        ),
        out_specs=(P(("ep", "tp"), None), P("ep", "tp")),
        check_vma=False,
    )
```

```python
import itertools

import jax
import jax.numpy as jnp
from jax import lax
from jax.experimental import pallas as pl
from jax.experimental.pallas import tpu as pltpu
from jax.sharding import PartitionSpec as P

HD = 64
BLOCK = 64
F32 = jnp.float32
BF16 = jnp.bfloat16
MESH = pl.DeviceIdType.MESH


def dot(a, b):
    return jnp.dot(a.astype(BF16), b.astype(BF16), preferred_element_type=F32)


def dot_rows(a, b):
    return lax.dot_general(
        a.astype(BF16), b.astype(BF16), (((1,), (1,)), ((), ())), preferred_element_type=F32
    )


def dot_cols(a, b):
    return lax.dot_general(
        a.astype(BF16), b.astype(BF16), (((0,), (0,)), ((), ())), preferred_element_type=F32
    )


def halves(a):
    high = a.astype(BF16)
    return high, (a - high.astype(F32)).astype(BF16)


def dot_left(mask, b):
    high, low = halves(b)
    return dot(mask, high) + dot(mask, low)


def dot_right(a, mask):
    high, low = halves(a)
    return dot(high, mask) + dot(low, mask)


def lane_head(rows, width):
    return lax.broadcasted_iota(jnp.int32, (rows, width), 1) // HD


def spread(packed):
    rows, width = packed.shape
    packed = packed.astype(BF16)
    head = lane_head(rows, width)
    return jnp.concatenate(
        [jnp.where(head == i, packed, jnp.zeros_like(packed)) for i in range(width // HD)], axis=0
    )


def fold(square):
    width = square.shape[1]
    head = lane_head(HD, width)
    out = jnp.zeros((HD, width), F32)
    for i in range(width // HD):
        out = jnp.where(head == i, square[i * HD : (i + 1) * HD], out)
    return out


def head_ones(width):
    row = lax.broadcasted_iota(jnp.int32, (width, width), 0) // HD
    return (row == lane_head(width, width)).astype(BF16)


def group_width(columns):
    return HD * max(g for g in (4, 2, 1) if columns % (g * HD) == 0)


def tables_block(block, mix_in, read_ref, local_ref, total_ref, carry, last):
    columns = read_ref.shape[1]
    width = group_width(columns)
    row = lax.broadcasted_iota(jnp.int32, (BLOCK, width), 0)
    lane = lax.broadcasted_iota(jnp.int32, (BLOCK, width), 1) % HD
    strict = lane < row
    closed = lane <= row
    eye = (lane == row).astype(F32)
    tril = (
        lax.broadcasted_iota(jnp.int32, (BLOCK, BLOCK), 1)
        <= lax.broadcasted_iota(jnp.int32, (BLOCK, BLOCK), 0)
    ).astype(BF16)
    ones = head_ones(width)
    rows = pl.ds(block * BLOCK, BLOCK)
    for group in range(columns // width):
        at = pl.ds(group * width, width)
        readout = mix_in[0, rows, at].astype(F32)
        key = mix_in[1, rows, at].astype(F32)
        value = mix_in[2, rows, at]
        log_decay = jax.nn.sigmoid(mix_in[3, rows, at].astype(F32)) * -0.6065306597126334
        rate = jax.nn.sigmoid(mix_in[4, rows, at].astype(F32))
        unit = key * lax.rsqrt(dot_right(key * key, ones) + 1.0)
        inclusive = dot_left(tril, log_decay)
        total = inclusive[BLOCK - 1 :]
        probe = -unit * jnp.exp(inclusive - log_decay)
        removal = unit * rate
        written = key * rate
        back = jnp.exp(-inclusive)
        tail = jnp.exp(total - inclusive)
        readout = readout * jnp.exp(inclusive)
        left = jnp.concatenate([probe, readout], axis=0)
        on_removal = dot_rows(left, spread(removal * back))
        on_write = dot_rows(left, spread(written * back))
        lower = jnp.where(strict, on_removal[:BLOCK], 0.0)
        reach = jnp.where(closed, on_removal[BLOCK:], 0.0)
        lower_write = jnp.where(strict, on_write[:BLOCK], 0.0)
        reach_write = jnp.where(closed, on_write[BLOCK:], 0.0)
        value_wide = spread(value)
        on_value = dot(jnp.concatenate([lower_write, reach_write], axis=0), value_wide)
        inverse = eye + lower
        power = dot(lower, spread(lower))
        for doubling in range(BLOCK.bit_length() - 2):
            wide = spread(power)
            if doubling < BLOCK.bit_length() - 3:
                both = dot(jnp.concatenate([inverse, power], axis=0), wide)
                inverse = inverse + both[:BLOCK]
                power = both[BLOCK:]
            else:
                inverse = inverse + dot(inverse, wide)
        solved_probe = dot(inverse, spread(probe))
        solved_values = dot(inverse, spread(on_value[:BLOCK]))
        transition = eye * jnp.exp(total) + fold(dot_cols(removal * tail, solved_probe))
        increment = fold(
            dot_cols(
                jnp.concatenate([removal * tail, written * tail], axis=0),
                jnp.concatenate([solved_values.astype(BF16), value], axis=0),
            )
        )
        read_state = readout + dot(reach, spread(solved_probe))
        local_out = dot(reach, spread(solved_values)) + on_value[BLOCK:]
        if block == 0:
            new_map, new_add = transition, increment
            read_ref[rows, at] = read_state.astype(BF16)
            local_ref[rows, at] = local_out
        else:
            left = jnp.concatenate([read_state, transition], axis=0)
            on_map = dot(left, spread(carry[0, group]))
            on_add = dot(left, spread(carry[1, group]))
            read_ref[rows, at] = on_map[:BLOCK].astype(BF16)
            local_ref[rows, at] = on_add[:BLOCK] + local_out
            new_map, new_add = on_map[BLOCK:], on_add[BLOCK:] + increment
        if last:
            total_ref[0, group] = new_map.astype(BF16)
            total_ref[1, group] = new_add.astype(BF16)
        else:
            carry[0, group] = new_map
            carry[1, group] = new_add


def flip(me, bits):
    bit = 1
    while bit <= bits:
        if bits & bit:
            me = me + bit - 2 * bit * ((me // bit) % 2)
        bit *= 2
    return me


def bit_list(count):
    return [1 << b for b in range(count.bit_length() - 1)]


class Exchange:
    def __init__(self, count, slots, sems, unit, wide=False):
        me = lax.axis_index("tp")
        half = slots.shape[1] // 2
        bits = bit_list(count)
        self.count, self.copies, self.heads, self.relays, self.seen = count, {}, [], [], set()
        whole = slots.at[pl.ds(0, count - 2 if wide else count - 1)]
        self.sent = pltpu.make_async_remote_copy(
            src_ref=whole,
            dst_ref=whole,
            send_sem=sems.at[unit, 2 * (count - 1)],
            recv_sem=sems.at[unit, 0],
            device_id={"tp": flip(me, bits[0])},
            device_id_type=MESH,
        )
        self.seconds = []
        for number in range(1 if wide else 0, len(bits)):
            for stream, order in enumerate((bits, bits[::-1])):
                at = pl.ds(stream * half, half)
                known = [0]
                for bit in order[:number]:
                    known += [k ^ bit for k in known]
                for from_delta in known:
                    bit = order[number]
                    key = (stream, from_delta ^ bit)
                    owner = flip(me, from_delta)
                    self.copies[key] = pltpu.make_async_remote_copy(
                        src_ref=slots.at[owner, at],
                        dst_ref=slots.at[owner, at],
                        send_sem=sems.at[unit, 2 * (count - 1)],
                        recv_sem=sems.at[unit, stream * (count - 1) + key[1] - 1],
                        device_id={"tp": flip(me, bit)},
                        device_id_type=MESH,
                    )
                    if wide and from_delta == order[0]:
                        self.seconds.append(key)
                    elif from_delta:
                        self.relays.append((key, from_delta))
                    else:
                        self.heads.append(key)

    def start(self, streams=(0, 1)):
        for key in self.heads:
            if key[0] in streams:
                self.copies[key].start()

    def start_seconds(self):
        for key in self.seconds:
            self.copies[key].start()

    def arrive(self, stream, delta):
        if (stream, delta) in self.copies and (stream, delta) not in self.seen:
            self.seen.add((stream, delta))
            self.copies[stream, delta].wait_recv()

    def relay(self):
        for key, from_delta in self.relays:
            self.arrive(key[0], from_delta)
            self.copies[key].start()

    def wait(self, delta):
        for stream in (0, 1):
            self.arrive(stream, delta)

    def finish(self):
        self.sent.wait_send()


class Prefix:
    def __init__(self, count, own, outgoing, incoming, before, sems):
        self.me, self.count = lax.axis_index("ep"), count
        self.own, self.outgoing, self.incoming, self.before = own, outgoing, incoming, before
        self.steps = bit_list(count)
        self.copies = []
        for number, step in enumerate(self.steps):
            source = own if number == 0 else outgoing.at[number - 1]
            target = incoming.at[number]
            if number == len(self.steps) - 1:
                source, target = source.at[1], target.at[1]
            self.copies.append(
                pltpu.make_async_remote_copy(
                    src_ref=source,
                    dst_ref=target,
                    send_sem=sems.at[0, number],
                    recv_sem=sems.at[1, number],
                    device_id={"ep": lax.rem(self.me + step, count)},
                    device_id_type=MESH,
                )
            )

    def begin(self):
        groups, width = self.own.shape[1], self.own.shape[3]
        lane = lax.broadcasted_iota(jnp.int32, (HD, width), 1) % HD
        eye = (lane == lax.broadcasted_iota(jnp.int32, (HD, width), 0)).astype(F32)
        for group in range(groups):
            self.before[0, group] = eye
            self.before[1, group] = jnp.zeros_like(eye)

    def send(self, number):
        pl.when(self.me + self.steps[number] < self.count)(self.copies[number].start)

    def receive(self, number):
        last = number == len(self.steps) - 1
        groups = self.own.shape[1]
        own, before, incoming = self.own, self.before, self.incoming

        @pl.when(self.me >= self.steps[number])
        def _():
            self.copies[number].wait_recv()
            for group in range(groups):
                left = before[0, group]
                before[1, group] += dot(left, spread(incoming[number, 1, group]))
                if not last:
                    before[0, group] = dot(left, spread(incoming[number, 0, group]))

        if not last:
            for group in range(groups):
                left = own[0, group]
                self.outgoing[number, 0, group] = dot(left, spread(before[0, group])).astype(BF16)
                self.outgoing[number, 1, group] = (
                    dot(left, spread(before[1, group])) + own[1, group].astype(F32)
                ).astype(BF16)

    def finish(self):
        for step, copy in zip(self.steps, self.copies):
            pl.when(self.me + step < self.count)(copy.wait_send)


class Reduce:
    def __init__(self, count, parts, landing, sems):
        self.me = lax.axis_index("tp")
        self.parts, self.landing = parts, landing
        self.half = parts.shape[2] // 2
        bits = bit_list(count)
        whole = landing.at[pl.ds(0, count - 1)]
        self.sent = pltpu.make_async_remote_copy(
            src_ref=whole,
            dst_ref=whole,
            send_sem=sems.at[2 * (count - 1)],
            recv_sem=sems.at[0],
            device_id={"tp": flip(self.me, bits[0])},
            device_id_type=MESH,
        )
        orders = (bits, bits[::-1])
        self.stages, self.finals, self.copies = [], [], {}
        left = [list(range(count))] * 2
        for number in range(len(bits)):
            passed, finals = [], []
            for stream in (0, 1):
                bit = orders[stream][number]
                sent = [d for d in left[stream] if d & bit]
                left[stream] = [d for d in left[stream] if not d & bit]
                at = pl.ds(stream * self.half, self.half)
                for delta in sent:
                    owner = flip(self.me, delta)
                    self.copies[stream, delta] = pltpu.make_async_remote_copy(
                        src_ref=parts.at[owner, :, at],
                        dst_ref=landing.at[delta, :, at],
                        send_sem=sems.at[2 * (count - 1)],
                        recv_sem=sems.at[stream * (count - 1) + delta - 1],
                        device_id={"tp": flip(self.me, bit)},
                        device_id_type=MESH,
                    )
                    (finals if delta == bit else passed).append((stream, delta, bit))
            self.stages.append(passed)
            self.finals.append(finals)

    def start_passed(self, number):
        for stream, delta, _ in self.stages[number]:
            self.copies[stream, delta].start()

    def start_finals(self, number):
        for stream, delta, _ in self.finals[number]:
            self.copies[stream, delta].start()

    def land(self, number):
        for stream, delta, bit in self.stages[number]:
            at = pl.ds(stream * self.half, self.half)
            self.copies[stream, delta].wait_recv()
            mine = flip(self.me, delta ^ bit)
            total = self.parts[mine, :, at].astype(F32) + self.landing[delta, :, at].astype(F32)
            self.parts[mine, :, at] = total.astype(BF16)

    def last(self, out):
        for stream in (0, 1):
            at = pl.ds(stream * self.half, self.half)
            total = self.parts[self.me, :, at].astype(F32)
            for finals in self.finals:
                for owner, delta, _ in finals:
                    if owner == stream:
                        self.copies[stream, delta].wait_recv()
                        total += self.landing[delta, :, at].astype(F32)
            out[:, at] = total.astype(BF16)

    def finish(self):
        self.sent.wait_send()


class Dispatch:
    def __init__(
        self, chips, tp_count, rows, info, extra, sems, info_sems, pair_sems, pair_info, extra_sems
    ):
        me = lax.axis_index("ep")
        self.tp = lax.axis_index("tp")
        self.tp_count = tp_count
        self.core, self.chip, self.chips = lax.rem(me, 2), me // 2, chips
        self.me, self.partner = me, me + 1 - 2 * self.core
        self.rows, self.info = rows, info
        self.sems, self.info_sems = sems, info_sems
        self.pair_sems, self.pair_info = pair_sems, pair_info
        self.half = rows.shape[2] // 2
        bits = bit_list(tp_count)
        self.seconds = [flip(self.tp, bits[0]), flip(self.tp, bits[-1])]
        self.extra, self.extra_sems = extra, extra_sems
        self.end = (self.chip == 0) | (self.chip == chips - 1)
        self.last = self.last_of(self.chip)
        self.passed = chips - 1 - self.last

    def last_of(self, chip):
        return jnp.where(chip >= self.chips // 2, 0, self.chips - 1)

    def second(self, k, half):
        return self.rows.at[
            2 * k + self.core, self.seconds[half], pl.ds(half * self.half, self.half)
        ]

    def through(self, half):
        return self.extra.at[pl.ds(half * self.half, self.half)]

    def move(self, source, target, sender, receiver, half, to):
        return pltpu.make_async_remote_copy(
            src_ref=source,
            dst_ref=target,
            send_sem=self.extra_sems.at[0, sender, half],
            recv_sem=self.extra_sems.at[1, receiver, half],
            device_id={"ep": 2 * jnp.clip(to, 0, self.chips - 1) + self.core},
            device_id_type=MESH,
        )

    def origin_moves(self):
        to = jnp.where(self.chip == 0, 1, self.chips - 2)
        for half in (0, 1):
            source = self.second(self.chip, half)
            if self.chips > 2:
                yield self.move(source, self.through(half), 0, 0, half, to)
            else:
                yield self.move(source, source, 0, 1, half, to)

    def away(self, k):
        return jnp.where(k == 0, self.chip + 1, self.chip - 1)

    def send_second(self):
        @pl.when(self.end)
        def _():
            for move in self.origin_moves():
                move.start()

    def pass_moves(self):
        to = self.away(self.passed)
        final = self.last_of(to) == self.passed
        for half in (0, 1):
            source = self.through(half)
            yield final, self.move(source, self.second(self.passed, half), 0, 1, half, to)
            if self.chips > 4:
                yield jnp.logical_not(final), self.move(source, source, 0, 0, half, to)

    def passing(self):
        if self.chips > 2:

            @pl.when(jnp.logical_not(self.end))
            def _():
                for half in (0, 1):
                    source = self.through(half)
                    self.move(source, source, 0, 0, half, self.chip).wait_recv()
                for wanted, move in self.pass_moves():
                    pl.when(wanted)(move.start)

    def last_moves(self):
        to = self.away(self.last)
        for half in (0, 1):
            source = self.second(self.last, half)
            yield (to >= 0) & (to < self.chips), self.move(source, source, 1, 1, half, to)

    def take_second(self, exchange):
        for half, (moving, move) in enumerate(self.last_moves()):
            move.wait_recv()
            pl.when(moving)(move.start)
        exchange.start_seconds()

    def finish_second(self):
        @pl.when(self.end)
        def _():
            for move in self.origin_moves():
                move.wait_send()

        if self.chips > 2:

            @pl.when(jnp.logical_not(self.end))
            def _():
                for wanted, move in self.pass_moves():
                    pl.when(wanted)(move.wait_send)

        for moving, move in self.last_moves():
            pl.when(moving)(move.wait_send)

    def remote(self, ref, send, recv, to):
        return pltpu.make_async_remote_copy(
            src_ref=ref,
            dst_ref=ref,
            send_sem=send,
            recv_sem=recv,
            device_id={"ep": to},
            device_id_type=MESH,
        )

    def along(self, k, half, way, to):
        to = jnp.clip(to, 0, self.chips - 1)
        ref = self.rows.at[2 * k + self.core, self.tp, pl.ds(half * self.half, self.half)]
        return self.remote(
            ref, self.sems.at[way, k, half], self.sems.at[2, k, half], 2 * to + self.core
        )

    def along_info(self, k, way, to):
        to = jnp.clip(to, 0, self.chips - 1)
        ref = self.info.at[2 * k + self.core]
        return self.remote(
            ref, self.info_sems.at[way, k], self.info_sems.at[2, k], 2 * to + self.core
        )

    def across(self, k, place):
        ref = self.rows.at[2 * k + self.core, place]
        return self.remote(ref, self.pair_sems.at[self.chips], self.pair_sems.at[k], self.partner)

    def all_across(self, k, other=False):
        ref = self.rows.at[2 * k + (1 - self.core if other else self.core)]
        return self.remote(ref, self.pair_sems.at[self.chips], self.pair_sems.at[k], self.partner)

    def across_info(self, k, other=False):
        core = 1 - self.core if other else self.core
        ref = self.info.at[2 * k + core]
        return self.remote(ref, self.pair_info.at[self.chips], self.pair_info.at[k], self.partner)

    def sides(self):
        return (
            (self.chip + 1 < self.chips, 0, self.chip + 1),
            (self.chip > 0, 1, self.chip - 1),
        )

    def send_own(self):
        for half in (0, 1):
            for inside, way, to in self.sides():
                pl.when(inside)(self.along(self.chip, half, way, to).start)
        for place in range(self.tp_count):
            self.across(self.chip, place).start()

    def send_info(self):
        for inside, way, to in self.sides():
            pl.when(inside)(self.along_info(self.chip, way, to).start)
        self.across_info(self.chip).start()
        self.send_second()

    def onward(self, k):
        right = k < self.chip
        to = jnp.where(right, self.chip + 1, self.chip - 1)
        return (to >= 0) & (to < self.chips), jnp.where(right, 0, 1), to

    def landed_half(self, k, exchange, half):
        moving, way, to = self.onward(k)
        self.along(k, half, way, to).wait_recv()
        pl.when(moving)(self.along(k, half, way, to).start)
        exchange.start((half,))

    def landed_rest(self, k):
        moving, way, to = self.onward(k)
        self.across(k, self.tp).start()
        self.along_info(k, way, to).wait_recv()
        pl.when(moving)(self.along_info(k, way, to).start)
        self.across_info(k).start()

    def shared(self, k, exchange, delta):
        exchange.wait(delta)
        self.across(k, flip(self.tp, delta)).start()

    def finish(self, order):
        self.finish_second()
        for half in (0, 1):
            for inside, way, to in self.sides():
                pl.when(inside)(self.along(self.chip, half, way, to).wait_send)
        for inside, way, to in self.sides():
            pl.when(inside)(self.along_info(self.chip, way, to).wait_send)
        for k in order:
            moving, way, to = self.onward(k)
            for half in (0, 1):
                pl.when(moving)(self.along(k, half, way, to).wait_send)
            pl.when(moving)(self.along_info(k, way, to).wait_send)
        for ref, sems in ((self.rows, self.pair_sems), (self.info, self.pair_info)):
            whole = ref.at[pl.ds(0, self.chips)]
            self.remote(whole, sems.at[self.chips], sems.at[0], self.partner).wait_send()


def chip_order(chip, chips):
    table = [
        sorted((k for k in range(chips) if k != at), key=lambda k: (abs(k - at), abs(k - (0 if at < chips / 2 else chips - 1))))
        for at in range(chips)
    ]
    return [
        sum(jnp.where(chip == at, table[at][number], 0) for at in range(chips))
        for number in range(chips - 1)
    ]


class Back:
    def __init__(self, count, placed, out, pair_in, held, from_left, from_right, sems):
        me = lax.axis_index("ep")
        self.chips = count // 2
        self.core = lax.rem(me, 2)
        self.chip = me // 2
        self.partner = me + 1 - 2 * self.core
        self.parts = 4
        self.half = out.shape[0] // self.parts
        self.right_to = jnp.minimum(me + 2, count - 2 + self.core)
        self.left_to = jnp.maximum(me - 2, self.core)
        self.placed, self.out, self.pair_in, self.held = placed, out, pair_in, held
        self.from_left, self.from_right, self.sems = from_left, from_right, sems

    def send(self, source, target, kind, item, to):
        at, part = item
        rows = pl.ds(part * self.half, self.half)
        return pltpu.make_async_remote_copy(
            src_ref=source.at[rows],
            dst_ref=target.at[at, rows],
            send_sem=self.sems.at[0],
            recv_sem=self.sems.at[
                2 + self.chips + self.parts * (self.chips * (kind - 1) + at) + part
            ],
            device_id={"ep": to},
            device_id_type=MESH,
        )

    def pair(self, at):
        return pltpu.make_async_remote_copy(
            src_ref=self.placed.at[2 * at + 1 - self.core],
            dst_ref=self.pair_in.at[at],
            send_sem=self.sems.at[1],
            recv_sem=self.sems.at[2 + at],
            device_id={"ep": self.partner},
            device_id_type=MESH,
        )

    def right(self, item, source=None):
        source = self.from_left if source is None else source
        return self.send(source.at[item[0]], self.from_left, 1, item, self.right_to)

    def left(self, item, source=None):
        source = self.from_right if source is None else source
        return self.send(source.at[item[0]], self.from_right, 2, item, self.left_to)

    def pair_sum(self, at):
        self.pair(at).wait_recv()
        self.held[at] = (
            self.placed[2 * at + self.core].astype(F32) + self.pair_in[at].astype(F32)
        ).astype(BF16)

    def forward(self, item, moving, hop, landing):
        at, part = item
        rows = pl.ds(part * self.half, self.half)

        @pl.when(moving)
        def _():
            relay = hop(item)
            relay.wait_recv()
            landing[at, rows] = (
                landing[at, rows].astype(F32) + self.held[at, rows].astype(F32)
            ).astype(BF16)
            relay.start()

    def origin(self, at):
        self.pair_sum(at)
        for part in range(self.parts):
            item = (at, part)
            pl.when(self.chip == 0)(self.right(item, self.held).start)
            pl.when(self.chip > 0)(self.left(item, self.held).start)

    def relays(self):
        chips, chip, parts = self.chips, self.chip, self.parts
        order = [1, *range(chips - 1, 1, -1)]
        ready = set()

        def summed(at):
            if at not in ready:
                ready.add(at)
                self.pair_sum(at)

        def step(near, number):
            part = number % parts
            right_at = order[number // parts]
            left_at = chips - 1 - right_at

            def rightward():
                self.forward((right_at, part), right_at > chip, self.right, self.from_left)

            def leftward():
                self.forward((left_at, part), left_at < chip, self.left, self.from_right)

            first, second = (rightward, leftward) if near else (leftward, rightward)
            pl.when(chip < chips // 2)(first)
            pl.when(chip >= chips // 2)(second)

        items = parts * (chips - 1)
        for number in range(items + parts):
            if number < items:
                summed(order[number // parts])
                summed(chips - 1 - order[number // parts])
                step(True, number)
            if number >= parts:
                step(False, number - parts)
            yield

    def collect(self):
        chip, at = self.chip, self.chip

        @pl.when((chip == 0) | (chip == self.chips - 1))
        def _():
            self.pair_sum(at)

        for part in range(self.parts):
            rows = pl.ds(part * self.half, self.half)
            self.out[rows] = self.held[at, rows]
            for inside, hop, landing in (
                (chip > 0, self.right, self.from_left),
                (chip < self.chips - 1, self.left, self.from_right),
            ):

                @pl.when(inside)
                def _():
                    hop((at, part)).wait_recv()
                    self.out[rows] = (
                        self.out[rows].astype(F32) + landing[at, rows].astype(F32)
                    ).astype(BF16)

    def finish(self):
        for whole, sem in (
            (self.from_left.at[pl.ds(0, self.chips - 1)], 0),
            (self.placed.at[pl.ds(0, self.chips)], 1),
        ):
            pltpu.make_async_remote_copy(
                src_ref=whole,
                dst_ref=whole,
                send_sem=self.sems.at[sem],
                recv_sem=self.sems.at[2],
                device_id={"ep": self.partner},
                device_id_type=MESH,
            ).wait_send()


def layer_kernel(
    tp_count,
    ep_count,
    cap,
    expert_count,
    mixer_hbm,
    gain_hbm,
    weight_hbm,
    moe_hbm,
    ffn_hbm,
    routes_hbm,
    route_weights_hbm,
    gate_hbm,
    up_hbm,
    down_hbm,
    mixer_hbm_out,
    moe_hbm_out,
    mixer_out,
    moe_out,
    gain_ref,
    ffn_ref,
    routes_ref,
    route_weights_ref,
    rows,
    info,
    extra,
    mix_in,
    gate_w,
    up_w,
    down_w,
    out_w,
    picked,
    hidden,
    read,
    local_out,
    carry,
    total,
    outgoing,
    incoming,
    before,
    mixed,
    product,
    landing,
    placed,
    pair_in,
    held,
    from_left,
    from_right,
    load_sems,
    along_sems,
    along_info_sems,
    pair_sems,
    pair_info_sems,
    extra_sems,
    row_sems,
    hidden_sems,
    prefix_sems,
    reduce_sems,
    back_sems,
):
    tp = lax.axis_index("tp")
    place = lax.axis_index("ep")
    chips = ep_count // 2
    chip = place // 2
    steps, bits = bit_list(ep_count), bit_list(tp_count)
    row_count, part_width = rows.shape[2], rows.shape[3]
    units = gate_w.shape[1]
    moe_loads = [
        pltpu.make_async_copy(
            moe_hbm.at[:, pl.ds(t * part_width, part_width)], rows.at[place, t], load_sems.at[0]
        )
        for t in range(tp_count)
    ]
    mixer_loads = [
        pltpu.make_async_copy(source, mix_in.at[i], load_sems.at[1])
        for i, source in enumerate(mixer_hbm)
    ]
    weight_loads = [
        pltpu.make_async_copy(source, target, load_sems.at[2 + i])
        for i, (source, target) in enumerate(
            ((gate_hbm, gate_w), (up_hbm, up_w), (down_hbm, down_w), (weight_hbm, out_w))
        )
    ]
    small_loads = [
        pltpu.make_async_copy(source, target, load_sems.at[6 + i])
        for i, (source, target) in enumerate(
            (
                (routes_hbm, routes_ref),
                (route_weights_hbm, route_weights_ref),
                (ffn_hbm, ffn_ref),
                (gain_hbm, gain_ref),
            )
        )
    ]
    for load in moe_loads:
        load.start()

    barrier = pltpu.get_barrier_semaphore()

    def signal(axis, to):
        pl.semaphore_signal(barrier, inc=1, device_id={axis: to}, device_id_type=MESH)

    for bit in bits:
        signal("tp", flip(tp, bit))
    for step in steps:
        pl.when(place + step < ep_count)(lambda: signal("ep", place + step))
        pl.when(place >= step)(lambda: signal("ep", place - step))
    for load in small_loads + weight_loads[:2] + mixer_loads + weight_loads[2:]:
        load.start()
    peers = sum(
        jnp.where(place + step < ep_count, 1, 0) + jnp.where(place >= step, 1, 0)
        for step in steps
    )
    pltpu.make_async_copy(rows.at[place], rows.at[place], load_sems.at[0]).wait()
    pl.semaphore_wait(barrier, peers + len(bits))

    dispatch = Dispatch(
        chips,
        tp_count,
        rows,
        info,
        extra,
        along_sems,
        along_info_sems,
        pair_sems,
        pair_info_sems,
        extra_sems,
    )
    order = chip_order(chip, chips)
    dispatch.send_own()

    squares = jnp.zeros((row_count, 1), F32)
    for t in range(tp_count):
        part = rows[place, t].astype(F32)
        squares += jnp.sum(part * part, axis=1, keepdims=True)
    scale = lax.rsqrt(squares / (tp_count * part_width) + 1.0)
    for load in small_loads:
        load.wait()
    names = lax.broadcasted_iota(jnp.int32, (expert_count, row_count), 0)
    portion = route_weights_ref[...]
    portion = portion / jnp.sum(portion, axis=0, keepdims=True)
    named = jnp.zeros((expert_count, row_count), F32)
    table = jnp.zeros((expert_count, row_count), F32)
    for choice in range(routes_ref.shape[0]):
        match = routes_ref[choice : choice + 1] == names
        named = jnp.where(match, 1.0, named)
        table = jnp.where(match, portion[choice : choice + 1], table)
    earlier = (
        lax.broadcasted_iota(jnp.int32, (row_count, row_count), 0)
        < lax.broadcasted_iota(jnp.int32, (row_count, row_count), 1)
    ).astype(BF16)
    info[place, :expert_count] = jnp.where(named > 0.0, dot(named, earlier), -1.0)
    info[place, expert_count : 2 * expert_count] = table
    info[place, 2 * expert_count :] = jnp.broadcast_to(scale, (row_count, row_count)).T[:8]
    dispatch.send_info()

    slot = lax.broadcasted_iota(jnp.int32, (cap, row_count), 0).astype(F32)

    def chosen(source):
        return info[source, pl.ds(place, 1), :] == slot

    def slot_value(pick, source, index):
        return jnp.sum(
            jnp.where(pick, info[source, pl.ds(index, 1), :], 0.0), axis=1, keepdims=True
        )

    sources = [chip] + order
    exchanges = [None] + [
        Exchange(tp_count, rows.at[2 * k + dispatch.core], row_sems, n, n == chips - 2)
        for n, k in enumerate(order)
    ]
    hidden_exchanges = [
        Exchange(tp_count, hidden.at[n], hidden_sems, n) for n in range(chips)
    ]

    def gate_up(n):
        k = sources[n]
        if n > 0:
            for delta in range(1, tp_count):
                exchanges[n].wait(delta)
        dispatch.all_across(k, True).wait_recv()
        dispatch.across_info(k, True).wait_recv()
        for core in (0, 1):
            source = 2 * k + core
            pick = chosen(source)
            factor = slot_value(pick, source, 2 * expert_count)
            onehot = pick.astype(BF16)
            for t in range(tp_count):
                part = dot(onehot, rows[source, t]) * factor * ffn_ref[t]
                picked[core * cap : (core + 1) * cap, t * part_width : (t + 1) * part_width] = (
                    part.astype(BF16)
                )
        gate = dot(picked[...], gate_w[...])
        up = dot(picked[...], up_w[...])
        hidden[n, tp] = (jax.nn.silu(gate) * up).astype(BF16)
        hidden_exchanges[n].start()

    back = Back(ep_count, placed, moe_out, pair_in, held, from_left, from_right, back_sems)

    def down(n):
        k = sources[n]
        for delta in range(1, tp_count):
            hidden_exchanges[n].wait(delta)
        result = dot(
            jnp.concatenate([hidden[n, t] for t in range(tp_count)], axis=1), down_w[...]
        )
        for core in (0, 1):
            source = 2 * k + core
            pick = chosen(source)
            share = slot_value(pick, source, expert_count + place)
            mine = result[core * cap : (core + 1) * cap] * share
            placed[source] = dot_cols(pick.astype(BF16), mine).astype(BF16)
        back.pair(k).start()

    def landed_half(n, half):
        dispatch.landed_half(sources[n], exchanges[n], half)

    def landed_rest(n):
        dispatch.landed_rest(sources[n])

    def landed(n):
        landed_half(n, 0)
        landed_half(n, 1)
        landed_rest(n)

    def relay(n):
        exchanges[n].relay()
        for delta in range(1, tp_count):
            if delta & (delta - 1) == 0:
                dispatch.shared(sources[n], exchanges[n], delta)

    def share_rest(n):
        for delta in range(1, tp_count):
            if delta & (delta - 1):
                dispatch.shared(sources[n], exchanges[n], delta)

    tokens = read.shape[0]
    blocks = tokens // BLOCK

    def relay_hidden(n):
        hidden_exchanges[n].relay()

    def tables(b):
        tables_block(b, mix_in, read, local_out, total, carry, b == blocks - 1)

    prefix = Prefix(ep_count, total, outgoing, incoming, before, prefix_sems)

    def wait_loads(loads):
        for load in loads:
            load.wait()

    remote = chips - 1
    last_step = len(steps) - 1

    def prefix_step(number):
        prefix.receive(number)
        if number < last_step:
            prefix.send(number + 1)

    def mixer_start():
        prefix.begin()
        prefix.send(0)

    def heads():
        columns = read.shape[1]
        groups, width = total.shape[1], total.shape[3]
        ones = head_ones(width)
        for group in range(groups):
            at = pl.ds(group * width, width)
            heads_out = dot(read[:, at], spread(before[1, group])) + local_out[:, at]
            center = heads_out - dot_right(heads_out, ones) / HD
            variance = dot_right(center * center, ones) / HD
            mixed[:, at] = (center * lax.rsqrt(variance + 1.0) * gain_ref[:, at]).astype(BF16)

    def project():
        weight_loads[3].wait()
        out_rows = tokens // tp_count
        tile = out_w.shape[1] // 4
        for number in range(4):
            at = pl.ds(number * tile, tile)
            part = dot(mixed[...], out_w[:, at]).astype(BF16)
            for t in range(tp_count):
                product[t, :, at] = part[t * out_rows : (t + 1) * out_rows]

    reduce = Reduce(tp_count, product, landing, reduce_sems)

    out_copies = [
        pltpu.make_async_copy(source, target, load_sems.at[10 + i])
        for i, (source, target) in enumerate(
            ((mixer_out, mixer_hbm_out), (moe_out, moe_hbm_out))
        )
    ]

    def reduce_pass():
        for number in range(len(bits) - 1):
            reduce.land(number)
            reduce.start_passed(number + 1)
            reduce.start_finals(number + 1)

    def reduce_last():
        reduce.last(mixer_out)
        out_copies[0].start()

    def origin(n):
        pl.when(jnp.logical_not(inner))(lambda: back.origin(sources[n]))

    relays = back.relays()

    def run(count):
        @pl.when(inner)
        def _():
            for _ in itertools.islice(relays, count):
                pass

    def relay_inner(n):
        seen = set(exchanges[n].seen)
        pl.when(inner)(lambda: relay(n))
        exchanges[n].seen = seen

    def relay_outer(n):
        pl.when(jnp.logical_not(inner))(lambda: relay(n))

    def collect():
        back.collect()
        out_copies[1].start()

    inner = (chip > 0) & (chip < chips - 1)

    def landed_inner(n):
        pl.when(inner)(lambda: landed(n))

    def landed_outer(n):
        pl.when(jnp.logical_not(inner))(lambda: landed(n))

    def finish_dispatch():
        dispatch.finish(order)
        for exchange in exchanges[1:]:
            exchange.finish()

    def finish_hidden():
        for exchange in hidden_exchanges:
            exchange.finish()
        prefix.finish()

    def take_second():
        dispatch.take_second(exchanges[remote])

    def second_inner():
        pl.when(inner)(take_second)

    def second_outer():
        pl.when(jnp.logical_not(inner))(take_second)

    more = [(tables, b) for b in range(blocks)]
    chain = [(prefix_step, number) for number in range(len(steps))]
    all_mixer = pltpu.make_async_copy(mix_in, mix_in, load_sems.at[1])
    plan = [(wait_loads, [all_mixer]), *more[:1], (landed_half, 1, 0)]
    plan += [(wait_loads, weight_loads[:2]), (gate_up, 0), (landed_half, 1, 1), (landed_rest, 1)]
    plan += [(landed_inner, 2)] * (remote > 1)
    plan += [*more[1:2]]
    plan += [(relay, 1), (dispatch.passing,)] if remote > 1 else []
    plan += [(landed_inner, 3)] * (remote > 2)
    plan += [(landed_outer, 2)] * (remote > 1)
    plan += more[2:3]
    plan += [(second_inner,)] * (remote == 3)
    plan += [(share_rest, 1)] if remote > 1 else []
    plan += [(relay_inner, 2)] if remote > 2 else []
    plan += [(gate_up, 1), (relay_hidden, 0)] if remote > 1 else []
    plan += [(landed_outer, 3), (relay_outer, 2)] if remote > 2 else []
    plan += [*more[3:], (mixer_start,)]
    plan += [(second_outer,)] * (remote == 3)
    for n in range(2, remote):
        if n > 2:
            plan += [(landed, n + 1), (relay, n)]
        plan += [(share_rest, n), *chain[:1], (relay_hidden, n - 1), (gate_up, n)]
        chain = chain[1:] if n == 2 else chain
    plan += [(take_second,)] * (remote != 3)
    plan += [(relay, remote), (share_rest, remote), (gate_up, remote)]
    plan += [(wait_loads, weight_loads[2:3])]
    plan += [(down, 1)] if remote > 2 else []
    plan += [*chain[:1], (relay_hidden, remote - 1)]
    plan += [(origin, 1)] if remote > 2 else []
    plan += [*chain[1:], (heads,), (relay_hidden, remote), (project,)]
    plan += [(reduce.start_passed, 0), (reduce.start_finals, 0)]
    plan += [(down, n) for n in range(2 if remote > 2 else 1, remote + 1)]
    plan += [(origin, n) for n in range(remote, 1 if remote > 2 else 0, -1)]
    plan += [(finish_dispatch,), (down, 0)]
    plan += [(run, back.parts + 2), (reduce_pass,), (run, None)]
    plan += [(finish_hidden,), (reduce_last,), (collect,)]
    for step, (action, *given) in enumerate(plan):
        with jax.named_scope(f"{action.__name__}#{step}"):
            action(*given)

    reduce.finish()
    back.finish()
    for copy in out_copies:
        copy.wait()


def settle_kernel(*refs):
    sems = refs[-1]
    count = (len(refs) - 1) // 3
    takes, puts = [], []
    for i in range(count):
        held = refs[2 * count + i]
        takes.append(pltpu.make_async_copy(refs[i], held, sems.at[0, i]))
        puts.append(pltpu.make_async_copy(held, refs[count + i], sems.at[1, i]))
    for take in takes:
        take.start()
    for take, put in zip(takes, puts):
        take.wait()
        put.start()
    for put in puts:
        put.wait()


def settle(*arrays):
    hbm = pl.BlockSpec(memory_space=pltpu.HBM)
    return pl.pallas_call(
        settle_kernel,
        out_shape=[jax.ShapeDtypeStruct(a.shape, a.dtype) for a in arrays],
        in_specs=[hbm] * len(arrays),
        out_specs=[hbm] * len(arrays),
        scratch_shapes=[pltpu.VMEM(a.shape, a.dtype) for a in arrays]
        + [pltpu.SemaphoreType.DMA((2, len(arrays)))],
        compiler_params=pltpu.CompilerParams(vmem_limit_bytes=63 * 2**20),
        name="settle",
    )(*arrays)


def local(
    receptance,
    key_in,
    value_in,
    decay_in,
    rate_in,
    norm_gain,
    out_weight,
    moe_in,
    ffn_gain,
    routes,
    route_weights,
    gate_weight,
    up_weight,
    down_weight,
):
    tp_count, ep_count = lax.axis_size("tp"), lax.axis_size("ep")
    row_count, feature_count = moe_in.shape
    expert_count = gate_weight.shape[0] * ep_count
    cap = 5 * row_count * routes.shape[1] // (4 * expert_count)
    cap = -(-cap // 16) * 16
    chips = ep_count // 2
    part_width = feature_count // tp_count
    units, out_part = gate_weight.shape[2], down_weight.shape[2]
    tokens, columns = receptance.shape
    width = group_width(columns)
    groups = columns // width
    steps = ep_count.bit_length() - 1
    out_rows = tokens // tp_count
    dim = out_weight.shape[1]
    hbm = pl.BlockSpec(memory_space=pltpu.HBM)
    state = (2, groups, HD, width)
    dma = pltpu.SemaphoreType.DMA

    buffers = [
        pltpu.VMEM((out_rows, dim), BF16),
        pltpu.VMEM((row_count, out_part), BF16),
        pltpu.VMEM((1, columns), F32),
        pltpu.VMEM((tp_count, 1, part_width), F32),
        pltpu.VMEM((routes.shape[1], row_count), routes.dtype),
        pltpu.VMEM((routes.shape[1], row_count), F32),
        pltpu.VMEM((ep_count, tp_count, row_count, part_width), BF16),
        pltpu.VMEM((ep_count, 2 * expert_count + 8, row_count), F32),
        pltpu.VMEM((row_count, part_width), BF16),
        pltpu.VMEM((5, tokens, columns), BF16),
        pltpu.VMEM((feature_count, units), BF16),
        pltpu.VMEM((feature_count, units), BF16),
        pltpu.VMEM(down_weight.shape[1:], BF16),
        pltpu.VMEM(out_weight.shape, BF16),
        pltpu.VMEM((2 * cap, feature_count), BF16),
        pltpu.VMEM((chips, tp_count, 2 * cap, units), BF16),
        pltpu.VMEM((tokens, columns), BF16),
        pltpu.VMEM((tokens, columns), F32),
        pltpu.VMEM(state, F32),
        pltpu.VMEM(state, BF16),
        pltpu.VMEM((steps, *state), BF16),
        pltpu.VMEM((steps, *state), BF16),
        pltpu.VMEM(state, F32),
        pltpu.VMEM((tokens, columns), BF16),
        pltpu.VMEM((tp_count, out_rows, dim), BF16),
        pltpu.VMEM((tp_count, out_rows, dim), BF16),
        pltpu.VMEM((ep_count, row_count, out_part), BF16),
        pltpu.VMEM((chips, row_count, out_part), BF16),
        pltpu.VMEM((chips, row_count, out_part), BF16),
        pltpu.VMEM((chips, row_count, out_part), BF16),
        pltpu.VMEM((chips, row_count, out_part), BF16),
    ]
    sems = [
        dma((12,)),
        dma((3, chips, 2)),
        dma((3, chips)),
        dma((chips + 1,)),
        dma((chips + 1,)),
        dma((2, 2, 2)),
        dma((chips - 1, 2 * tp_count - 1)),
        dma((chips, 2 * tp_count - 1)),
        dma((2, steps)),
        dma((2 * tp_count - 1,)),
        dma((2 + 9 * chips,)),
    ]
    def kernel(r, k, v, d, a, *refs):
        layer_kernel(tp_count, ep_count, cap, expert_count, (r, k, v, d, a), *refs)

    results = pl.pallas_call(
        kernel,
        out_shape=[
            jax.ShapeDtypeStruct((out_rows, dim), BF16),
            jax.ShapeDtypeStruct((row_count, out_part), BF16),
        ],
        in_specs=[hbm] * 14,
        out_specs=[hbm, hbm],
        scratch_shapes=buffers + sems,
        compiler_params=pltpu.CompilerParams(
            collective_id=0, has_side_effects=True, vmem_limit_bytes=63 * 2**20
        ),
        name="layer",
    )(
        receptance,
        key_in,
        value_in,
        decay_in,
        rate_in,
        norm_gain[None],
        out_weight,
        moe_in,
        ffn_gain.reshape(tp_count, 1, part_width),
        routes.T,
        route_weights.T,
        gate_weight[0],
        up_weight[0],
        down_weight[0],
    )
    return settle(*results)


def solution(mesh):
    return jax.shard_map(
        local,
        mesh=mesh,
        in_specs=(
            P("ep", "tp"),
            P("ep", "tp"),
            P("ep", "tp"),
            P("ep", "tp"),
            P("ep", "tp"),
            P("tp"),
            P("tp", None),
            P("ep", None),
            P(),
            P("ep", None),
            P("ep", None),
            P("ep", None, "tp"),
            P("ep", None, "tp"),
            P("ep", None, "tp"),
        ),
        out_specs=(P(("ep", "tp"), None), P("ep", "tp")),
        check_vma=False,
    )
```
